32 devices in a mesh: sp: 8 (over z, core), tp: 4 (over y, x).
Axes of the slice: x: 2, y: 2, z: 4, core: 2. Of those that a mesh axis runs over, the one named last changes fastest.
Arguments:
- tokens: bfloat16 [2048, 4096], P('sp'), may hold values from -6 to 6
- norm_gain: float32 [2, 4096], replicated, may hold values from 0.1 to 1.9
- w_outer: bfloat16 [2, 4096, 1024], P(None, 'sp', 'tp'), may hold values from -0.09375 to 0.09375
- w_inner: bfloat16 [2, 4096, 1024], P(None, 'sp', 'tp'), may hold values from -0.09375 to 0.09375
- w_value: bfloat16 [2, 4096, 1024], P(None, 'sp', 'tp'), may hold values from -0.09375 to 0.09375
- w_back: bfloat16 [2, 1024, 4096], P(None, 'sp', 'tp'), may hold values from -0.1875 to 0.1875
- taps: float32 [2, 3, 1024], P(None, None, 'tp'), may hold values from -3 to 3
Outputs:
- result: bfloat16 [2048, 4096], P('sp', 'tp')
The draws below stay inside these ranges and needn't reach their ends.
All inputs are finite; a program needn't handle non-finite values.
Results may differ from the reference program's by a relative error of at most 0.022.
Values may be sent and summed in bfloat16 or wider, within the bound.
A program may use at most 64 MiB of HBM per device.

```python
import jax
import jax.numpy as jnp
from jax import lax

D = 4096
MIX = 1024
LAYERS = 2
TAPS = 3
TOKENS = 2048


def level_of(own_key, shape, cuts, low, top_value):
    factor_of = 1.0
    for dim, blocks in cuts:
        draws = jax.random.uniform(jax.random.fold_in(jax.random.fold_in(own_key, 6), dim), (blocks,), jnp.float32, low / len(cuts), top_value / len(cuts))
        factor_of = factor_of * jnp.repeat(jnp.exp(draws), shape[dim] // blocks).reshape((-1,) + (1,) * (len(shape) - 1 - dim))
    return factor_of


def bell_draw(key, extent, spread, bound, split=(), dtype=jnp.bfloat16):
    loudness = level_of(key, extent, split, -0.22, 0.18) if split else 1.0
    result = jax.random.normal(key, extent, jnp.float32) * spread * loudness
    return jnp.minimum(jnp.maximum(result, -bound), bound).astype(dtype)


def setup_inputs(seed: int = 0) -> dict:
    key_list = jax.random.split(jax.random.key(seed), 8)
    return {
        "tokens": bell_draw(key_list[0], (TOKENS, D), 1.0, 6.0, ((0, 8),)),
        "norm_gain": jnp.clip(1.0 + 0.18 * jax.random.normal(key_list[1], (LAYERS, D), jnp.float32), 0.1, 1.9),
        "w_outer": bell_draw(key_list[2], (LAYERS, D, MIX), D ** -0.5, 0.09375, ((1, 8), (2, 4))),
        "w_inner": bell_draw(key_list[3], (LAYERS, D, MIX), D ** -0.5, 0.09375, ((1, 8), (2, 4))),
        "w_value": bell_draw(key_list[4], (LAYERS, D, MIX), D ** -0.5, 0.09375, ((1, 8), (2, 4))),
        "w_back": bell_draw(key_list[5], (LAYERS, MIX, D), MIX ** -0.5, 0.1875, ((1, 8), (2, 4))),
        "taps": bell_draw(key_list[6], (LAYERS, TAPS, MIX), 0.6, 3.0, ((2, 4),), jnp.float32),
    }


eps = 1e-06

def reference(tokens, norm_gain, w_outer, w_inner, w_value, w_back, taps):
    current = tokens
    for layer in range(LAYERS):
        xf = current.astype(jnp.float32)
        normed = (xf * lax.rsqrt(lax.optimization_barrier(jnp.mean(xf * xf, axis=-1, keepdims=True)) + eps) * norm_gain[layer]).astype(jnp.bfloat16)
        outer = jnp.dot(normed, w_outer[layer], preferred_element_type=jnp.float32).astype(jnp.bfloat16)
        inner = jnp.dot(normed, w_inner[layer], preferred_element_type=jnp.float32).astype(jnp.bfloat16)
        value = jnp.dot(normed, w_value[layer], preferred_element_type=jnp.float32).astype(jnp.bfloat16)
        mixed = (inner.astype(jnp.float32) * value.astype(jnp.float32)).astype(jnp.bfloat16)
        padded = jnp.pad(mixed.astype(jnp.float32), ((2, 0), (0, 0)))
        conv = taps[layer, 0] * padded[:-2] + taps[layer, 1] * padded[1:-1] + taps[layer, 2] * padded[2:]
        gated = (outer.astype(jnp.float32) * conv).astype(jnp.bfloat16)
        proj = jnp.dot(gated, w_back[layer], preferred_element_type=jnp.float32)
        current = (current.astype(jnp.float32) + proj).astype(jnp.bfloat16)
    return current
```

```python
import functools

import jax
import jax.numpy as jnp
from jax import lax
from jax.experimental import pallas as pl
from jax.experimental.pallas import tpu as pltpu
from jax.sharding import PartitionSpec as P

MESH = pl.DeviceIdType.MESH
f32 = jnp.float32
bf16 = jnp.bfloat16

eps = 1e-06

OUTER, INNER, VALUE, BACK = 0, 1, 2, 3
FIRST = (INNER, VALUE, OUTER, BACK)
SECOND = tuple(4 + m for m in FIRST)
PIECES = (1, 1, 1, 2, 4, 2, 2, 4)
KINDS = 9


def shifted(block, axis, distance):
    devices = range(lax.axis_size(axis))
    route = [(i - distance, i) for i in devices if i - distance in devices]
    return lax.ppermute(block, axis, route)


def per_device(tokens, norm_gain, w_outer, w_inner, w_value, w_back, taps):
    layers = w_outer.shape[0]
    count = tokens.shape[0]
    feats = w_back.shape[2]
    own = lax.axis_index("tp")
    held = (
        lax.all_gather(w_outer, "sp", axis=1, tiled=True),
        lax.all_gather(w_inner, "sp", axis=1, tiled=True),
        lax.all_gather(w_value, "sp", axis=1, tiled=True),
        lax.all_gather(w_back, "sp", axis=1, tiled=True),
    )
    current = tokens
    resid = lax.dynamic_slice_in_dim(tokens, own * feats, feats, 1)
    for layer in range(layers):
        if layer > 0:
            current = lax.all_gather(resid, "tp", axis=1, tiled=True)
        xf = current.astype(jnp.float32)
        normed = (
            xf * lax.rsqrt(jnp.mean(xf * xf, axis=-1, keepdims=True) + eps) * norm_gain[layer]
        ).astype(jnp.bfloat16)
        outer = jnp.dot(normed, held[0][layer], preferred_element_type=jnp.float32)
        inner = jnp.dot(normed, held[1][layer], preferred_element_type=jnp.float32)
        value = jnp.dot(normed, held[2][layer], preferred_element_type=jnp.float32)
        outer = outer.astype(jnp.bfloat16)
        inner = inner.astype(jnp.bfloat16)
        value = value.astype(jnp.bfloat16)
        mixed = (inner.astype(jnp.float32) * value.astype(jnp.float32)).astype(jnp.bfloat16)
        before = shifted(mixed[count - 2 :], "sp", 1)
        padded = jnp.concatenate([before, mixed], axis=0).astype(jnp.float32)
        conv = (
            taps[layer, 0] * padded[:count]
            + taps[layer, 1] * padded[1 : count + 1]
            + taps[layer, 2] * padded[2:]
        )
        gated = (outer.astype(jnp.float32) * conv).astype(jnp.bfloat16)
        whole = lax.all_gather(gated, "tp", axis=1, tiled=True)
        proj = jnp.dot(whole, held[3][layer], preferred_element_type=jnp.float32)
        resid = (resid.astype(jnp.float32) + proj).astype(jnp.bfloat16)
    return resid


def first_chunk(u):
    return sum(PIECES[:u])


def mixer_kernel(
    tok, gain, w_outer, w_inner, w_value, w_back, taps, out,
    xr, x1, scl, win, wback, acc, bacc, ss, gat, gat_end, mixed, halo,
    sem_local, sem_tok, tok_send, tok_recv, w_send, w_recv,
    g_send, g_recv, h_send, h_recv, e_send, e_recv,
):
    s, t = lax.axis_index("sp"), lax.axis_index("tp")
    n_sp, n_tp = win.shape[1], xr.shape[1]
    rows, feats = xr.shape[2:]
    half = rows // 2
    width = feats * n_tp
    units = len(PIECES)
    core = lax.rem(s, 2)
    flip = 1 - 2 * core
    left = s < n_sp // 2
    side = jnp.where(left, 1, -1)
    plane = lax.div(s, 2)
    planes = n_sp // 2
    is_end = jnp.logical_or(plane == 0, plane == planes - 1)
    is_mid = jnp.logical_not(is_end)
    partner = s + flip
    near = jnp.where(is_mid, s - 2 * side, s + 2 * side)
    opp = jnp.where(is_mid, s + 2 * side, s + 4 * side)
    far = jnp.where(is_mid, s + 4 * side, s + 6 * side)
    tx = t + 1 - 2 * lax.rem(t, 2)
    ty = t + 2 - 4 * lax.div(t, 2)
    td = n_tp - 1 - t

    barrier = pltpu.get_barrier_semaphore()

    def greet(sp, tp):
        pl.semaphore_signal(barrier, inc=1, device_id=(sp, tp), device_id_type=MESH)

    greet(partner, t)
    greet(s, tx)
    greet(s, ty)
    greet(near, t)
    greet(near + flip, t)

    @pl.when(is_mid)
    def _():
        greet(opp, t)
        greet(opp + flip, t)
    pl.semaphore_wait(barrier, jnp.where(is_mid, 7, 5))

    projections = (w_outer, w_inner, w_value)

    def own_w(u):
        layer, m = u // 4, u % 4
        return projections[m].at[layer] if m < 3 else w_back.at[layer]

    def held_w(u, source):
        layer, m = u // 4, u % 4
        return win.at[3 * layer + m, source] if m < 3 else wback.at[layer, source]

    def remote(a, b, ssem, rsem, sp, tp):
        return pltpu.make_async_remote_copy(
            src_ref=a, dst_ref=b, send_sem=ssem, recv_sem=rsem, device_id=(sp, tp), device_id_type=MESH
        )

    def piece(ref, u, k):
        size = ref.shape[0] // PIECES[u]
        return ref.at[pl.ds(k * size, size)]

    def w_copy(u, k, source, kind, target, own=False):
        to = piece(held_w(u, source), u, k)
        a = piece(own_w(u), u, k) if own else to
        i = first_chunk(u) + k
        return remote(a, to, w_send.at[i, kind], w_recv.at[i, source], target, t)

    def send_own(u, kind, target):
        for k in range(PIECES[u]):
            w_copy(u, k, s, kind, target, own=True).start()

    def pieces_of(u):
        return range(PIECES[u])

    def relay_near(u, ks=None):
        for k in ks or pieces_of(u):
            w_copy(u, k, near, 3, partner).wait_recv()

            @pl.when(is_mid)
            def _():
                w_copy(u, k, near, 4, opp).start()
            w_copy(u, k, near, 3, partner).start()

    def relay_across(u, source, kind, ks=None):
        for k in ks or pieces_of(u):
            w_copy(u, k, source, kind, partner).wait_recv()
            if u >= 3:
                @pl.when(is_mid)
                def _():
                    w_copy(u, k, source, kind + 1, near).start()
            w_copy(u, k, source, kind, partner).start()

    def relay_opp(u, ks=None):
        relay_across(u, opp, 5, ks)

    def relay_far(u, ks=None):
        relay_across(u, far, 7, ks)

    def settle(u, source):
        for k in pieces_of(u):
            w_copy(u, k, source + flip, 1, partner).wait_recv()

    def local_w(u):
        return pltpu.make_async_copy(own_w(u), held_w(u, s), sem_local.at[u])

    def tok_cols(j):
        return tok.at[:, pl.ds(pl.multiple_of(j * feats, feats), feats)]

    def tok_local(j):
        return pltpu.make_async_copy(tok_cols(j), xr.at[1, j], sem_tok.at[j])

    def tok_part(h):
        cols = pl.ds(pl.multiple_of(t * feats, feats), feats)
        return remote(
            tok.at[pl.ds(h * half, half), cols], xr.at[0, t, pl.ds(h * half, half)],
            tok_send.at[h], tok_recv.at[h], near, t,
        )

    def end_part(h):
        return remote(
            gat_end.at[pl.ds(h * half, half)], gat.at[0, t, pl.ds(h * half, half)],
            e_send.at[h], e_recv.at[h], near, t,
        )

    class Gather:
        def __init__(self, g, buf):
            self.g, self.buf = g, buf

        def part(self, block, h, k, target):
            size = self.buf.shape[1] // 2
            ref = self.buf.at[block, pl.ds(h * size, size)]
            return remote(ref, ref, g_send.at[self.g, k], g_recv.at[self.g, k], s, target)

        def start(self, h):
            if h == 0:
                self.part(t, 0, 0, tx).start()
                self.part(t, 0, 3, ty).start()
            else:
                self.part(t, 1, 1, ty).start()
                self.part(t, 1, 2, tx).start()

        def start_all(self):
            self.part(t, 0, 0, tx).start()
            self.part(t, 1, 1, ty).start()
            self.part(t, 1, 2, tx).start()
            self.part(t, 0, 3, ty).start()

        def forward(self, h):
            if h == 0:
                self.part(tx, 0, 0, tx).wait_recv()
                self.part(tx, 0, 4, ty).start()
            else:
                self.part(ty, 1, 1, ty).wait_recv()
                self.part(ty, 1, 5, tx).start()

        def beside(self):
            self.part(tx, 1, 2, tx).wait_recv()
            self.part(ty, 0, 3, ty).wait_recv()

        def across(self):
            self.part(td, 0, 4, ty).wait_recv()
            self.part(td, 1, 5, tx).wait_recv()

        def drain(self):
            self.part(t, 0, 0, tx).wait_send()
            self.part(t, 1, 1, ty).wait_send()
            self.part(t, 1, 2, tx).wait_send()
            self.part(t, 0, 3, ty).wait_send()
            self.part(tx, 0, 4, ty).wait_send()
            self.part(ty, 1, 5, tx).wait_send()

    gather_tok = Gather(0, xr.at[0])
    gather_gat = (Gather(1, gat.at[0]), Gather(3, gat.at[1]))
    gather_x = Gather(2, x1)

    def scale(layer, source, b, j):
        step = 64

        def tile(r, carry):
            span = pl.ds(pl.multiple_of(r * step, step), step)
            x = source[j, span, :].astype(f32)
            sq = x * x
            part = sq[:, :128]
            for q in range(1, feats // 128):
                part = part + sq[:, 128 * q : 128 * (q + 1)]
            ss[b, span, :] += part
            cols = pl.ds(pl.multiple_of(j * feats, feats), feats)
            scl[b, j, span, :] = (x * gain[layer : layer + 1, cols]).astype(bf16)
            return carry

        lax.fori_loop(0, rows // step, tile, 0)

    def project(layer, m, sources, first):
        blocks = (0, 1) if layer == 0 else (0,)
        depth = win.shape[2]

        def tile(b, carry):
            total = None
            for source in sources:
                z = lax.div(source, 2)
                w = win[3 * layer + m, pl.ds(2 * z, 2)].reshape(2 * depth, win.shape[3])
                dot = jnp.dot(scl[b, z], w, preferred_element_type=f32)
                total = dot if total is None else total + dot
            if first:
                acc[m, b] = total
            else:
                acc[m, b] += total
            return carry

        if len(blocks) == 1:
            tile(0, 0)
        else:
            lax.fori_loop(0, len(blocks), tile, 0)

    def inv_of(b):
        return lax.rsqrt(jnp.sum(ss[b], axis=-1, keepdims=True) / width + eps)

    def mix(b, slot):
        inv = inv_of(b)
        inner = (acc[INNER, b] * inv).astype(bf16)
        value = (acc[VALUE, b] * inv).astype(bf16)
        mixed[slot] = (inner.astype(f32) * value.astype(f32)).astype(bf16)

    def convolve(layer, b, slot):
        now = mixed[slot].astype(f32)
        tail = halo[slot].astype(f32)
        row = lax.broadcasted_iota(jnp.int32, now.shape, 0)
        one = jnp.where(row == 0, tail[15:16], pltpu.roll(now, 1, 0))
        two = pltpu.roll(now, 2, 0)
        two = jnp.where(row == 0, tail[14:15], jnp.where(row == 1, tail[15:16], two))
        acc[VALUE, b] = taps[layer, 0:1] * two + taps[layer, 1:2] * one + taps[layer, 2:3] * now

    def gate(b):
        outer = (acc[OUTER, b] * inv_of(b)).astype(bf16).astype(f32)
        return (outer * acc[VALUE, b]).astype(bf16)

    def tail_copy(slot, to_slot, h, target):
        return remote(
            mixed.at[slot, pl.ds(rows - 16, 16)], halo.at[to_slot], h_send.at[slot], h_recv.at[h], target, t
        )

    def back_dot(layer, sources, cols):
        total = None
        for source in sources:
            z = lax.div(source, 2)
            w = wback[layer, pl.ds(2 * z, 2), :, cols].reshape(2 * wback.shape[2], cols.size)
            dot = jnp.dot(gat[layer, z], w, preferred_element_type=f32)
            total = dot if total is None else total + dot
        return total

    def by_columns(body):
        step = 256

        def tile(c, carry):
            body(pl.ds(pl.multiple_of(c * step, step), step))
            return carry

        lax.fori_loop(0, feats // step, tile, 0)

    @pl.when(is_mid)
    def _():
        for u in FIRST[:3]:
            send_own(u, 0, opp)
        for u in FIRST + SECOND:
            send_own(u, 1, partner)
        for u in FIRST[3:] + SECOND:
            send_own(u, 2, near)
        for j in range(n_tp):
            tok_local(j).start()
        for u in FIRST + SECOND:
            local_w(u).start()
        ss[...] = jnp.zeros(ss.shape, f32)
        for j in range(n_tp):
            tok_local(j).wait()

        def scale_own(j, carry):
            scale(0, xr.at[1], 1, j)
            return carry

        lax.fori_loop(0, n_tp, scale_own, 0)
        relay_near(INNER)
        send_own(BACK, 0, opp)
        relay_opp(INNER)
        for h in range(2):
            tok_part(h).wait_recv()
            gather_tok.start(h)
            relay_opp((VALUE, OUTER)[h])
        gather_tok.forward(0)
        relay_near(VALUE)
        relay_far(INNER)
        scale(0, xr.at[0], 0, t)
        gather_tok.forward(1)
        relay_near(OUTER)
        relay_opp(BACK)
        gather_tok.beside()
        scale(0, xr.at[0], 0, tx)
        scale(0, xr.at[0], 0, ty)
        gather_tok.across()
        scale(0, xr.at[0], 0, td)
        for u in FIRST[:3]:
            local_w(u).wait()
            settle(u, s)
            settle(u, near)
            settle(u, opp)
        settle(INNER, far)
        project(0, INNER, (s, near, opp, far), True)
        relay_near(BACK)
        for u in SECOND[:3]:
            send_own(u, 0, opp)
        project(0, OUTER, (s, near, opp), True)
        relay_far(VALUE)
        settle(VALUE, far)
        project(0, VALUE, (s, near, opp, far), True)
        for b in range(2):
            mix(b, b)

        @pl.when(core == 0)
        def _():
            for b in range(2):
                tail_copy(b, b, b, partner).start()

        @pl.when(jnp.logical_and(core == 1, left))
        def _():
            tail_copy(0, 1, 1, partner).start()
            tail_copy(1, 1, 1, s + 1).start()

        @pl.when(jnp.logical_and(core == 1, jnp.logical_not(left)))
        def _():
            tail_copy(1, 0, 0, partner).start()

        for b in range(2):
            if b == 0:
                start_of_all = s == 2

                @pl.when(start_of_all)
                def _():
                    halo[0] = jnp.zeros(halo.shape[1:], bf16)

                @pl.when(jnp.logical_not(start_of_all))
                def _():
                    tail_copy(0, 0, 0, partner).wait_recv()
            else:
                tail_copy(1, 1, 1, partner).wait_recv()
            convolve(0, b, b)
        relay_far(OUTER)
        settle(OUTER, far)
        project(0, OUTER, (far,), False)
        gat_end[...] = gate(0)
        for h in range(2):
            end_part(h).start()
        gat[0, t] = gate(1)
        gather_gat[0].start_all()
        relay_near(SECOND[0])
        gather_gat[0].forward(0)
        gather_gat[0].forward(1)
        relay_far(BACK)

    @pl.when(is_end)
    def _():
        send_own(INNER, 0, near)
        for h in range(2):
            tok_part(h).start()
        for u in FIRST[1:] + SECOND:
            send_own(u, 0, near)
        for u in FIRST[3:] + SECOND:
            send_own(u, 1, partner)
        tok_local(t).start()
        for u in FIRST[3:] + SECOND:
            local_w(u).start()
        tok_local(t).wait()
        for u in FIRST[3:] + SECOND:
            relay_near(u)
        relay_opp(BACK)
        for h in range(2):
            end_part(h).wait_recv()
            gather_gat[0].start(h)
        relay_far(BACK, (0,))
        gather_gat[0].forward(0)
        gather_gat[0].forward(1)
        relay_far(BACK, (1,))

    gather_gat[0].beside()
    gather_gat[0].across()
    local_w(BACK).wait()
    for source in (s, near, opp, far):
        settle(BACK, source)

    def finish_first(cols):
        total = xr[1, t, :, cols].astype(f32) + back_dot(0, (s, near, opp, far), cols)
        x1[t, :, cols] = total.astype(bf16)

    by_columns(finish_first)
    gather_x.start_all()

    @pl.when(is_mid)
    def _():
        relay_near(SECOND[1])
    relay_opp(SECOND[0])

    @pl.when(is_mid)
    def _():
        relay_near(SECOND[2])
        send_own(SECOND[3], 0, opp)
    ss[0] = jnp.zeros(ss.shape[1:], f32)
    scale(1, x1, 0, t)
    gather_x.forward(0)
    gather_x.forward(1)
    relay_opp(SECOND[1])

    @pl.when(is_mid)
    def _():
        relay_near(SECOND[3])
    gather_x.beside()
    scale(1, x1, 0, tx)
    scale(1, x1, 0, ty)
    relay_opp(SECOND[2])
    gather_x.across()
    scale(1, x1, 0, td)
    relay_far(SECOND[0])
    for u in SECOND[:3]:
        local_w(u).wait()
        settle(u, s)
        settle(u, near)
        settle(u, opp)
    for u in SECOND[:3]:
        project(1, u % 4, (s, near, opp), True)
    settle(SECOND[0], far)
    project(1, INNER, (far,), False)
    relay_far(SECOND[1])
    settle(SECOND[1], far)
    project(1, VALUE, (far,), False)

    @pl.when(is_mid)
    def _():
        @pl.when(core == 0)
        def _():
            for b in range(2):
                tail_copy(b, b, b, partner).wait_send()

        @pl.when(jnp.logical_and(core == 1, left))
        def _():
            tail_copy(0, 1, 1, partner).wait_send()
            tail_copy(1, 1, 1, s + 1).wait_send()

        @pl.when(jnp.logical_and(core == 1, jnp.logical_not(left)))
        def _():
            tail_copy(1, 0, 0, partner).wait_send()
    mix(0, 2)

    @pl.when(s < n_sp - 1)
    def _():
        tail_copy(2, 2, 2, s + 1).start()

    @pl.when(s == 0)
    def _():
        halo[2] = jnp.zeros(halo.shape[1:], bf16)

    @pl.when(s > 0)
    def _():
        tail_copy(2, 2, 2, partner).wait_recv()
    convolve(1, 0, 2)
    relay_far(SECOND[2])
    settle(SECOND[2], far)
    project(1, OUTER, (far,), False)
    gat[1, t] = gate(0)
    gather_gat[1].start_all()
    last = SECOND[3]
    relay_opp(last, (0, 1, 2))
    gather_gat[1].forward(0)
    gather_gat[1].forward(1)
    relay_opp(last, (3,))
    relay_far(last, (0,))
    gather_gat[1].beside()
    gather_gat[1].across()
    relay_far(last, (1,))
    local_w(last).wait()
    for source in (s, near, opp):
        settle(last, source)

    def start_last(cols):
        bacc[:, cols] = x1[t, :, cols].astype(f32) + back_dot(1, (s, near, opp), cols)

    by_columns(start_last)
    relay_far(last, (2, 3))
    settle(last, far)

    def finish_last(cols):
        out[:, cols] = (bacc[:, cols] + back_dot(1, (far,), cols)).astype(bf16)

    by_columns(finish_last)

    def sent(u, kind):
        for k in pieces_of(u):
            w_copy(u, k, s, kind, partner).wait_send()

    for u in range(units):
        if u >= 3:
            for kind in (0, 1, 3, 5, 7):
                sent(u, kind)

            @pl.when(is_mid)
            def _():
                for kind in (2, 4, 6, 8):
                    sent(u, kind)
        else:
            sent(u, 0)

            @pl.when(is_mid)
            def _():
                for kind in (1, 3, 4, 5, 7):
                    sent(u, kind)

    @pl.when(is_mid)
    def _():
        gather_tok.drain()
        for h in range(2):
            end_part(h).wait_send()

    @pl.when(is_end)
    def _():
        for h in range(2):
            tok_part(h).wait_send()
    gather_gat[0].drain()
    gather_x.drain()
    gather_gat[1].drain()

    @pl.when(s < n_sp - 1)
    def _():
        tail_copy(2, 2, 2, partner).wait_send()


def fused(tokens, norm_gain, w_outer, w_inner, w_value, w_back, taps):
    n_sp, n_tp = lax.axis_size("sp"), lax.axis_size("tp")
    rows, width = tokens.shape
    layers, depth, chans = w_outer.shape
    back_rows, feats = w_back.shape[1:]
    if 4 * layers != len(PIECES):
        return per_device(tokens, norm_gain, w_outer, w_inner, w_value, w_back, taps)
    chunks = sum(PIECES)
    dma = pltpu.SemaphoreType.DMA
    hbm, vmem = pl.BlockSpec(memory_space=pl.ANY), pl.BlockSpec(memory_space=pltpu.VMEM)
    return pl.pallas_call(
        mixer_kernel,
        out_shape=jax.ShapeDtypeStruct((rows, feats), bf16),
        in_specs=[hbm, vmem, hbm, hbm, hbm, hbm, vmem],
        out_specs=vmem,
        scratch_shapes=[
            pltpu.VMEM((2, n_tp, rows, feats), bf16),
            pltpu.VMEM((n_tp, rows, feats), bf16),
            pltpu.VMEM((2, n_tp, rows, feats), bf16),
            pltpu.VMEM((3 * layers, n_sp, depth, chans), bf16),
            pltpu.VMEM((layers, n_sp, back_rows, feats), bf16),
            pltpu.VMEM((3, 2, rows, chans), f32),
            pltpu.VMEM((rows, feats), f32),
            pltpu.VMEM((2, rows, 128), f32),
            pltpu.VMEM((layers, n_tp, rows, chans), bf16),
            pltpu.VMEM((rows, chans), bf16),
            pltpu.VMEM((3, rows, chans), bf16),
            pltpu.VMEM((3, 16, chans), bf16),
            dma((4 * layers,)),
            dma((n_tp,)),
            dma((2,)),
            dma((2,)),
            dma((chunks, KINDS)),
            dma((chunks, n_sp)),
            dma((4, 6)),
            dma((4, 6)),
            dma((3,)),
            dma((3,)),
            dma((2,)),
            dma((2,)),
        ],
        compiler_params=pltpu.CompilerParams(
            collective_id=0, has_side_effects=True, vmem_limit_bytes=60 * 1024 * 1024
        ),
        name="mixer",
    )(tokens, norm_gain, w_outer, w_inner, w_value, w_back, taps)


def solution(mesh):
    in_specs = (
        P("sp", None),
        P(),
        P(None, "sp", "tp"),
        P(None, "sp", "tp"),
        P(None, "sp", "tp"),
        P(None, "sp", "tp"),
        P(None, None, "tp"),
    )
    out_specs = P("sp", "tp")
    body = fused if (mesh.shape["sp"], mesh.shape["tp"]) == (8, 4) else per_device
    return jax.shard_map(
        body, mesh=mesh, in_specs=in_specs, out_specs=out_specs, check_vma=False
    )
```

```python
import functools

import jax
import jax.numpy as jnp
from jax import lax
from jax.experimental import pallas as pl
from jax.experimental.pallas import tpu as pltpu
from jax.sharding import PartitionSpec as P

MESH = pl.DeviceIdType.MESH
f32 = jnp.float32
bf16 = jnp.bfloat16

eps = 1e-06

OUTER, INNER, VALUE, BACK = 0, 1, 2, 3
FIRST = (INNER, VALUE, OUTER, BACK)
SECOND = tuple(4 + m for m in FIRST)
PIECES = (1, 1, 1, 2, 4, 2, 2, 4)
KINDS = 9


def shifted(block, axis, distance):
    devices = range(lax.axis_size(axis))
    route = [(i - distance, i) for i in devices if i - distance in devices]
    return lax.ppermute(block, axis, route)


def per_device(tokens, norm_gain, w_outer, w_inner, w_value, w_back, taps):
    layers = w_outer.shape[0]
    count = tokens.shape[0]
    feats = w_back.shape[2]
    own = lax.axis_index("tp")
    held = (
        lax.all_gather(w_outer, "sp", axis=1, tiled=True),
        lax.all_gather(w_inner, "sp", axis=1, tiled=True),
        lax.all_gather(w_value, "sp", axis=1, tiled=True),
        lax.all_gather(w_back, "sp", axis=1, tiled=True),
    )
    current = tokens
    resid = lax.dynamic_slice_in_dim(tokens, own * feats, feats, 1)
    for layer in range(layers):
        if layer > 0:
            current = lax.all_gather(resid, "tp", axis=1, tiled=True)
        xf = current.astype(jnp.float32)
        normed = (
            xf * lax.rsqrt(jnp.mean(xf * xf, axis=-1, keepdims=True) + eps) * norm_gain[layer]
        ).astype(jnp.bfloat16)
        outer = jnp.dot(normed, held[0][layer], preferred_element_type=jnp.float32)
        inner = jnp.dot(normed, held[1][layer], preferred_element_type=jnp.float32)
        value = jnp.dot(normed, held[2][layer], preferred_element_type=jnp.float32)
        outer = outer.astype(jnp.bfloat16)
        inner = inner.astype(jnp.bfloat16)
        value = value.astype(jnp.bfloat16)
        mixed = (inner.astype(jnp.float32) * value.astype(jnp.float32)).astype(jnp.bfloat16)
        before = shifted(mixed[count - 2 :], "sp", 1)
        padded = jnp.concatenate([before, mixed], axis=0).astype(jnp.float32)
        conv = (
            taps[layer, 0] * padded[:count]
            + taps[layer, 1] * padded[1 : count + 1]
            + taps[layer, 2] * padded[2:]
        )
        gated = (outer.astype(jnp.float32) * conv).astype(jnp.bfloat16)
        whole = lax.all_gather(gated, "tp", axis=1, tiled=True)
        proj = jnp.dot(whole, held[3][layer], preferred_element_type=jnp.float32)
        resid = (resid.astype(jnp.float32) + proj).astype(jnp.bfloat16)
    return resid


def first_chunk(u):
    return sum(PIECES[:u])


def mixer_kernel(
    tok, gain, w_outer, w_inner, w_value, w_back, taps, out,
    xr, x1, scl, win, wback, acc, bacc, ss, gat, gat_end, mixed, halo,
    sem_local, sem_tok, tok_send, tok_recv, w_send, w_recv, p_recv,
    g_send, g_recv, h_send, h_recv, e_send, e_recv,
):
    s, t = lax.axis_index("sp"), lax.axis_index("tp")
    n_sp, n_tp = win.shape[1], xr.shape[1]
    rows, feats = xr.shape[2:]
    half = rows // 2
    width = feats * n_tp
    units = len(PIECES)
    core = lax.rem(s, 2)
    flip = 1 - 2 * core
    left = s < n_sp // 2
    side = jnp.where(left, 1, -1)
    plane = lax.div(s, 2)
    planes = n_sp // 2
    is_end = jnp.logical_or(plane == 0, plane == planes - 1)
    is_mid = jnp.logical_not(is_end)
    partner = s + flip
    near = jnp.where(is_mid, s - 2 * side, s + 2 * side)
    opp = jnp.where(is_mid, s + 2 * side, s + 4 * side)
    far = jnp.where(is_mid, s + 4 * side, s + 6 * side)
    tx = t + 1 - 2 * lax.rem(t, 2)
    ty = t + 2 - 4 * lax.div(t, 2)
    td = n_tp - 1 - t

    barrier = pltpu.get_barrier_semaphore()

    def greet(sp, tp):
        pl.semaphore_signal(barrier, inc=1, device_id=(sp, tp), device_id_type=MESH)

    greet(partner, t)
    greet(s, tx)
    greet(s, ty)
    greet(near, t)
    greet(near + flip, t)

    @pl.when(is_mid)
    def _():
        greet(opp, t)
        greet(opp + flip, t)
    pl.semaphore_wait(barrier, jnp.where(is_mid, 7, 5))

    projections = (w_outer, w_inner, w_value)

    def own_w(u):
        layer, m = u // 4, u % 4
        return projections[m].at[layer] if m < 3 else w_back.at[layer]

    def held_w(u, source):
        layer, m = u // 4, u % 4
        return win.at[3 * layer + m, source] if m < 3 else wback.at[layer, source]

    def remote(a, b, ssem, rsem, sp, tp):
        return pltpu.make_async_remote_copy(
            src_ref=a, dst_ref=b, send_sem=ssem, recv_sem=rsem, device_id=(sp, tp), device_id_type=MESH
        )

    def piece(ref, u, k):
        size = ref.shape[0] // PIECES[u]
        return ref.at[pl.ds(k * size, size)]

    OWN, NEAR, OPP, FAR = 0, 1, 2, 3
    source_of = (s, near, opp, far)

    def w_copy(u, k, role, kind, to_role, target):
        to = piece(held_w(u, source_of[role]), u, k)
        a = piece(own_w(u), u, k) if role == OWN else to
        return remote(a, to, w_send.at[kind], w_recv.at[first_chunk(u) + k, to_role - 1], target, t)

    def to_partner(u, k, role):
        to = piece(held_w(u, source_of[role]), u, k)
        a = piece(own_w(u), u, k) if role == OWN else to
        return remote(a, to, w_send.at[role], p_recv.at[u, role], partner, t)

    def pieces_of(u):
        return range(PIECES[u])

    def arrived(u, k, role):
        to = piece(held_w(u, source_of[role]), u, k)
        remote(to, to, w_send.at[0], w_recv.at[first_chunk(u) + k, role - 1], partner, t).wait_recv()

    def send_opp(u):
        for k in pieces_of(u):
            w_copy(u, k, OWN, 4, OPP, opp).start()

    def send_near(u):
        for k in pieces_of(u):
            w_copy(u, k, OWN, 5, NEAR, near).start()

    def send_partner(u):
        for k in pieces_of(u):
            to_partner(u, k, OWN).start()

    def relay_near(u, ks=None):
        for k in ks or pieces_of(u):
            arrived(u, k, NEAR)

            @pl.when(is_mid)
            def _():
                w_copy(u, k, NEAR, 6, FAR, opp).start()
            to_partner(u, k, NEAR).start()

    def relay_across(u, role, ks=None):
        for k in ks or pieces_of(u):
            arrived(u, k, role)
            if u >= 3:
                @pl.when(is_mid)
                def _():
                    w_copy(u, k, role, 5 + role, role, near).start()
            to_partner(u, k, role).start()

    def relay_opp(u, ks=None):
        relay_across(u, OPP, ks)

    def relay_far(u, ks=None):
        relay_across(u, FAR, ks)

    def settle(u, role):
        to = held_w(u, source_of[role] + flip)
        remote(to, to, w_send.at[0], p_recv.at[u, role], partner, t).wait_recv()

    def sent(kind, count):
        ref = win.at[0, pl.ds(0, count)]
        remote(ref, ref, w_send.at[kind], p_recv.at[0, 0], partner, t).wait_send()

    def local_w(u):
        return pltpu.make_async_copy(own_w(u), held_w(u, s), sem_local.at[u])

    def tok_cols(j):
        return tok.at[:, pl.ds(pl.multiple_of(j * feats, feats), feats)]

    def tok_local(j):
        return pltpu.make_async_copy(tok_cols(j), xr.at[1, j], sem_tok.at[j])

    def tok_part(h):
        cols = pl.ds(pl.multiple_of(t * feats, feats), feats)
        return remote(
            tok.at[pl.ds(h * half, half), cols], xr.at[0, t, pl.ds(h * half, half)],
            tok_send.at[h], tok_recv.at[h], near, t,
        )

    def end_part(h):
        return remote(
            gat_end.at[pl.ds(h * half, half)], gat.at[0, t, pl.ds(h * half, half)],
            e_send.at[h], e_recv.at[h], near, t,
        )

    class Gather:
        def __init__(self, g, buf):
            self.g, self.buf = g, buf

        def part(self, block, h, k, target):
            size = self.buf.shape[1] // 2
            ref = self.buf.at[block, pl.ds(h * size, size)]
            slot = (0, 1, 2, 2, 3, 3)[k]
            return remote(ref, ref, g_send.at[self.g], g_recv.at[self.g, slot], s, target)

        def whole(self, blocks, slot):
            ref = self.buf.at[pl.ds(0, blocks)]
            return remote(ref, ref, g_send.at[self.g], g_recv.at[self.g, slot], s, tx)

        def start(self, h):
            if h == 0:
                self.part(t, 0, 0, tx).start()
                self.part(t, 0, 3, ty).start()
            else:
                self.part(t, 1, 1, ty).start()
                self.part(t, 1, 2, tx).start()

        def start_all(self):
            self.part(t, 0, 0, tx).start()
            self.part(t, 1, 1, ty).start()
            self.part(t, 1, 2, tx).start()
            self.part(t, 0, 3, ty).start()

        def forward(self, h):
            if h == 0:
                self.part(tx, 0, 0, tx).wait_recv()
                self.part(tx, 0, 4, ty).start()
            else:
                self.part(ty, 1, 1, ty).wait_recv()
                self.part(ty, 1, 5, tx).start()

        def beside(self):
            self.whole(1, 2).wait_recv()

        def across(self):
            self.whole(1, 3).wait_recv()

        def drain(self):
            self.whole(3, 0).wait_send()

    gather_tok = Gather(0, xr.at[0])
    gather_gat = (Gather(1, gat.at[0]), Gather(3, gat.at[1]))
    gather_x = Gather(2, x1)

    def scale(layer, source, b, j):
        step = 64

        def tile(r, carry):
            span = pl.ds(pl.multiple_of(r * step, step), step)
            x = source[j, span, :].astype(f32)
            sq = x * x
            part = sq[:, :128]
            for q in range(1, feats // 128):
                part = part + sq[:, 128 * q : 128 * (q + 1)]
            ss[b, span, :] += part
            cols = pl.ds(pl.multiple_of(j * feats, feats), feats)
            scl[b, j, span, :] = (x * gain[layer : layer + 1, cols]).astype(bf16)
            return carry

        lax.fori_loop(0, rows // step, tile, 0)

    def project(layer, m, sources, first):
        blocks = (0, 1) if layer == 0 else (0,)
        depth = win.shape[2]

        def tile(b, carry):
            total = None
            for role in sources:
                z = lax.div(source_of[role], 2)
                w = win[3 * layer + m, pl.ds(2 * z, 2)].reshape(2 * depth, win.shape[3])
                dot = jnp.dot(scl[b, z], w, preferred_element_type=f32)
                total = dot if total is None else total + dot
            if first:
                acc[m, b] = total
            else:
                acc[m, b] += total
            return carry

        if len(blocks) == 1:
            tile(0, 0)
        else:
            lax.fori_loop(0, len(blocks), tile, 0)

    def inv_of(b):
        return lax.rsqrt(jnp.sum(ss[b], axis=-1, keepdims=True) / width + eps)

    def mix(b, slot):
        inv = inv_of(b)
        inner = (acc[INNER, b] * inv).astype(bf16)
        value = (acc[VALUE, b] * inv).astype(bf16)
        mixed[slot] = (inner.astype(f32) * value.astype(f32)).astype(bf16)

    def convolve(layer, b, slot):
        now = mixed[slot].astype(f32)
        tail = halo[slot].astype(f32)
        row = lax.broadcasted_iota(jnp.int32, now.shape, 0)
        one = jnp.where(row == 0, tail[15:16], pltpu.roll(now, 1, 0))
        two = pltpu.roll(now, 2, 0)
        two = jnp.where(row == 0, tail[14:15], jnp.where(row == 1, tail[15:16], two))
        acc[VALUE, b] = taps[0, layer : layer + 1] * two + taps[1, layer : layer + 1] * one + taps[2, layer : layer + 1] * now

    def gate(b):
        outer = (acc[OUTER, b] * inv_of(b)).astype(bf16).astype(f32)
        return (outer * acc[VALUE, b]).astype(bf16)

    def tail_copy(slot, to_slot, h, target):
        return remote(
            mixed.at[slot, pl.ds(rows - 16, 16)], halo.at[to_slot], h_send.at[slot], h_recv.at[h], target, t
        )

    def back_dot(layer, sources, cols):
        total = None
        for role in sources:
            z = lax.div(source_of[role], 2)
            w = wback[layer, pl.ds(2 * z, 2), :, cols].reshape(2 * wback.shape[2], cols.size)
            dot = jnp.dot(gat[layer, z], w, preferred_element_type=f32)
            total = dot if total is None else total + dot
        return total

    def by_columns(body):
        step = 256

        def tile(c, carry):
            body(pl.ds(pl.multiple_of(c * step, step), step))
            return carry

        lax.fori_loop(0, feats // step, tile, 0)

    @pl.when(is_mid)
    def _():
        for u in FIRST[:3]:
            send_opp(u)
        for u in FIRST + SECOND:
            send_partner(u)
        for u in FIRST[3:] + SECOND:
            send_near(u)
        for j in range(n_tp):
            tok_local(j).start()
        for u in FIRST + SECOND:
            local_w(u).start()
        ss[...] = jnp.zeros(ss.shape, f32)
        for j in range(n_tp):
            tok_local(j).wait()

        def scale_own(j, carry):
            scale(0, xr.at[1], 1, j)
            return carry

        lax.fori_loop(0, n_tp, scale_own, 0)
        relay_near(INNER)
        send_opp(BACK)
        relay_opp(INNER)
        for h in range(2):
            tok_part(h).wait_recv()
            gather_tok.start(h)
            relay_opp((VALUE, OUTER)[h])
        gather_tok.forward(0)
        relay_near(VALUE)
        relay_far(INNER)
        scale(0, xr.at[0], 0, t)
        gather_tok.forward(1)
        relay_near(OUTER)
        relay_opp(BACK)
        gather_tok.beside()
        scale(0, xr.at[0], 0, tx)
        scale(0, xr.at[0], 0, ty)
        gather_tok.across()
        scale(0, xr.at[0], 0, td)
        for u in FIRST[:3]:
            local_w(u).wait()
            for role in (OWN, NEAR, OPP):
                settle(u, role)
        settle(INNER, FAR)
        project(0, INNER, (OWN, NEAR, OPP, FAR), True)
        project(0, VALUE, (OWN, NEAR, OPP), True)
        relay_far(VALUE)
        settle(VALUE, FAR)
        project(0, VALUE, (FAR,), False)
        for b in range(2):
            mix(b, b)

        @pl.when(core == 0)
        def _():
            for b in range(2):
                tail_copy(b, b, b, partner).start()

        @pl.when(jnp.logical_and(core == 1, left))
        def _():
            tail_copy(1, 1, 1, s + 1).start()
            tail_copy(0, 1, 1, partner).start()

        @pl.when(jnp.logical_and(core == 1, jnp.logical_not(left)))
        def _():
            tail_copy(1, 0, 0, partner).start()
        relay_near(BACK)
        for u in SECOND[:3]:
            send_opp(u)
        project(0, OUTER, (OWN, NEAR, OPP), True)
        relay_far(OUTER)
        for b in range(2):
            if b == 0:
                start_of_all = s == 2

                @pl.when(start_of_all)
                def _():
                    halo[0] = jnp.zeros(halo.shape[1:], bf16)

                @pl.when(jnp.logical_not(start_of_all))
                def _():
                    tail_copy(0, 0, 0, partner).wait_recv()
            else:
                tail_copy(1, 1, 1, partner).wait_recv()
            convolve(0, b, b)
        settle(OUTER, FAR)
        project(0, OUTER, (FAR,), False)
        gat_end[...] = gate(0)
        for h in range(2):
            end_part(h).start()
        gat[0, t] = gate(1)
        gather_gat[0].start_all()
        relay_near(SECOND[0])
        gather_gat[0].forward(0)
        gather_gat[0].forward(1)
        relay_far(BACK)

    @pl.when(is_end)
    def _():
        send_near(INNER)
        for h in range(2):
            tok_part(h).start()
        for u in FIRST[1:] + SECOND:
            send_near(u)
        for u in FIRST[3:] + SECOND:
            send_partner(u)
        tok_local(t).start()
        for u in FIRST[3:] + SECOND:
            local_w(u).start()
        tok_local(t).wait()
        for u in FIRST[3:] + SECOND:
            relay_near(u)
        relay_opp(BACK)
        for h in range(2):
            end_part(h).wait_recv()
            gather_gat[0].start(h)
        relay_far(BACK, (0,))
        gather_gat[0].forward(0)
        gather_gat[0].forward(1)
        relay_far(BACK, (1,))

    gather_gat[0].beside()
    gather_gat[0].across()
    local_w(BACK).wait()
    for role in (OWN, NEAR, OPP, FAR):
        settle(BACK, role)

    def finish_first(cols):
        total = xr[1, t, :, cols].astype(f32) + back_dot(0, (OWN, NEAR, OPP, FAR), cols)
        x1[t, :, cols] = total.astype(bf16)

    by_columns(finish_first)
    gather_x.start_all()

    @pl.when(is_mid)
    def _():
        relay_near(SECOND[1])
    relay_opp(SECOND[0])

    @pl.when(is_mid)
    def _():
        relay_near(SECOND[2])
    ss[0] = jnp.zeros(ss.shape[1:], f32)
    scale(1, x1, 0, t)
    gather_x.forward(0)
    gather_x.forward(1)
    relay_opp(SECOND[1])
    gather_x.beside()
    scale(1, x1, 0, tx)
    scale(1, x1, 0, ty)
    relay_opp(SECOND[2])
    gather_x.across()
    scale(1, x1, 0, td)
    relay_far(SECOND[0])
    for u in SECOND[:3]:
        local_w(u).wait()
        for role in (OWN, NEAR, OPP):
            settle(u, role)
    for u in SECOND[:3]:
        project(1, u % 4, (OWN, NEAR, OPP), True)
    settle(SECOND[0], FAR)
    project(1, INNER, (FAR,), False)
    relay_far(SECOND[1])
    settle(SECOND[1], FAR)
    project(1, VALUE, (FAR,), False)
    mix(0, 2)

    @pl.when(s < n_sp - 1)
    def _():
        tail_copy(2, 2, 2, s + 1).start()
    last = SECOND[3]

    @pl.when(is_mid)
    def _():
        send_opp(last)
        relay_near(last)
    relay_far(SECOND[2])

    @pl.when(is_mid)
    def _():
        relay_opp(last, (0, 1))

    @pl.when(s == 0)
    def _():
        halo[2] = jnp.zeros(halo.shape[1:], bf16)

    @pl.when(s > 0)
    def _():
        tail_copy(2, 2, 2, partner).wait_recv()
    convolve(1, 0, 2)
    settle(SECOND[2], FAR)
    project(1, OUTER, (FAR,), False)
    gat[1, t] = gate(0)
    gather_gat[1].start_all()

    @pl.when(is_end)
    def _():
        relay_opp(last, (0, 1))
    relay_opp(last, (2, 3))
    gather_gat[1].forward(0)
    gather_gat[1].forward(1)
    relay_far(last, (0,))
    gather_gat[1].beside()
    gather_gat[1].across()
    relay_far(last, (1,))
    local_w(last).wait()
    for role in (OWN, NEAR, OPP):
        settle(last, role)

    def start_last(cols):
        bacc[:, cols] = x1[t, :, cols].astype(f32) + back_dot(1, (OWN, NEAR, OPP), cols)

    by_columns(start_last)
    relay_far(last, (2, 3))
    settle(last, FAR)

    def finish_last(cols):
        out[:, cols] = (bacc[:, cols] + back_dot(1, (FAR,), cols)).astype(bf16)

    by_columns(finish_last)

    some = units - 3

    @pl.when(is_mid)
    def _():
        for kind in (0, 1, 2, 3, 4, 6):
            sent(kind, units)
        for kind in (5, 7, 8):
            sent(kind, some)
        gather_tok.drain()
        for h in range(2):
            end_part(h).wait_send()

        @pl.when(core == 0)
        def _():
            for b in range(2):
                tail_copy(b, b, b, partner).wait_send()

        @pl.when(jnp.logical_and(core == 1, left))
        def _():
            tail_copy(0, 1, 1, partner).wait_send()
            tail_copy(1, 1, 1, s + 1).wait_send()

        @pl.when(jnp.logical_and(core == 1, jnp.logical_not(left)))
        def _():
            tail_copy(1, 0, 0, partner).wait_send()

    @pl.when(is_end)
    def _():
        for kind in (0, 1, 2, 3):
            sent(kind, some)
        sent(5, units)
        for h in range(2):
            tok_part(h).wait_send()
    gather_gat[0].drain()
    gather_x.drain()
    gather_gat[1].drain()

    @pl.when(s < n_sp - 1)
    def _():
        tail_copy(2, 2, 2, partner).wait_send()


def fused(tokens, norm_gain, w_outer, w_inner, w_value, w_back, taps):
    n_sp, n_tp = lax.axis_size("sp"), lax.axis_size("tp")
    rows, width = tokens.shape
    layers, depth, chans = w_outer.shape
    back_rows, feats = w_back.shape[1:]
    if 4 * layers != len(PIECES):
        return per_device(tokens, norm_gain, w_outer, w_inner, w_value, w_back, taps)
    chunks = sum(PIECES)
    dma = pltpu.SemaphoreType.DMA
    hbm, vmem = pl.BlockSpec(memory_space=pl.ANY), pl.BlockSpec(memory_space=pltpu.VMEM)
    return pl.pallas_call(
        mixer_kernel,
        out_shape=jax.ShapeDtypeStruct((rows, feats), bf16),
        in_specs=[hbm, vmem, hbm, hbm, hbm, hbm, vmem],
        out_specs=vmem,
        scratch_shapes=[
            pltpu.VMEM((2, n_tp, rows, feats), bf16),
            pltpu.VMEM((n_tp, rows, feats), bf16),
            pltpu.VMEM((2, n_tp, rows, feats), bf16),
            pltpu.VMEM((3 * layers, n_sp, depth, chans), bf16),
            pltpu.VMEM((layers, n_sp, back_rows, feats), bf16),
            pltpu.VMEM((3, 2, rows, chans), f32),
            pltpu.VMEM((rows, feats), f32),
            pltpu.VMEM((2, rows, 128), f32),
            pltpu.VMEM((layers, n_tp, rows, chans), bf16),
            pltpu.VMEM((rows, chans), bf16),
            pltpu.VMEM((3, rows, chans), bf16),
            pltpu.VMEM((3, 16, chans), bf16),
            dma((4 * layers,)),
            dma((n_tp,)),
            dma((2,)),
            dma((2,)),
            dma((KINDS,)),
            dma((chunks, 3)),
            dma((4 * layers, 4)),
            dma((4,)),
            dma((4, 4)),
            dma((3,)),
            dma((3,)),
            dma((2,)),
            dma((2,)),
        ],
        compiler_params=pltpu.CompilerParams(
            collective_id=0, has_side_effects=True, vmem_limit_bytes=60 * 1024 * 1024
        ),
        name="mixer",
    )(tokens, norm_gain, w_outer, w_inner, w_value, w_back, taps.transpose(1, 0, 2))


def solution(mesh):
    in_specs = (
        P("sp", None),
        P(),
        P(None, "sp", "tp"),
        P(None, "sp", "tp"),
        P(None, "sp", "tp"),
        P(None, "sp", "tp"),
        P(None, None, "tp"),
    )
    out_specs = P("sp", "tp")
    body = fused if (mesh.shape["sp"], mesh.shape["tp"]) == (8, 4) else per_device
    return jax.shard_map(
        body, mesh=mesh, in_specs=in_specs, out_specs=out_specs, check_vma=False
    )
```

```python
import functools

import jax
import jax.numpy as jnp
from jax import lax
from jax.experimental import pallas as pl
from jax.experimental.pallas import tpu as pltpu
from jax.sharding import PartitionSpec as P

MESH = pl.DeviceIdType.MESH
f32 = jnp.float32
bf16 = jnp.bfloat16

eps = 1e-06

OUTER, INNER, VALUE, BACK = 0, 1, 2, 3
FIRST = (INNER, VALUE, OUTER, BACK)
SECOND = tuple(4 + m for m in FIRST)
PIECES = (1, 1, 1, 2, 4, 2, 2, 4)
KINDS = 9


def shifted(block, axis, distance):
    devices = range(lax.axis_size(axis))
    route = [(i - distance, i) for i in devices if i - distance in devices]
    return lax.ppermute(block, axis, route)


def per_device(tokens, norm_gain, w_outer, w_inner, w_value, w_back, taps):
    layers = w_outer.shape[0]
    count = tokens.shape[0]
    feats = w_back.shape[2]
    own = lax.axis_index("tp")
    held = (
        lax.all_gather(w_outer, "sp", axis=1, tiled=True),
        lax.all_gather(w_inner, "sp", axis=1, tiled=True),
        lax.all_gather(w_value, "sp", axis=1, tiled=True),
        lax.all_gather(w_back, "sp", axis=1, tiled=True),
    )
    current = tokens
    resid = lax.dynamic_slice_in_dim(tokens, own * feats, feats, 1)
    for layer in range(layers):
        if layer > 0:
            current = lax.all_gather(resid, "tp", axis=1, tiled=True)
        xf = current.astype(jnp.float32)
        normed = (
            xf * lax.rsqrt(jnp.mean(xf * xf, axis=-1, keepdims=True) + eps) * norm_gain[layer]
        ).astype(jnp.bfloat16)
        outer = jnp.dot(normed, held[0][layer], preferred_element_type=jnp.float32)
        inner = jnp.dot(normed, held[1][layer], preferred_element_type=jnp.float32)
        value = jnp.dot(normed, held[2][layer], preferred_element_type=jnp.float32)
        outer = outer.astype(jnp.bfloat16)
        inner = inner.astype(jnp.bfloat16)
        value = value.astype(jnp.bfloat16)
        mixed = (inner.astype(jnp.float32) * value.astype(jnp.float32)).astype(jnp.bfloat16)
        before = shifted(mixed[count - 2 :], "sp", 1)
        padded = jnp.concatenate([before, mixed], axis=0).astype(jnp.float32)
        conv = (
            taps[layer, 0] * padded[:count]
            + taps[layer, 1] * padded[1 : count + 1]
            + taps[layer, 2] * padded[2:]
        )
        gated = (outer.astype(jnp.float32) * conv).astype(jnp.bfloat16)
        whole = lax.all_gather(gated, "tp", axis=1, tiled=True)
        proj = jnp.dot(whole, held[3][layer], preferred_element_type=jnp.float32)
        resid = (resid.astype(jnp.float32) + proj).astype(jnp.bfloat16)
    return resid


def first_chunk(u):
    return sum(PIECES[:u])


def mixer_kernel(
    tok, gain, w_outer, w_inner, w_value, w_back, taps, out,
    xr, x1, scl, win, wback, acc, bacc, ss, gat, gat_end, mixed, halo,
    sem_local, sem_tok, tok_send, tok_recv, w_send, w_recv, p_recv,
    g_send, g_recv, h_send, h_recv, e_send, e_recv,
):
    s, t = lax.axis_index("sp"), lax.axis_index("tp")
    n_sp, n_tp = win.shape[1], xr.shape[1]
    rows, feats = xr.shape[2:]
    half = rows // 2
    width = feats * n_tp
    units = len(PIECES)
    core = lax.rem(s, 2)
    flip = 1 - 2 * core
    left = s < n_sp // 2
    side = jnp.where(left, 1, -1)
    plane = lax.div(s, 2)
    planes = n_sp // 2
    is_end = jnp.logical_or(plane == 0, plane == planes - 1)
    is_mid = jnp.logical_not(is_end)
    partner = s + flip
    near = jnp.where(is_mid, s - 2 * side, s + 2 * side)
    opp = jnp.where(is_mid, s + 2 * side, s + 4 * side)
    far = jnp.where(is_mid, s + 4 * side, s + 6 * side)
    tx = t + 1 - 2 * lax.rem(t, 2)
    ty = t + 2 - 4 * lax.div(t, 2)
    td = n_tp - 1 - t

    barrier = pltpu.get_barrier_semaphore()

    def greet(sp, tp):
        pl.semaphore_signal(barrier, inc=1, device_id=(sp, tp), device_id_type=MESH)

    greet(partner, t)
    greet(s, tx)
    greet(s, ty)
    greet(near, t)
    greet(near + flip, t)

    @pl.when(is_mid)
    def _():
        greet(opp, t)
        greet(opp + flip, t)
    pl.semaphore_wait(barrier, jnp.where(is_mid, 7, 5))

    projections = (w_outer, w_inner, w_value)

    def own_w(u):
        layer, m = u // 4, u % 4
        return projections[m].at[layer] if m < 3 else w_back.at[layer]

    def held_w(u, source):
        layer, m = u // 4, u % 4
        return win.at[3 * layer + m, source] if m < 3 else wback.at[layer, source]

    def remote(a, b, ssem, rsem, sp, tp):
        return pltpu.make_async_remote_copy(
            src_ref=a, dst_ref=b, send_sem=ssem, recv_sem=rsem, device_id=(sp, tp), device_id_type=MESH
        )

    def piece(ref, u, k):
        size = ref.shape[0] // PIECES[u]
        return ref.at[pl.ds(k * size, size)]

    OWN, NEAR, OPP, FAR = 0, 1, 2, 3
    source_of = (s, near, opp, far)

    def w_copy(u, k, role, kind, to_role, target):
        to = piece(held_w(u, source_of[role]), u, k)
        a = piece(own_w(u), u, k) if role == OWN else to
        return remote(a, to, w_send.at[kind], w_recv.at[first_chunk(u) + k, to_role - 1], target, t)

    def to_partner(u, k, role):
        to = piece(held_w(u, source_of[role]), u, k)
        a = piece(own_w(u), u, k) if role == OWN else to
        return remote(a, to, w_send.at[role], p_recv.at[u, role], partner, t)

    def pieces_of(u):
        return range(PIECES[u])

    def arrived(u, k, role):
        to = piece(held_w(u, source_of[role]), u, k)
        remote(to, to, w_send.at[0], w_recv.at[first_chunk(u) + k, role - 1], partner, t).wait_recv()

    def send_opp(u):
        for k in pieces_of(u):
            w_copy(u, k, OWN, 4, OPP, opp).start()

    def send_near(u):
        for k in pieces_of(u):
            w_copy(u, k, OWN, 5, NEAR, near).start()

    def send_partner(u):
        for k in pieces_of(u):
            to_partner(u, k, OWN).start()

    def relay_near(u, ks=None):
        for k in ks or pieces_of(u):
            arrived(u, k, NEAR)

            @pl.when(is_mid)
            def _():
                w_copy(u, k, NEAR, 6, FAR, opp).start()
            to_partner(u, k, NEAR).start()

    def relay_across(u, role, ks=None):
        for k in ks or pieces_of(u):
            arrived(u, k, role)
            if u >= 3:
                @pl.when(is_mid)
                def _():
                    w_copy(u, k, role, 5 + role, role, near).start()
            to_partner(u, k, role).start()

    def relay_opp(u, ks=None):
        relay_across(u, OPP, ks)

    def relay_far(u, ks=None):
        relay_across(u, FAR, ks)

    def settle(u, role):
        to = held_w(u, source_of[role] + flip)
        remote(to, to, w_send.at[0], p_recv.at[u, role], partner, t).wait_recv()

    def sent(kind, count):
        ref = win.at[0, pl.ds(0, count)]
        remote(ref, ref, w_send.at[kind], p_recv.at[0, 0], partner, t).wait_send()

    def local_w(u):
        return pltpu.make_async_copy(own_w(u), held_w(u, s), sem_local.at[u])

    def tok_cols(j):
        return tok.at[:, pl.ds(pl.multiple_of(j * feats, feats), feats)]

    def tok_local(j):
        return pltpu.make_async_copy(tok_cols(j), xr.at[1, j], sem_tok.at[j])

    def tok_part(h):
        cols = pl.ds(pl.multiple_of(t * feats, feats), feats)
        return remote(
            tok.at[pl.ds(h * half, half), cols], xr.at[0, t, pl.ds(h * half, half)],
            tok_send.at[h], tok_recv.at[h], near, t,
        )

    def end_part(h):
        return remote(
            gat_end.at[pl.ds(h * half, half)], gat.at[0, t, pl.ds(h * half, half)],
            e_send.at[h], e_recv.at[h], near, t,
        )

    class Gather:
        def __init__(self, g, buf):
            self.g, self.buf = g, buf

        def part(self, block, h, k, target):
            size = self.buf.shape[1] // 2
            ref = self.buf.at[block, pl.ds(h * size, size)]
            slot = (0, 1, 2, 2, 3, 3)[k]
            return remote(ref, ref, g_send.at[self.g], g_recv.at[self.g, slot], s, target)

        def whole(self, blocks, slot):
            ref = self.buf.at[pl.ds(0, blocks)]
            return remote(ref, ref, g_send.at[self.g], g_recv.at[self.g, slot], s, tx)

        def start(self, h):
            if h == 0:
                self.part(t, 0, 0, tx).start()
                self.part(t, 0, 3, ty).start()
            else:
                self.part(t, 1, 1, ty).start()
                self.part(t, 1, 2, tx).start()

        def start_all(self):
            self.part(t, 0, 0, tx).start()
            self.part(t, 1, 1, ty).start()
            self.part(t, 1, 2, tx).start()
            self.part(t, 0, 3, ty).start()

        def forward(self, h):
            if h == 0:
                self.part(tx, 0, 0, tx).wait_recv()
                self.part(tx, 0, 4, ty).start()
            else:
                self.part(ty, 1, 1, ty).wait_recv()
                self.part(ty, 1, 5, tx).start()

        def beside(self):
            self.whole(1, 2).wait_recv()

        def across(self):
            self.whole(1, 3).wait_recv()

        def drain(self):
            self.whole(3, 0).wait_send()

    gather_tok = Gather(0, xr.at[0])
    gather_gat = (Gather(1, gat.at[0]), Gather(3, gat.at[1]))
    gather_x = Gather(2, x1)

    def scale(layer, source, b, j):
        step = 64

        def tile(r, carry):
            span = pl.ds(pl.multiple_of(r * step, step), step)
            x = source[j, span, :].astype(f32)
            sq = x * x
            part = sq[:, :128]
            for q in range(1, feats // 128):
                part = part + sq[:, 128 * q : 128 * (q + 1)]
            ss[b, span, :] += part
            cols = pl.ds(pl.multiple_of(j * feats, feats), feats)
            scl[b, j, span, :] = (x * gain[layer : layer + 1, cols]).astype(bf16)
            return carry

        lax.fori_loop(0, rows // step, tile, 0)

    def project(layer, m, sources, first):
        blocks = (0, 1) if layer == 0 else (0,)
        depth = win.shape[2]

        def tile(b, carry):
            total = None
            for role in sources:
                z = lax.div(source_of[role], 2)
                w = win[3 * layer + m, pl.ds(2 * z, 2)].reshape(2 * depth, win.shape[3])
                dot = jnp.dot(scl[b, z], w, preferred_element_type=f32)
                total = dot if total is None else total + dot
            if first:
                acc[m, b] = total
            else:
                acc[m, b] += total
            return carry

        if len(blocks) == 1:
            tile(0, 0)
        else:
            lax.fori_loop(0, len(blocks), tile, 0)

    def inv_of(b):
        return lax.rsqrt(jnp.sum(ss[b], axis=-1, keepdims=True) / width + eps)

    def mix(b, slot):
        inv = inv_of(b)
        inner = (acc[INNER, b] * inv).astype(bf16)
        value = (acc[VALUE, b] * inv).astype(bf16)
        mixed[slot] = (inner.astype(f32) * value.astype(f32)).astype(bf16)

    def convolve(layer, b, slot):
        now = mixed[slot].astype(f32)
        tail = halo[slot].astype(f32)
        row = lax.broadcasted_iota(jnp.int32, now.shape, 0)
        one = jnp.where(row == 0, tail[15:16], pltpu.roll(now, 1, 0))
        two = pltpu.roll(now, 2, 0)
        two = jnp.where(row == 0, tail[14:15], jnp.where(row == 1, tail[15:16], two))
        acc[VALUE, b] = taps[0, layer : layer + 1] * two + taps[1, layer : layer + 1] * one + taps[2, layer : layer + 1] * now

    def gate(b):
        outer = (acc[OUTER, b] * inv_of(b)).astype(bf16).astype(f32)
        return (outer * acc[VALUE, b]).astype(bf16)

    def tail_copy(slot, to_slot, h, target):
        return remote(
            mixed.at[slot, pl.ds(rows - 16, 16)], halo.at[to_slot], h_send.at[slot], h_recv.at[h], target, t
        )

    def back_dot(layer, sources, cols):
        total = None
        for role in sources:
            z = lax.div(source_of[role], 2)
            w = wback[layer, pl.ds(2 * z, 2), :, cols].reshape(2 * wback.shape[2], cols.size)
            dot = jnp.dot(gat[layer, z], w, preferred_element_type=f32)
            total = dot if total is None else total + dot
        return total

    def by_columns(body):
        step = 256

        def tile(c, carry):
            body(pl.ds(pl.multiple_of(c * step, step), step))
            return carry

        lax.fori_loop(0, feats // step, tile, 0)

    @pl.when(is_mid)
    def _():
        for u in FIRST[:3]:
            send_opp(u)
        for u in FIRST + SECOND:
            send_partner(u)
        for u in FIRST[3:] + SECOND:
            send_near(u)
        for j in range(n_tp):
            tok_local(j).start()
        for u in FIRST + SECOND:
            local_w(u).start()
        ss[...] = jnp.zeros(ss.shape, f32)
        for j in range(n_tp):
            tok_local(j).wait()

        def scale_own(j, carry):
            scale(0, xr.at[1], 1, j)
            return carry

        lax.fori_loop(0, n_tp, scale_own, 0)
        relay_near(INNER)
        send_opp(BACK)
        relay_opp(INNER)
        for h in range(2):
            tok_part(h).wait_recv()
            gather_tok.start(h)
            relay_opp((VALUE, OUTER)[h])
        gather_tok.forward(0)
        relay_near(VALUE)
        relay_far(INNER)
        scale(0, xr.at[0], 0, t)
        gather_tok.forward(1)
        relay_near(OUTER)
        relay_opp(BACK)
        gather_tok.beside()
        scale(0, xr.at[0], 0, tx)
        scale(0, xr.at[0], 0, ty)
        gather_tok.across()
        scale(0, xr.at[0], 0, td)
        for u in FIRST[:3]:
            local_w(u).wait()
            for role in (OWN, NEAR, OPP):
                settle(u, role)
        settle(INNER, FAR)
        project(0, INNER, (OWN, NEAR, OPP, FAR), True)
        project(0, VALUE, (OWN, NEAR, OPP), True)
        relay_far(VALUE)
        settle(VALUE, FAR)
        project(0, VALUE, (FAR,), False)
        for b in range(2):
            mix(b, b)

        @pl.when(core == 0)
        def _():
            for b in range(2):
                tail_copy(b, b, b, partner).start()

        @pl.when(jnp.logical_and(core == 1, left))
        def _():
            tail_copy(1, 1, 1, s + 1).start()
            tail_copy(0, 1, 1, partner).start()

        @pl.when(jnp.logical_and(core == 1, jnp.logical_not(left)))
        def _():
            tail_copy(1, 0, 0, partner).start()
        relay_near(BACK)
        for u in SECOND[:3]:
            send_opp(u)
        project(0, OUTER, (OWN, NEAR, OPP), True)
        relay_far(OUTER)
        for b in range(2):
            if b == 0:
                start_of_all = s == 2

                @pl.when(start_of_all)
                def _():
                    halo[0] = jnp.zeros(halo.shape[1:], bf16)

                @pl.when(jnp.logical_not(start_of_all))
                def _():
                    tail_copy(0, 0, 0, partner).wait_recv()
            else:
                tail_copy(1, 1, 1, partner).wait_recv()
            convolve(0, b, b)
        settle(OUTER, FAR)
        project(0, OUTER, (FAR,), False)
        gat_end[...] = gate(0)
        for h in range(2):
            end_part(h).start()
        gat[0, t] = gate(1)
        gather_gat[0].start_all()
        relay_near(SECOND[0])
        gather_gat[0].forward(0)
        gather_gat[0].forward(1)
        relay_far(BACK)

    @pl.when(is_end)
    def _():
        send_near(INNER)
        for h in range(2):
            tok_part(h).start()
        for u in FIRST[1:] + SECOND:
            send_near(u)
        for u in FIRST[3:] + SECOND:
            send_partner(u)
        tok_local(t).start()
        for u in FIRST[3:] + SECOND:
            local_w(u).start()
        tok_local(t).wait()
        for u in FIRST[3:] + SECOND:
            relay_near(u)
        relay_opp(BACK)
        for h in range(2):
            end_part(h).wait_recv()
            gather_gat[0].start(h)
        relay_far(BACK, (0,))
        gather_gat[0].forward(0)
        gather_gat[0].forward(1)
        relay_far(BACK, (1,))

    gather_gat[0].beside()
    gather_gat[0].across()
    local_w(BACK).wait()
    for role in (OWN, NEAR, OPP, FAR):
        settle(BACK, role)

    def finish_first(cols):
        total = xr[1, t, :, cols].astype(f32) + back_dot(0, (OWN, NEAR, OPP, FAR), cols)
        x1[t, :, cols] = total.astype(bf16)

    by_columns(finish_first)
    gather_x.start_all()

    @pl.when(is_mid)
    def _():
        relay_near(SECOND[1])
    relay_opp(SECOND[0])

    @pl.when(is_mid)
    def _():
        relay_near(SECOND[2])
    ss[0] = jnp.zeros(ss.shape[1:], f32)
    scale(1, x1, 0, t)
    relay_opp(SECOND[1])
    gather_x.forward(0)
    gather_x.forward(1)
    relay_opp(SECOND[2])
    gather_x.beside()
    scale(1, x1, 0, tx)
    scale(1, x1, 0, ty)
    relay_far(SECOND[0])
    gather_x.across()
    scale(1, x1, 0, td)
    for u in SECOND[:3]:
        local_w(u).wait()
        for role in (OWN, NEAR, OPP):
            settle(u, role)
    for u in SECOND[:3]:
        project(1, u % 4, (OWN, NEAR, OPP), True)
    settle(SECOND[0], FAR)
    project(1, INNER, (FAR,), False)
    relay_far(SECOND[1])
    settle(SECOND[1], FAR)
    project(1, VALUE, (FAR,), False)
    mix(0, 2)

    @pl.when(s < n_sp - 1)
    def _():
        tail_copy(2, 2, 2, s + 1).start()
    last = SECOND[3]

    @pl.when(is_mid)
    def _():
        send_opp(last)
        relay_near(last)
    relay_far(SECOND[2])

    @pl.when(is_mid)
    def _():
        relay_opp(last)

    @pl.when(s == 0)
    def _():
        halo[2] = jnp.zeros(halo.shape[1:], bf16)

    @pl.when(s > 0)
    def _():
        tail_copy(2, 2, 2, partner).wait_recv()
    convolve(1, 0, 2)
    settle(SECOND[2], FAR)
    project(1, OUTER, (FAR,), False)
    gat[1, t] = gate(0)
    gather_gat[1].start_all()

    @pl.when(is_end)
    def _():
        relay_opp(last)

    @pl.when(is_mid)
    def _():
        relay_far(last, (0, 1))
    gather_gat[1].forward(0)
    gather_gat[1].forward(1)

    @pl.when(is_mid)
    def _():
        relay_far(last, (2, 3))
    gather_gat[1].beside()
    gather_gat[1].across()
    local_w(last).wait()
    for role in (OWN, NEAR, OPP):
        settle(last, role)

    def start_last(cols):
        bacc[:, cols] = x1[t, :, cols].astype(f32) + back_dot(1, (OWN, NEAR, OPP), cols)

    by_columns(start_last)

    @pl.when(is_end)
    def _():
        relay_far(last)
    settle(last, FAR)

    def finish_last(cols):
        out[:, cols] = (bacc[:, cols] + back_dot(1, (FAR,), cols)).astype(bf16)

    by_columns(finish_last)

    some = units - 3

    @pl.when(is_mid)
    def _():
        for kind in (0, 1, 2, 3, 4, 6):
            sent(kind, units)
        for kind in (5, 7, 8):
            sent(kind, some)
        gather_tok.drain()
        for h in range(2):
            end_part(h).wait_send()

        @pl.when(core == 0)
        def _():
            for b in range(2):
                tail_copy(b, b, b, partner).wait_send()

        @pl.when(jnp.logical_and(core == 1, left))
        def _():
            tail_copy(0, 1, 1, partner).wait_send()
            tail_copy(1, 1, 1, s + 1).wait_send()

        @pl.when(jnp.logical_and(core == 1, jnp.logical_not(left)))
        def _():
            tail_copy(1, 0, 0, partner).wait_send()

    @pl.when(is_end)
    def _():
        for kind in (0, 1, 2, 3):
            sent(kind, some)
        sent(5, units)
        for h in range(2):
            tok_part(h).wait_send()
    gather_gat[0].drain()
    gather_x.drain()
    gather_gat[1].drain()

    @pl.when(s < n_sp - 1)
    def _():
        tail_copy(2, 2, 2, partner).wait_send()


def fused(tokens, norm_gain, w_outer, w_inner, w_value, w_back, taps):
    n_sp, n_tp = lax.axis_size("sp"), lax.axis_size("tp")
    rows, width = tokens.shape
    layers, depth, chans = w_outer.shape
    back_rows, feats = w_back.shape[1:]
    if 4 * layers != len(PIECES):
        return per_device(tokens, norm_gain, w_outer, w_inner, w_value, w_back, taps)
    chunks = sum(PIECES)
    dma = pltpu.SemaphoreType.DMA
    hbm, vmem = pl.BlockSpec(memory_space=pl.ANY), pl.BlockSpec(memory_space=pltpu.VMEM)
    return pl.pallas_call(
        mixer_kernel,
        out_shape=jax.ShapeDtypeStruct((rows, feats), bf16),
        in_specs=[hbm, vmem, hbm, hbm, hbm, hbm, vmem],
        out_specs=vmem,
        scratch_shapes=[
            pltpu.VMEM((2, n_tp, rows, feats), bf16),
            pltpu.VMEM((n_tp, rows, feats), bf16),
            pltpu.VMEM((2, n_tp, rows, feats), bf16),
            pltpu.VMEM((3 * layers, n_sp, depth, chans), bf16),
            pltpu.VMEM((layers, n_sp, back_rows, feats), bf16),
            pltpu.VMEM((3, 2, rows, chans), f32),
            pltpu.VMEM((rows, feats), f32),
            pltpu.VMEM((2, rows, 128), f32),
            pltpu.VMEM((layers, n_tp, rows, chans), bf16),
            pltpu.VMEM((rows, chans), bf16),
            pltpu.VMEM((3, rows, chans), bf16),
            pltpu.VMEM((3, 16, chans), bf16),
            dma((4 * layers,)),
            dma((n_tp,)),
            dma((2,)),
            dma((2,)),
            dma((KINDS,)),
            dma((chunks, 3)),
            dma((4 * layers, 4)),
            dma((4,)),
            dma((4, 4)),
            dma((3,)),
            dma((3,)),
            dma((2,)),
            dma((2,)),
        ],
        compiler_params=pltpu.CompilerParams(
            collective_id=0, has_side_effects=True, vmem_limit_bytes=60 * 1024 * 1024
        ),
        name="mixer",
    )(tokens, norm_gain, w_outer, w_inner, w_value, w_back, taps.transpose(1, 0, 2))


def solution(mesh):
    in_specs = (
        P("sp", None),
        P(),
        P(None, "sp", "tp"),
        P(None, "sp", "tp"),
        P(None, "sp", "tp"),
        P(None, "sp", "tp"),
        P(None, None, "tp"),
    )
    out_specs = P("sp", "tp")
    body = fused if (mesh.shape["sp"], mesh.shape["tp"]) == (8, 4) else per_device
    return jax.shard_map(
        body, mesh=mesh, in_specs=in_specs, out_specs=out_specs, check_vma=False
    )
```

```python
import functools

import jax
import jax.numpy as jnp
from jax import lax
from jax.experimental import pallas as pl
from jax.experimental.pallas import tpu as pltpu
from jax.sharding import PartitionSpec as P

MESH = pl.DeviceIdType.MESH
f32 = jnp.float32
bf16 = jnp.bfloat16

eps = 1e-06

OUTER, INNER, VALUE, BACK = 0, 1, 2, 3
FIRST = (INNER, VALUE, OUTER, BACK)
SECOND = tuple(4 + m for m in FIRST)
PIECES = (1, 1, 1, 2, 4, 2, 2, 4)
KINDS = 9


def shifted(block, axis, distance):
    devices = range(lax.axis_size(axis))
    route = [(i - distance, i) for i in devices if i - distance in devices]
    return lax.ppermute(block, axis, route)


def per_device(tokens, norm_gain, w_outer, w_inner, w_value, w_back, taps):
    layers = w_outer.shape[0]
    count = tokens.shape[0]
    feats = w_back.shape[2]
    own = lax.axis_index("tp")
    held = (
        lax.all_gather(w_outer, "sp", axis=1, tiled=True),
        lax.all_gather(w_inner, "sp", axis=1, tiled=True),
        lax.all_gather(w_value, "sp", axis=1, tiled=True),
        lax.all_gather(w_back, "sp", axis=1, tiled=True),
    )
    current = tokens
    resid = lax.dynamic_slice_in_dim(tokens, own * feats, feats, 1)
    for layer in range(layers):
        if layer > 0:
            current = lax.all_gather(resid, "tp", axis=1, tiled=True)
        xf = current.astype(jnp.float32)
        normed = (
            xf * lax.rsqrt(jnp.mean(xf * xf, axis=-1, keepdims=True) + eps) * norm_gain[layer]
        ).astype(jnp.bfloat16)
        outer = jnp.dot(normed, held[0][layer], preferred_element_type=jnp.float32)
        inner = jnp.dot(normed, held[1][layer], preferred_element_type=jnp.float32)
        value = jnp.dot(normed, held[2][layer], preferred_element_type=jnp.float32)
        outer = outer.astype(jnp.bfloat16)
        inner = inner.astype(jnp.bfloat16)
        value = value.astype(jnp.bfloat16)
        mixed = (inner.astype(jnp.float32) * value.astype(jnp.float32)).astype(jnp.bfloat16)
        before = shifted(mixed[count - 2 :], "sp", 1)
        padded = jnp.concatenate([before, mixed], axis=0).astype(jnp.float32)
        conv = (
            taps[layer, 0] * padded[:count]
            + taps[layer, 1] * padded[1 : count + 1]
            + taps[layer, 2] * padded[2:]
        )
        gated = (outer.astype(jnp.float32) * conv).astype(jnp.bfloat16)
        whole = lax.all_gather(gated, "tp", axis=1, tiled=True)
        proj = jnp.dot(whole, held[3][layer], preferred_element_type=jnp.float32)
        resid = (resid.astype(jnp.float32) + proj).astype(jnp.bfloat16)
    return resid


def first_chunk(u):
    return sum(PIECES[:u])


def mixer_kernel(
    tok, gain_hbm, w_outer, w_inner, w_value, w_back, taps_hbm, out,
    gain, taps, xr, x1, scl, win, wback, acc, bacc, ss, gat, gat_end, mixed, halo,
    sem_small, sem_local, sem_tok, tok_send, tok_recv, w_send, w_recv, p_recv,
    g_send, g_recv, h_send, h_recv, e_send, e_recv,
):
    s, t = lax.axis_index("sp"), lax.axis_index("tp")
    n_sp, n_tp = win.shape[1], xr.shape[1]
    rows, feats = xr.shape[2:]
    half = rows // 2
    width = feats * n_tp
    units = len(PIECES)
    core = lax.rem(s, 2)
    flip = 1 - 2 * core
    left = s < n_sp // 2
    side = jnp.where(left, 1, -1)
    plane = lax.div(s, 2)
    planes = n_sp // 2
    is_end = jnp.logical_or(plane == 0, plane == planes - 1)
    is_mid = jnp.logical_not(is_end)
    partner = s + flip
    near = jnp.where(is_mid, s - 2 * side, s + 2 * side)
    opp = jnp.where(is_mid, s + 2 * side, s + 4 * side)
    far = jnp.where(is_mid, s + 4 * side, s + 6 * side)
    tx = t + 1 - 2 * lax.rem(t, 2)
    ty = t + 2 - 4 * lax.div(t, 2)
    td = n_tp - 1 - t

    small = (
        pltpu.make_async_copy(gain_hbm, gain, sem_small.at[0]),
        pltpu.make_async_copy(taps_hbm, taps, sem_small.at[1]),
    )
    for copy in small:
        copy.start()
    barrier = pltpu.get_barrier_semaphore()

    def greet(sp, tp):
        pl.semaphore_signal(barrier, inc=1, device_id=(sp, tp), device_id_type=MESH)

    greet(partner, t)
    greet(s, tx)
    greet(s, ty)
    greet(near, t)
    greet(near + flip, t)

    @pl.when(is_mid)
    def _():
        greet(opp, t)
        greet(opp + flip, t)
    pl.semaphore_wait(barrier, jnp.where(is_mid, 7, 5))
    for copy in small:
        copy.wait()

    projections = (w_outer, w_inner, w_value)

    def own_w(u):
        layer, m = u // 4, u % 4
        return projections[m].at[layer] if m < 3 else w_back.at[layer]

    def held_w(u, source):
        layer, m = u // 4, u % 4
        return win.at[3 * layer + m, source] if m < 3 else wback.at[layer, source]

    def remote(a, b, ssem, rsem, sp, tp):
        return pltpu.make_async_remote_copy(
            src_ref=a, dst_ref=b, send_sem=ssem, recv_sem=rsem, device_id=(sp, tp), device_id_type=MESH
        )

    def piece(ref, u, k):
        size = ref.shape[0] // PIECES[u]
        return ref.at[pl.ds(k * size, size)]

    OWN, NEAR, OPP, FAR = 0, 1, 2, 3
    source_of = (s, near, opp, far)

    def w_copy(u, k, role, kind, to_role, target):
        to = piece(held_w(u, source_of[role]), u, k)
        a = piece(own_w(u), u, k) if role == OWN else to
        return remote(a, to, w_send.at[kind], w_recv.at[first_chunk(u) + k, to_role - 1], target, t)

    def to_partner(u, k, role):
        to = piece(held_w(u, source_of[role]), u, k)
        a = piece(own_w(u), u, k) if role == OWN else to
        return remote(a, to, w_send.at[role], p_recv.at[u, role], partner, t)

    def pieces_of(u):
        return range(PIECES[u])

    def arrived(u, k, role):
        to = piece(held_w(u, source_of[role]), u, k)
        remote(to, to, w_send.at[0], w_recv.at[first_chunk(u) + k, role - 1], partner, t).wait_recv()

    def send_opp(u):
        for k in pieces_of(u):
            w_copy(u, k, OWN, 4, OPP, opp).start()

    def send_near(u):
        for k in pieces_of(u):
            w_copy(u, k, OWN, 5, NEAR, near).start()

    def send_partner(u):
        for k in pieces_of(u):
            to_partner(u, k, OWN).start()

    def relay_near(u, ks=None):
        for k in ks or pieces_of(u):
            arrived(u, k, NEAR)

            @pl.when(is_mid)
            def _():
                w_copy(u, k, NEAR, 6, FAR, opp).start()
            to_partner(u, k, NEAR).start()

    def relay_across(u, role, ks=None):
        for k in ks or pieces_of(u):
            arrived(u, k, role)
            if u >= 3:
                @pl.when(is_mid)
                def _():
                    w_copy(u, k, role, 5 + role, role, near).start()
            to_partner(u, k, role).start()

    def relay_opp(u, ks=None):
        relay_across(u, OPP, ks)

    def relay_far(u, ks=None):
        relay_across(u, FAR, ks)

    def settle(u, role):
        to = held_w(u, source_of[role] + flip)
        remote(to, to, w_send.at[0], p_recv.at[u, role], partner, t).wait_recv()

    def sent(kind, count):
        ref = win.at[0, pl.ds(0, count)]
        remote(ref, ref, w_send.at[kind], p_recv.at[0, 0], partner, t).wait_send()

    def local_w(u):
        return pltpu.make_async_copy(own_w(u), held_w(u, s), sem_local.at[u])

    def tok_cols(j):
        return tok.at[:, pl.ds(pl.multiple_of(j * feats, feats), feats)]

    def tok_local(j):
        return pltpu.make_async_copy(tok_cols(j), xr.at[1, j], sem_tok.at[j])

    def tok_part(h):
        cols = pl.ds(pl.multiple_of(t * feats, feats), feats)
        return remote(
            tok.at[pl.ds(h * half, half), cols], xr.at[0, t, pl.ds(h * half, half)],
            tok_send.at[h], tok_recv.at[h], near, t,
        )

    def end_part(h):
        return remote(
            gat_end.at[pl.ds(h * half, half)], gat.at[0, t, pl.ds(h * half, half)],
            e_send.at[h], e_recv.at[h], near, t,
        )

    class Gather:
        def __init__(self, g, buf):
            self.g, self.buf = g, buf

        def part(self, block, h, k, target):
            size = self.buf.shape[1] // 2
            ref = self.buf.at[block, pl.ds(h * size, size)]
            slot = (0, 1, 2, 2, 3, 3)[k]
            return remote(ref, ref, g_send.at[self.g], g_recv.at[self.g, slot], s, target)

        def whole(self, blocks, slot):
            ref = self.buf.at[pl.ds(0, blocks)]
            return remote(ref, ref, g_send.at[self.g], g_recv.at[self.g, slot], s, tx)

        def start(self, h):
            if h == 0:
                self.part(t, 0, 0, tx).start()
                self.part(t, 0, 3, ty).start()
            else:
                self.part(t, 1, 1, ty).start()
                self.part(t, 1, 2, tx).start()

        def start_all(self):
            self.part(t, 0, 0, tx).start()
            self.part(t, 1, 1, ty).start()
            self.part(t, 1, 2, tx).start()
            self.part(t, 0, 3, ty).start()

        def forward(self, h):
            if h == 0:
                self.part(tx, 0, 0, tx).wait_recv()
                self.part(tx, 0, 4, ty).start()
            else:
                self.part(ty, 1, 1, ty).wait_recv()
                self.part(ty, 1, 5, tx).start()

        def beside(self):
            self.whole(1, 2).wait_recv()

        def across(self):
            self.whole(1, 3).wait_recv()

        def drain(self):
            self.whole(3, 0).wait_send()

    gather_tok = Gather(0, xr.at[0])
    gather_gat = (Gather(1, gat.at[0]), Gather(3, gat.at[1]))
    gather_x = Gather(2, x1)

    def scale(layer, source, b, j):
        step = 64

        def tile(r, carry):
            span = pl.ds(pl.multiple_of(r * step, step), step)
            x = source[j, span, :].astype(f32)
            sq = x * x
            part = sq[:, :128]
            for q in range(1, feats // 128):
                part = part + sq[:, 128 * q : 128 * (q + 1)]
            ss[b, span, :] += part
            cols = pl.ds(pl.multiple_of(j * feats, feats), feats)
            scl[b, j, span, :] = (x * gain[layer : layer + 1, cols]).astype(bf16)
            return carry

        lax.fori_loop(0, rows // step, tile, 0)

    def project(layer, m, sources, first):
        blocks = (0, 1) if layer == 0 else (0,)
        depth = win.shape[2]

        def tile(b, carry):
            total = None
            for role in sources:
                z = lax.div(source_of[role], 2)
                w = win[3 * layer + m, pl.ds(2 * z, 2)].reshape(2 * depth, win.shape[3])
                dot = jnp.dot(scl[b, z], w, preferred_element_type=f32)
                total = dot if total is None else total + dot
            if first:
                acc[m, b] = total
            else:
                acc[m, b] += total
            return carry

        if len(blocks) == 1:
            tile(0, 0)
        else:
            lax.fori_loop(0, len(blocks), tile, 0)

    def inv_of(b):
        return lax.rsqrt(jnp.sum(ss[b], axis=-1, keepdims=True) / width + eps)

    def mix(b, slot):
        inv = inv_of(b)
        inner = (acc[INNER, b] * inv).astype(bf16)
        value = (acc[VALUE, b] * inv).astype(bf16)
        mixed[slot] = (inner.astype(f32) * value.astype(f32)).astype(bf16)

    def convolve(layer, b, slot):
        now = mixed[slot].astype(f32)
        tail = halo[slot].astype(f32)
        row = lax.broadcasted_iota(jnp.int32, now.shape, 0)
        one = jnp.where(row == 0, tail[15:16], pltpu.roll(now, 1, 0))
        two = pltpu.roll(now, 2, 0)
        two = jnp.where(row == 0, tail[14:15], jnp.where(row == 1, tail[15:16], two))
        acc[VALUE, b] = taps[0, layer : layer + 1] * two + taps[1, layer : layer + 1] * one + taps[2, layer : layer + 1] * now

    def gate(b):
        outer = (acc[OUTER, b] * inv_of(b)).astype(bf16).astype(f32)
        return (outer * acc[VALUE, b]).astype(bf16)

    def tail_copy(slot, to_slot, h, target):
        return remote(
            mixed.at[slot, pl.ds(rows - 16, 16)], halo.at[to_slot], h_send.at[slot], h_recv.at[h], target, t
        )

    def back_dot(layer, sources, cols):
        total = None
        for role in sources:
            z = lax.div(source_of[role], 2)
            w = wback[layer, pl.ds(2 * z, 2), :, cols].reshape(2 * wback.shape[2], cols.size)
            dot = jnp.dot(gat[layer, z], w, preferred_element_type=f32)
            total = dot if total is None else total + dot
        return total

    def by_columns(body):
        step = 256

        def tile(c, carry):
            body(pl.ds(pl.multiple_of(c * step, step), step))
            return carry

        lax.fori_loop(0, feats // step, tile, 0)

    @pl.when(is_mid)
    def _():
        for u in FIRST[:3]:
            send_opp(u)
        for u in FIRST + SECOND:
            send_partner(u)
        for u in FIRST[3:] + SECOND:
            send_near(u)
        for j in range(n_tp):
            tok_local(j).start()
        for u in FIRST + SECOND:
            local_w(u).start()
        ss[...] = jnp.zeros(ss.shape, f32)
        for j in range(n_tp):
            tok_local(j).wait()

        def scale_own(j, carry):
            scale(0, xr.at[1], 1, j)
            return carry

        lax.fori_loop(0, n_tp, scale_own, 0)
        relay_near(INNER)
        send_opp(BACK)
        relay_opp(INNER)
        for h in range(2):
            tok_part(h).wait_recv()
            gather_tok.start(h)
            relay_opp((VALUE, OUTER)[h])
        gather_tok.forward(0)
        relay_near(VALUE)
        relay_far(INNER)
        scale(0, xr.at[0], 0, t)
        gather_tok.forward(1)
        relay_near(OUTER)
        relay_opp(BACK)
        gather_tok.beside()
        scale(0, xr.at[0], 0, tx)
        scale(0, xr.at[0], 0, ty)
        gather_tok.across()
        scale(0, xr.at[0], 0, td)
        for u in FIRST[:3]:
            local_w(u).wait()
            for role in (OWN, NEAR, OPP):
                settle(u, role)
        settle(INNER, FAR)
        project(0, INNER, (OWN, NEAR, OPP, FAR), True)
        project(0, VALUE, (OWN, NEAR, OPP), True)
        relay_far(VALUE)
        settle(VALUE, FAR)
        project(0, VALUE, (FAR,), False)
        for b in range(2):
            mix(b, b)

        @pl.when(core == 0)
        def _():
            for b in range(2):
                tail_copy(b, b, b, partner).start()

        @pl.when(jnp.logical_and(core == 1, left))
        def _():
            tail_copy(1, 1, 1, s + 1).start()
            tail_copy(0, 1, 1, partner).start()

        @pl.when(jnp.logical_and(core == 1, jnp.logical_not(left)))
        def _():
            tail_copy(1, 0, 0, partner).start()
        relay_near(BACK)
        for u in SECOND[:3]:
            send_opp(u)
        project(0, OUTER, (OWN, NEAR, OPP), True)
        relay_far(OUTER)
        for b in range(2):
            if b == 0:
                start_of_all = s == 2

                @pl.when(start_of_all)
                def _():
                    halo[0] = jnp.zeros(halo.shape[1:], bf16)

                @pl.when(jnp.logical_not(start_of_all))
                def _():
                    tail_copy(0, 0, 0, partner).wait_recv()
            else:
                tail_copy(1, 1, 1, partner).wait_recv()
            convolve(0, b, b)
        settle(OUTER, FAR)
        project(0, OUTER, (FAR,), False)
        gat_end[...] = gate(0)
        for h in range(2):
            end_part(h).start()
        gat[0, t] = gate(1)
        gather_gat[0].start_all()
        relay_near(SECOND[0])
        gather_gat[0].forward(0)
        gather_gat[0].forward(1)
        relay_far(BACK)

    @pl.when(is_end)
    def _():
        send_near(INNER)
        for h in range(2):
            tok_part(h).start()
        for u in FIRST[1:] + SECOND:
            send_near(u)
        for u in FIRST[3:] + SECOND:
            send_partner(u)
        tok_local(t).start()
        for u in FIRST[3:] + SECOND:
            local_w(u).start()
        tok_local(t).wait()
        for u in FIRST[3:] + SECOND:
            relay_near(u)
        relay_opp(BACK)
        for h in range(2):
            end_part(h).wait_recv()
            gather_gat[0].start(h)
        relay_far(BACK, (0,))
        gather_gat[0].forward(0)
        gather_gat[0].forward(1)
        relay_far(BACK, (1,))

    gather_gat[0].beside()
    gather_gat[0].across()
    local_w(BACK).wait()
    for role in (OWN, NEAR, OPP, FAR):
        settle(BACK, role)

    def finish_first(cols):
        total = xr[1, t, :, cols].astype(f32) + back_dot(0, (OWN, NEAR, OPP, FAR), cols)
        x1[t, :, cols] = total.astype(bf16)

    by_columns(finish_first)
    gather_x.start_all()

    @pl.when(is_mid)
    def _():
        relay_near(SECOND[1])
    relay_opp(SECOND[0])

    @pl.when(is_mid)
    def _():
        relay_near(SECOND[2])
    ss[0] = jnp.zeros(ss.shape[1:], f32)
    scale(1, x1, 0, t)
    relay_opp(SECOND[1])
    gather_x.forward(0)
    gather_x.forward(1)
    relay_opp(SECOND[2])
    gather_x.beside()
    scale(1, x1, 0, tx)
    scale(1, x1, 0, ty)
    relay_far(SECOND[0])
    gather_x.across()
    scale(1, x1, 0, td)
    for u in SECOND[:3]:
        local_w(u).wait()
        for role in (OWN, NEAR, OPP):
            settle(u, role)
    for u in SECOND[:3]:
        project(1, u % 4, (OWN, NEAR, OPP), True)
    settle(SECOND[0], FAR)
    project(1, INNER, (FAR,), False)
    relay_far(SECOND[1])
    settle(SECOND[1], FAR)
    project(1, VALUE, (FAR,), False)
    mix(0, 2)

    @pl.when(s < n_sp - 1)
    def _():
        tail_copy(2, 2, 2, s + 1).start()
    last = SECOND[3]

    @pl.when(is_mid)
    def _():
        send_opp(last)
        relay_near(last)
    relay_far(SECOND[2])

    @pl.when(is_mid)
    def _():
        relay_opp(last)

    @pl.when(s == 0)
    def _():
        halo[2] = jnp.zeros(halo.shape[1:], bf16)

    @pl.when(s > 0)
    def _():
        tail_copy(2, 2, 2, partner).wait_recv()
    convolve(1, 0, 2)
    settle(SECOND[2], FAR)
    project(1, OUTER, (FAR,), False)
    gat[1, t] = gate(0)
    gather_gat[1].start_all()

    @pl.when(is_end)
    def _():
        relay_opp(last)

    @pl.when(is_mid)
    def _():
        relay_far(last, (0, 1))
    gather_gat[1].forward(0)
    gather_gat[1].forward(1)

    @pl.when(is_mid)
    def _():
        relay_far(last, (2, 3))
    gather_gat[1].beside()
    gather_gat[1].across()
    local_w(last).wait()
    for role in (OWN, NEAR, OPP):
        settle(last, role)

    def start_last(cols):
        bacc[:, cols] = x1[t, :, cols].astype(f32) + back_dot(1, (OWN, NEAR, OPP), cols)

    by_columns(start_last)

    @pl.when(is_end)
    def _():
        relay_far(last)
    settle(last, FAR)

    def finish_last(cols):
        out[:, cols] = (bacc[:, cols] + back_dot(1, (FAR,), cols)).astype(bf16)

    by_columns(finish_last)

    some = units - 3

    @pl.when(is_mid)
    def _():
        for kind in (0, 1, 2, 3, 4, 6):
            sent(kind, units)
        for kind in (5, 7, 8):
            sent(kind, some)
        gather_tok.drain()
        for h in range(2):
            end_part(h).wait_send()

        @pl.when(core == 0)
        def _():
            for b in range(2):
                tail_copy(b, b, b, partner).wait_send()

        @pl.when(jnp.logical_and(core == 1, left))
        def _():
            tail_copy(0, 1, 1, partner).wait_send()
            tail_copy(1, 1, 1, s + 1).wait_send()

        @pl.when(jnp.logical_and(core == 1, jnp.logical_not(left)))
        def _():
            tail_copy(1, 0, 0, partner).wait_send()

    @pl.when(is_end)
    def _():
        for kind in (0, 1, 2, 3):
            sent(kind, some)
        sent(5, units)
        for h in range(2):
            tok_part(h).wait_send()
    gather_gat[0].drain()
    gather_x.drain()
    gather_gat[1].drain()

    @pl.when(s < n_sp - 1)
    def _():
        tail_copy(2, 2, 2, partner).wait_send()


def fused(tokens, norm_gain, w_outer, w_inner, w_value, w_back, taps):
    n_sp, n_tp = lax.axis_size("sp"), lax.axis_size("tp")
    rows, width = tokens.shape
    layers, depth, chans = w_outer.shape
    back_rows, feats = w_back.shape[1:]
    if 4 * layers != len(PIECES):
        return per_device(tokens, norm_gain, w_outer, w_inner, w_value, w_back, taps)
    chunks = sum(PIECES)
    dma = pltpu.SemaphoreType.DMA
    hbm, vmem = pl.BlockSpec(memory_space=pl.ANY), pl.BlockSpec(memory_space=pltpu.VMEM)
    held = [
        pltpu.with_memory_space_constraint(a, pltpu.HBM)
        for a in (tokens, norm_gain, w_outer, w_inner, w_value, w_back, taps.transpose(1, 0, 2))
    ]
    return pl.pallas_call(
        mixer_kernel,
        out_shape=jax.ShapeDtypeStruct((rows, feats), bf16),
        in_specs=[hbm] * 7,
        out_specs=vmem,
        scratch_shapes=[
            pltpu.VMEM((layers, width), f32),
            pltpu.VMEM(taps.shape[1:2] + taps.shape[:1] + taps.shape[2:], f32),
            pltpu.VMEM((2, n_tp, rows, feats), bf16),
            pltpu.VMEM((n_tp, rows, feats), bf16),
            pltpu.VMEM((2, n_tp, rows, feats), bf16),
            pltpu.VMEM((3 * layers, n_sp, depth, chans), bf16),
            pltpu.VMEM((layers, n_sp, back_rows, feats), bf16),
            pltpu.VMEM((3, 2, rows, chans), f32),
            pltpu.VMEM((rows, feats), f32),
            pltpu.VMEM((2, rows, 128), f32),
            pltpu.VMEM((layers, n_tp, rows, chans), bf16),
            pltpu.VMEM((rows, chans), bf16),
            pltpu.VMEM((3, rows, chans), bf16),
            pltpu.VMEM((3, 16, chans), bf16),
            dma((2,)),
            dma((4 * layers,)),
            dma((n_tp,)),
            dma((2,)),
            dma((2,)),
            dma((KINDS,)),
            dma((chunks, 3)),
            dma((4 * layers, 4)),
            dma((4,)),
            dma((4, 4)),
            dma((3,)),
            dma((3,)),
            dma((2,)),
            dma((2,)),
        ],
        compiler_params=pltpu.CompilerParams(
            collective_id=0, has_side_effects=True, vmem_limit_bytes=48 * 1024 * 1024
        ),
        name="mixer",
    )(*held)


def solution(mesh):
    in_specs = (
        P("sp", None),
        P(),
        P(None, "sp", "tp"),
        P(None, "sp", "tp"),
        P(None, "sp", "tp"),
        P(None, "sp", "tp"),
        P(None, None, "tp"),
    )
    out_specs = P("sp", "tp")
    body = fused if (mesh.shape["sp"], mesh.shape["tp"]) == (8, 4) else per_device
    return jax.shard_map(
        body, mesh=mesh, in_specs=in_specs, out_specs=out_specs, check_vma=False
    )
```

```python
import functools

import jax
import jax.numpy as jnp
from jax import lax
from jax.experimental import pallas as pl
from jax.experimental.pallas import tpu as pltpu
from jax.sharding import PartitionSpec as P

MESH = pl.DeviceIdType.MESH
f32 = jnp.float32
bf16 = jnp.bfloat16

eps = 1e-06

OUTER, INNER, VALUE, BACK = 0, 1, 2, 3
FIRST = (INNER, VALUE, OUTER)
SECOND = tuple(4 + m for m in FIRST + (BACK,))
SHARED = (BACK,) + SECOND
PIECES = (1, 1, 1, 2, 4, 2, 2, 4)
KINDS = 9


def shifted(block, axis, distance):
    devices = range(lax.axis_size(axis))
    route = [(i - distance, i) for i in devices if i - distance in devices]
    return lax.ppermute(block, axis, route)


def per_device(tokens, norm_gain, w_outer, w_inner, w_value, w_back, taps):
    layers = w_outer.shape[0]
    count = tokens.shape[0]
    feats = w_back.shape[2]
    own = lax.axis_index("tp")
    held = (
        lax.all_gather(w_outer, "sp", axis=1, tiled=True),
        lax.all_gather(w_inner, "sp", axis=1, tiled=True),
        lax.all_gather(w_value, "sp", axis=1, tiled=True),
        lax.all_gather(w_back, "sp", axis=1, tiled=True),
    )
    current = tokens
    resid = lax.dynamic_slice_in_dim(tokens, own * feats, feats, 1)
    for layer in range(layers):
        if layer > 0:
            current = lax.all_gather(resid, "tp", axis=1, tiled=True)
        xf = current.astype(jnp.float32)
        normed = (
            xf * lax.rsqrt(jnp.mean(xf * xf, axis=-1, keepdims=True) + eps) * norm_gain[layer]
        ).astype(jnp.bfloat16)
        outer = jnp.dot(normed, held[0][layer], preferred_element_type=jnp.float32)
        inner = jnp.dot(normed, held[1][layer], preferred_element_type=jnp.float32)
        value = jnp.dot(normed, held[2][layer], preferred_element_type=jnp.float32)
        outer = outer.astype(jnp.bfloat16)
        inner = inner.astype(jnp.bfloat16)
        value = value.astype(jnp.bfloat16)
        mixed = (inner.astype(jnp.float32) * value.astype(jnp.float32)).astype(jnp.bfloat16)
        before = shifted(mixed[count - 2 :], "sp", 1)
        padded = jnp.concatenate([before, mixed], axis=0).astype(jnp.float32)
        conv = (
            taps[layer, 0] * padded[:count]
            + taps[layer, 1] * padded[1 : count + 1]
            + taps[layer, 2] * padded[2:]
        )
        gated = (outer.astype(jnp.float32) * conv).astype(jnp.bfloat16)
        whole = lax.all_gather(gated, "tp", axis=1, tiled=True)
        proj = jnp.dot(whole, held[3][layer], preferred_element_type=jnp.float32)
        resid = (resid.astype(jnp.float32) + proj).astype(jnp.bfloat16)
    return resid


def first_chunk(u):
    return sum(PIECES[:u])


def mixer_kernel(
    tok, gain_hbm, w_outer, w_inner, w_value, w_back, taps_hbm, out,
    gain, taps, xr, xq, stage, x1, scl, sclh, cbuf, cin, win, wback, acc, bacc, ss, gat, gat_end, mixed, halo,
    sem_small, sem_local, sem_tok, t_send, t_recv, c_send, c_recv, s_send, s_recv, w_send, w_recv, p_recv,
    g_send, g_recv, h_send, h_recv, e_send, e_recv,
):
    s, t = lax.axis_index("sp"), lax.axis_index("tp")
    n_sp, n_tp = win.shape[1], xr.shape[0]
    rows, feats = xr.shape[1:]
    quarter = xq.shape[3]
    half = rows // 2
    width = feats * n_tp
    units = len(PIECES)
    core = lax.rem(s, 2)
    flip = 1 - 2 * core
    left = s < n_sp // 2
    side = jnp.where(left, 1, -1)
    own_half = jnp.where(left, 0, 1)
    plane = lax.div(s, 2)
    planes = n_sp // 2
    is_end = jnp.logical_or(plane == 0, plane == planes - 1)
    is_mid = jnp.logical_not(is_end)
    partner = s + flip
    near = jnp.where(is_mid, s - 2 * side, s + 2 * side)
    opp = jnp.where(is_mid, s + 2 * side, s + 4 * side)
    far = jnp.where(is_mid, s + 4 * side, s + 6 * side)
    tx = t + 1 - 2 * lax.rem(t, 2)
    ty = t + 2 - 4 * lax.div(t, 2)
    td = n_tp - 1 - t

    small = (
        pltpu.make_async_copy(gain_hbm, gain, sem_small.at[0]),
        pltpu.make_async_copy(taps_hbm, taps, sem_small.at[1]),
    )
    for copy in small:
        copy.start()
    barrier = pltpu.get_barrier_semaphore()

    def greet(sp, tp):
        pl.semaphore_signal(barrier, inc=1, device_id=(sp, tp), device_id_type=MESH)

    greet(partner, t)
    greet(s, tx)
    greet(s, ty)
    greet(near, t)
    greet(near + flip, t)

    @pl.when(is_mid)
    def _():
        greet(opp, t)
        greet(opp + flip, t)
    pl.semaphore_wait(barrier, jnp.where(is_mid, 7, 5))
    for copy in small:
        copy.wait()

    projections = (w_outer, w_inner, w_value)

    def own_w(u):
        layer, m = u // 4, u % 4
        return projections[m].at[layer] if m < 3 else w_back.at[layer]

    def held_w(u, source):
        layer, m = u // 4, u % 4
        return win.at[3 * layer + m, source] if m < 3 else wback.at[layer, source]

    def remote(a, b, ssem, rsem, sp, tp):
        return pltpu.make_async_remote_copy(
            src_ref=a, dst_ref=b, send_sem=ssem, recv_sem=rsem, device_id=(sp, tp), device_id_type=MESH
        )

    def piece(ref, u, k):
        size = ref.shape[0] // PIECES[u]
        return ref.at[pl.ds(k * size, size)]

    OWN, NEAR, OPP, FAR = 0, 1, 2, 3
    source_of = (s, near, opp, far)

    def w_copy(u, k, role, kind, to_role, target):
        to = piece(held_w(u, source_of[role]), u, k)
        a = piece(own_w(u), u, k) if role == OWN else to
        return remote(a, to, w_send.at[kind], w_recv.at[first_chunk(u) + k, to_role - 1], target, t)

    def to_partner(u, k, role):
        to = piece(held_w(u, source_of[role]), u, k)
        a = piece(own_w(u), u, k) if role == OWN else to
        return remote(a, to, w_send.at[role], p_recv.at[u, role], partner, t)

    def pieces_of(u):
        return range(PIECES[u])

    def arrived(u, k, role):
        to = piece(held_w(u, source_of[role]), u, k)
        remote(to, to, w_send.at[0], w_recv.at[first_chunk(u) + k, role - 1], partner, t).wait_recv()

    def send_opp(u):
        for k in pieces_of(u):
            w_copy(u, k, OWN, 4, OPP, opp).start()

    def send_near(u):
        for k in pieces_of(u):
            w_copy(u, k, OWN, 5, NEAR, near).start()

    def send_partner(u):
        for k in pieces_of(u):
            to_partner(u, k, OWN).start()

    def relay_near(u, ks=None):
        for k in ks or pieces_of(u):
            arrived(u, k, NEAR)

            if u >= 3:
                @pl.when(is_mid)
                def _():
                    w_copy(u, k, NEAR, 6, FAR, opp).start()
            to_partner(u, k, NEAR).start()

    def relay_across(u, role, ks=None):
        for k in ks or pieces_of(u):
            arrived(u, k, role)

            @pl.when(is_mid)
            def _():
                w_copy(u, k, role, 5 + role, role, near).start()
            to_partner(u, k, role).start()

    def relay_opp(u, ks=None):
        relay_across(u, OPP, ks)

    def relay_far(u, ks=None):
        relay_across(u, FAR, ks)

    def settle(u, role):
        to = held_w(u, source_of[role] + flip)
        remote(to, to, w_send.at[0], p_recv.at[u, role], partner, t).wait_recv()

    def sent(kind, count):
        ref = win.at[0, pl.ds(0, count)]
        remote(ref, ref, w_send.at[kind], p_recv.at[0, 0], partner, t).wait_send()

    def local_w(u):
        return pltpu.make_async_copy(own_w(u), held_w(u, s), sem_local.at[u])

    def tok_cols(j):
        return tok.at[:, pl.ds(pl.multiple_of(j * feats, feats), feats)]

    def tok_local(j):
        return pltpu.make_async_copy(tok_cols(j), xr.at[j], sem_tok.at[j])

    def tok_quarter(of_half):
        start = of_half * (width // 2) + t * quarter
        return tok.at[:, pl.ds(pl.multiple_of(start, quarter), quarter)]

    def end_tok():
        return remote(tok_quarter(own_half), xq.at[0, t], t_send.at[0], t_recv.at[0], near, t)

    def mid_tok():
        return remote(tok_quarter(1 - own_half), xq.at[2, t], t_send.at[0], t_recv.at[2], opp, t)

    def to_stage(h):
        span = pl.ds(h * half, half)
        a = tok_quarter(1 - own_half).at[span]
        return remote(a, stage.at[span], t_send.at[1], t_recv.at[3 + h], near, t)

    def from_stage(h):
        span = pl.ds(h * half, half)
        return remote(stage.at[span], xq.at[1, t, span], t_send.at[1], t_recv.at[1], opp, t)

    def tok_arrived(i):
        remote(stage, stage, t_send.at[0], t_recv.at[i], partner, t).wait_recv()

    def part_sum(m, b):
        return remote(cbuf.at[m, b], cin.at[m, b], c_send.at[m], c_recv.at[m], opp, t)

    def part_sums(m):
        return remote(cbuf.at[m], cin.at[m], c_send.at[m], c_recv.at[m], opp, t)

    def squares_copy():
        return remote(ss.at[1], ss.at[0], s_send, s_recv, near, t)

    def end_part(h):
        return remote(
            gat_end.at[pl.ds(h * half, half)], gat.at[0, t, pl.ds(h * half, half)],
            e_send.at[h], e_recv.at[h], near, t,
        )

    class Gather:
        def __init__(self, g, buf):
            self.g, self.buf = g, buf

        def part(self, block, h, k, target):
            size = self.buf.shape[1] // 2
            ref = self.buf.at[block, pl.ds(h * size, size)]
            slot = (0, 1, 2, 2, 3, 3)[k]
            return remote(ref, ref, g_send.at[self.g], g_recv.at[self.g, slot], s, target)

        def whole(self, blocks, slot):
            ref = self.buf.at[pl.ds(0, blocks)]
            return remote(ref, ref, g_send.at[self.g], g_recv.at[self.g, slot], s, tx)

        def start(self, h):
            if h == 0:
                self.part(t, 0, 0, tx).start()
                self.part(t, 0, 3, ty).start()
            else:
                self.part(t, 1, 1, ty).start()
                self.part(t, 1, 2, tx).start()

        def start_all(self):
            self.part(t, 0, 0, tx).start()
            self.part(t, 1, 1, ty).start()
            self.part(t, 1, 2, tx).start()
            self.part(t, 0, 3, ty).start()

        def forward(self, h):
            if h == 0:
                self.part(tx, 0, 0, tx).wait_recv()
                self.part(tx, 0, 4, ty).start()
            else:
                self.part(ty, 1, 1, ty).wait_recv()
                self.part(ty, 1, 5, tx).start()

        def beside(self):
            self.whole(1, 2).wait_recv()

        def across(self):
            self.whole(1, 3).wait_recv()

        def drain(self):
            self.whole(3, 0).wait_send()

    gather_tok = (Gather(0, xq.at[0]), Gather(4, xq.at[1]), Gather(5, xq.at[2]))
    gather_gat = (Gather(1, gat.at[0]), Gather(3, gat.at[1]))
    gather_x = Gather(2, x1)

    def row_tiles(body):
        step = 64

        def tile(r, carry):
            body(pl.ds(pl.multiple_of(r * step, step), step))
            return carry

        lax.fori_loop(0, rows // step, tile, 0)

    def lane_sums(x):
        sq = x * x
        part = sq[:, :128]
        for q in range(1, x.shape[1] // 128):
            part = part + sq[:, 128 * q : 128 * (q + 1)]
        return part

    def squares(b):
        ss[b] = jnp.zeros(ss.shape[1:], f32)

        def one(j, carry):
            def body(span):
                ss[b, span, :] += lane_sums(xr[j, span, :].astype(f32))
            row_tiles(body)
            return carry

        lax.fori_loop(0, n_tp, one, 0)

    def scale(j):
        def body(span):
            x = x1[j, span, :].astype(f32)
            ss[0, span, :] += lane_sums(x)
            cols = pl.ds(pl.multiple_of(j * feats, feats), feats)
            scl[j, span, :] = (x * gain[1:2, cols]).astype(bf16)
        row_tiles(body)

    def scale_part(load, block, j):
        at = pl.multiple_of(j * quarter, quarter)
        cols = pl.ds(pl.multiple_of(own_half * (width // 2) + at, quarter), quarter)

        def body(span):
            sclh[block, span, pl.ds(at, quarter)] = (load(span).astype(f32) * gain[0:1, cols]).astype(bf16)
        row_tiles(body)

    def scale_sent(i, j):
        scale_part(lambda span: xq[i, j, span, :], (0, 2, 3)[i], j)

    def half_dot(m, block):
        depth = win.shape[2]
        sources = pl.ds(own_half * (n_sp // 2), n_sp // 2)
        w = win[m, sources].reshape(n_sp // 2 * depth, win.shape[3])
        return jnp.dot(sclh[block], w, preferred_element_type=f32)

    def send_part_sum(m, b):
        cbuf[m, b] = half_dot(m, 2 + b).astype(bf16)
        part_sum(m, b).start()

    def add_part_sums(m):
        part_sums(m).wait_recv()
        for b in range(2):
            acc[m, b] += cin[m, b].astype(f32)

    def project(m, sources, first):
        depth = win.shape[2]
        total = None
        for role in sources:
            z = lax.div(source_of[role], 2)
            w = win[3 + m, pl.ds(2 * z, 2)].reshape(2 * depth, win.shape[3])
            dot = jnp.dot(scl[z], w, preferred_element_type=f32)
            total = dot if total is None else total + dot
        if first:
            acc[m, 0] = total
        else:
            acc[m, 0] += total

    def inv_of(b):
        return lax.rsqrt(jnp.sum(ss[b], axis=-1, keepdims=True) / width + eps)

    def mix(b, slot):
        inv = inv_of(b)
        inner = (acc[INNER, b] * inv).astype(bf16)
        value = (acc[VALUE, b] * inv).astype(bf16)
        mixed[slot] = (inner.astype(f32) * value.astype(f32)).astype(bf16)

    def convolve(layer, b, slot):
        now = mixed[slot].astype(f32)
        tail = halo[slot].astype(f32)
        row = lax.broadcasted_iota(jnp.int32, now.shape, 0)
        one = jnp.where(row == 0, tail[15:16], pltpu.roll(now, 1, 0))
        two = pltpu.roll(now, 2, 0)
        two = jnp.where(row == 0, tail[14:15], jnp.where(row == 1, tail[15:16], two))
        acc[VALUE, b] = taps[0, layer : layer + 1] * two + taps[1, layer : layer + 1] * one + taps[2, layer : layer + 1] * now

    def gate(b):
        outer = (acc[OUTER, b] * inv_of(b)).astype(bf16).astype(f32)
        return (outer * acc[VALUE, b]).astype(bf16)

    def tail_copy(slot, to_slot, h, target):
        return remote(
            mixed.at[slot, pl.ds(rows - 16, 16)], halo.at[to_slot], h_send.at[slot], h_recv.at[h], target, t
        )

    def back_dot(layer, sources, cols):
        total = None
        for role in sources:
            z = lax.div(source_of[role], 2)
            w = wback[layer, pl.ds(2 * z, 2), :, cols].reshape(2 * wback.shape[2], cols.size)
            dot = jnp.dot(gat[layer, z], w, preferred_element_type=f32)
            total = dot if total is None else total + dot
        return total

    def by_columns(body):
        step = 256

        def tile(c, carry):
            body(pl.ds(pl.multiple_of(c * step, step), step))
            return carry

        lax.fori_loop(0, feats // step, tile, 0)

    @pl.when(is_mid)
    def _():
        mid_tok().start()
        for u in FIRST + SHARED:
            send_partner(u)
        for u in SHARED:
            send_near(u)
        for j in range(n_tp):
            tok_local(j).start()
        for u in FIRST + SHARED:
            local_w(u).start()
        for j in range(n_tp):
            tok_local(j).wait()
        squares(1)

        def scale_own(j, carry):
            piece_of = own_half * (n_tp // 2) + lax.div(j, 2)
            cols = pl.ds(pl.multiple_of(lax.rem(j, 2) * quarter, quarter), quarter)
            scale_part(lambda span: xr[piece_of, span, cols], 1, j)
            return carry

        lax.fori_loop(0, n_tp, scale_own, 0)
        own_end, far_end, far_mid = gather_tok
        for h in range(2):
            to_stage(h).wait_recv()
            from_stage(h).start()
        send_opp(BACK)
        send_opp(SECOND[0])
        tok_arrived(2)
        far_mid.start_all()
        scale_sent(2, t)
        far_mid.forward(0)
        far_mid.forward(1)
        tok_arrived(1)
        far_end.start_all()
        far_mid.beside()
        scale_sent(2, tx)
        scale_sent(2, ty)
        far_mid.across()
        scale_sent(2, td)
        relay_near(INNER)
        scale_sent(1, t)
        relay_opp(BACK)

        def have(u):
            local_w(u).wait()
            settle(u, OWN)
            settle(u, NEAR)

        have(INNER)
        send_part_sum(INNER, 1)
        far_end.forward(0)
        far_end.forward(1)
        tok_arrived(0)
        own_end.start_all()
        scale_sent(0, t)
        far_end.beside()
        scale_sent(1, tx)
        scale_sent(1, ty)
        relay_near(VALUE)
        relay_opp(SECOND[0])
        have(VALUE)
        send_part_sum(VALUE, 1)
        far_end.across()
        scale_sent(1, td)
        send_part_sum(INNER, 0)
        send_part_sum(VALUE, 0)
        own_end.forward(0)
        own_end.forward(1)
        relay_near(OUTER)
        have(OUTER)
        send_part_sum(OUTER, 1)
        send_part_sum(OUTER, 0)
        own_end.beside()
        scale_sent(0, tx)
        scale_sent(0, ty)
        own_end.across()
        scale_sent(0, td)
        for m in FIRST:
            for b in range(2):
                acc[m, b] = half_dot(m, b)
        relay_near(BACK)
        add_part_sums(INNER)
        add_part_sums(VALUE)
        squares_copy().wait_recv()
        for b in range(2):
            mix(b, b)

        @pl.when(core == 0)
        def _():
            for b in range(2):
                tail_copy(b, b, b, partner).start()

        @pl.when(jnp.logical_and(core == 1, left))
        def _():
            tail_copy(1, 1, 1, s + 1).start()
            tail_copy(0, 1, 1, partner).start()

        @pl.when(jnp.logical_and(core == 1, jnp.logical_not(left)))
        def _():
            tail_copy(1, 0, 0, partner).start()
        send_opp(SECOND[1])
        send_opp(SECOND[2])
        add_part_sums(OUTER)
        for b in range(2):
            if b == 0:
                start_of_all = s == 2

                @pl.when(start_of_all)
                def _():
                    halo[0] = jnp.zeros(halo.shape[1:], bf16)

                @pl.when(jnp.logical_not(start_of_all))
                def _():
                    tail_copy(0, 0, 0, partner).wait_recv()
            else:
                tail_copy(1, 1, 1, partner).wait_recv()
            convolve(0, b, b)
            if b == 0:
                gat_end[...] = gate(0)
                for h in range(2):
                    end_part(h).start()
        gat[0, t] = gate(1)
        gather_gat[0].start_all()
        relay_far(BACK, (0,))
        gather_gat[0].forward(0)
        gather_gat[0].forward(1)
        relay_near(SECOND[0])
        relay_far(BACK, (1,))

    @pl.when(is_end)
    def _():
        for h in range(2):
            to_stage(h).start()
        end_tok().start()
        for u in FIRST + (BACK,):
            send_near(u)
        for j in range(n_tp):
            tok_local(j).start()
        for u in SHARED:
            send_partner(u)
        for u in SHARED:
            local_w(u).start()
        for j in range(n_tp):
            tok_local(j).wait()
        squares(1)
        squares_copy().start()
        for u in SECOND:
            send_near(u)
        for u in SHARED:
            relay_near(u)
        relay_opp(BACK)
        relay_opp(SECOND[0])
        for h in range(2):
            end_part(h).wait_recv()
            gather_gat[0].start(h)
        gather_gat[0].forward(0)
        relay_far(BACK, (0,))
        gather_gat[0].forward(1)
        relay_far(BACK, (1,))

    gather_gat[0].beside()
    gather_gat[0].across()
    local_w(BACK).wait()
    for role in (OWN, NEAR, OPP, FAR):
        settle(BACK, role)

    def finish_first(cols):
        total = xr[t, :, cols].astype(f32) + back_dot(0, (OWN, NEAR, OPP, FAR), cols)
        x1[t, :, cols] = total.astype(bf16)

    by_columns(finish_first)
    gather_x.start_all()
    relay_opp(SECOND[1])

    @pl.when(is_mid)
    def _():
        relay_near(SECOND[1])
    ss[0] = jnp.zeros(ss.shape[1:], f32)
    scale(t)
    relay_opp(SECOND[2])

    @pl.when(is_mid)
    def _():
        relay_near(SECOND[2])
    gather_x.forward(0)
    gather_x.forward(1)
    relay_far(SECOND[0])
    gather_x.beside()
    scale(tx)
    scale(ty)
    relay_far(SECOND[1])
    gather_x.across()
    scale(td)
    for u in SECOND[:3]:
        local_w(u).wait()
        for role in (OWN, NEAR, OPP):
            settle(u, role)
    settle(SECOND[0], FAR)
    project(INNER, (OWN, NEAR, OPP, FAR), True)
    project(VALUE, (OWN, NEAR, OPP), True)
    settle(SECOND[1], FAR)
    project(VALUE, (FAR,), False)
    mix(0, 2)

    @pl.when(s < n_sp - 1)
    def _():
        tail_copy(2, 2, 2, s + 1).start()
    last = SECOND[3]

    @pl.when(is_mid)
    def _():
        send_opp(last)
        relay_near(last)
    project(OUTER, (OWN, NEAR, OPP), True)
    relay_far(SECOND[2])

    @pl.when(is_mid)
    def _():
        relay_opp(last)

    @pl.when(s == 0)
    def _():
        halo[2] = jnp.zeros(halo.shape[1:], bf16)

    @pl.when(s > 0)
    def _():
        tail_copy(2, 2, 2, partner).wait_recv()
    convolve(1, 0, 2)
    settle(SECOND[2], FAR)
    project(OUTER, (FAR,), False)
    gat[1, t] = gate(0)
    gather_gat[1].start_all()

    @pl.when(is_end)
    def _():
        relay_opp(last)

    @pl.when(is_mid)
    def _():
        relay_far(last, (0, 1))
    gather_gat[1].forward(0)
    gather_gat[1].forward(1)

    @pl.when(is_mid)
    def _():
        relay_far(last, (2, 3))
    gather_gat[1].beside()
    gather_gat[1].across()
    local_w(last).wait()
    for role in (OWN, NEAR, OPP):
        settle(last, role)

    def start_last(cols):
        bacc[:, cols] = x1[t, :, cols].astype(f32) + back_dot(1, (OWN, NEAR, OPP), cols)

    by_columns(start_last)

    @pl.when(is_end)
    def _():
        relay_far(last)
    settle(last, FAR)

    def finish_last(cols):
        out[:, cols] = (bacc[:, cols] + back_dot(1, (FAR,), cols)).astype(bf16)

    by_columns(finish_last)

    some = units - 3

    @pl.when(is_mid)
    def _():
        for kind in (0, 1):
            sent(kind, units)
        for kind in (2, 3, 4, 5, 6, 7, 8):
            sent(kind, some)
        for g in gather_tok:
            g.drain()
        for i in range(2):
            remote(stage, stage, t_send.at[i], t_recv.at[0], partner, t).wait_send()
        for m in range(3):
            part_sums(m).wait_send()
        for h in range(2):
            end_part(h).wait_send()

        @pl.when(core == 0)
        def _():
            for b in range(2):
                tail_copy(b, b, b, partner).wait_send()

        @pl.when(jnp.logical_and(core == 1, left))
        def _():
            tail_copy(0, 1, 1, partner).wait_send()
            tail_copy(1, 1, 1, s + 1).wait_send()

        @pl.when(jnp.logical_and(core == 1, jnp.logical_not(left)))
        def _():
            tail_copy(1, 0, 0, partner).wait_send()

    @pl.when(is_end)
    def _():
        for kind in (0, 1, 2, 3):
            sent(kind, some)
        sent(5, units)
        for i in range(2):
            remote(stage, stage, t_send.at[i], t_recv.at[0], partner, t).wait_send()
        squares_copy().wait_send()
    gather_gat[0].drain()
    gather_x.drain()
    gather_gat[1].drain()

    @pl.when(s < n_sp - 1)
    def _():
        tail_copy(2, 2, 2, partner).wait_send()


def fused(tokens, norm_gain, w_outer, w_inner, w_value, w_back, taps):
    n_sp, n_tp = lax.axis_size("sp"), lax.axis_size("tp")
    rows, width = tokens.shape
    layers, depth, chans = w_outer.shape
    back_rows, feats = w_back.shape[1:]
    if 4 * layers != len(PIECES):
        return per_device(tokens, norm_gain, w_outer, w_inner, w_value, w_back, taps)
    chunks = sum(PIECES)
    dma = pltpu.SemaphoreType.DMA
    hbm, vmem = pl.BlockSpec(memory_space=pl.ANY), pl.BlockSpec(memory_space=pltpu.VMEM)
    held = [
        pltpu.with_memory_space_constraint(a, pltpu.HBM)
        for a in (tokens, norm_gain, w_outer, w_inner, w_value, w_back, taps.transpose(1, 0, 2))
    ]
    return pl.pallas_call(
        mixer_kernel,
        out_shape=jax.ShapeDtypeStruct((rows, feats), bf16),
        in_specs=[hbm] * 7,
        out_specs=vmem,
        scratch_shapes=[
            pltpu.VMEM((layers, width), f32),
            pltpu.VMEM(taps.shape[1:2] + taps.shape[:1] + taps.shape[2:], f32),
            pltpu.VMEM((n_tp, rows, feats), bf16),
            pltpu.VMEM((3, n_tp, rows, width // 2 // n_tp), bf16),
            pltpu.VMEM((rows, width // 2 // n_tp), bf16),
            pltpu.VMEM((n_tp, rows, feats), bf16),
            pltpu.VMEM((n_tp, rows, feats), bf16),
            pltpu.VMEM((4, rows, width // 2), bf16),
            pltpu.VMEM((3, 2, rows, chans), bf16),
            pltpu.VMEM((3, 2, rows, chans), bf16),
            pltpu.VMEM((3 * layers, n_sp, depth, chans), bf16),
            pltpu.VMEM((layers, n_sp, back_rows, feats), bf16),
            pltpu.VMEM((3, 2, rows, chans), f32),
            pltpu.VMEM((rows, feats), f32),
            pltpu.VMEM((2, rows, 128), f32),
            pltpu.VMEM((layers, n_tp, rows, chans), bf16),
            pltpu.VMEM((rows, chans), bf16),
            pltpu.VMEM((3, rows, chans), bf16),
            pltpu.VMEM((3, 16, chans), bf16),
            dma((2,)),
            dma((4 * layers,)),
            dma((n_tp,)),
            dma((2,)),
            dma((5,)),
            dma((3,)),
            dma((3,)),
            dma,
            dma,
            dma((KINDS,)),
            dma((chunks, 3)),
            dma((4 * layers, 4)),
            dma((6,)),
            dma((6, 4)),
            dma((3,)),
            dma((3,)),
            dma((2,)),
            dma((2,)),
        ],
        compiler_params=pltpu.CompilerParams(
            collective_id=0, has_side_effects=True, vmem_limit_bytes=48 * 1024 * 1024
        ),
        name="mixer",
    )(*held)


def solution(mesh):
    in_specs = (
        P("sp", None),
        P(),
        P(None, "sp", "tp"),
        P(None, "sp", "tp"),
        P(None, "sp", "tp"),
        P(None, "sp", "tp"),
        P(None, None, "tp"),
    )
    out_specs = P("sp", "tp")
    body = fused if (mesh.shape["sp"], mesh.shape["tp"]) == (8, 4) else per_device
    return jax.shard_map(
        body, mesh=mesh, in_specs=in_specs, out_specs=out_specs, check_vma=False
    )
```

```python
import functools

import jax
import jax.numpy as jnp
from jax import lax
from jax.experimental import pallas as pl
from jax.experimental.pallas import tpu as pltpu
from jax.sharding import PartitionSpec as P

MESH = pl.DeviceIdType.MESH
f32 = jnp.float32
bf16 = jnp.bfloat16

eps = 1e-06

OUTER, INNER, VALUE, BACK = 0, 1, 2, 3
FIRST = (INNER, VALUE, OUTER)
SECOND = tuple(4 + m for m in FIRST + (BACK,))
SHARED = (BACK,) + SECOND
PIECES = (1, 1, 1, 2, 4, 2, 2, 4)
KINDS = 9
GROUP = 8


def shifted(block, axis, distance):
    devices = range(lax.axis_size(axis))
    route = [(i - distance, i) for i in devices if i - distance in devices]
    return lax.ppermute(block, axis, route)


def per_device(tokens, norm_gain, w_outer, w_inner, w_value, w_back, taps):
    layers = w_outer.shape[0]
    count = tokens.shape[0]
    feats = w_back.shape[2]
    own = lax.axis_index("tp")
    held = (
        lax.all_gather(w_outer, "sp", axis=1, tiled=True),
        lax.all_gather(w_inner, "sp", axis=1, tiled=True),
        lax.all_gather(w_value, "sp", axis=1, tiled=True),
        lax.all_gather(w_back, "sp", axis=1, tiled=True),
    )
    current = tokens
    resid = lax.dynamic_slice_in_dim(tokens, own * feats, feats, 1)
    for layer in range(layers):
        if layer > 0:
            current = lax.all_gather(resid, "tp", axis=1, tiled=True)
        xf = current.astype(jnp.float32)
        normed = (
            xf * lax.rsqrt(jnp.mean(xf * xf, axis=-1, keepdims=True) + eps) * norm_gain[layer]
        ).astype(jnp.bfloat16)
        outer = jnp.dot(normed, held[0][layer], preferred_element_type=jnp.float32)
        inner = jnp.dot(normed, held[1][layer], preferred_element_type=jnp.float32)
        value = jnp.dot(normed, held[2][layer], preferred_element_type=jnp.float32)
        outer = outer.astype(jnp.bfloat16)
        inner = inner.astype(jnp.bfloat16)
        value = value.astype(jnp.bfloat16)
        mixed = (inner.astype(jnp.float32) * value.astype(jnp.float32)).astype(jnp.bfloat16)
        before = shifted(mixed[count - 2 :], "sp", 1)
        padded = jnp.concatenate([before, mixed], axis=0).astype(jnp.float32)
        conv = (
            taps[layer, 0] * padded[:count]
            + taps[layer, 1] * padded[1 : count + 1]
            + taps[layer, 2] * padded[2:]
        )
        gated = (outer.astype(jnp.float32) * conv).astype(jnp.bfloat16)
        whole = lax.all_gather(gated, "tp", axis=1, tiled=True)
        proj = jnp.dot(whole, held[3][layer], preferred_element_type=jnp.float32)
        resid = (resid.astype(jnp.float32) + proj).astype(jnp.bfloat16)
    return resid


def first_chunk(u):
    return sum(PIECES[:u])


def mixer_kernel(
    tok, gain_hbm, w_outer, w_inner, w_value, w_back, taps_hbm, out,
    gain, taps, xr, xq, stage, x1, scl, sclh, cbuf, cin, win, wback, acc, bacc, ss, gat, gat_end, mixed, halo,
    sem_small, sem_local, sem_tok, t_send, t_recv, c_send, c_recv, s_send, s_recv, w_send, w_recv, p_recv,
    g_send, g_recv, h_send, h_recv, e_send, e_recv,
):
    s, t = lax.axis_index("sp"), lax.axis_index("tp")
    n_sp, n_tp = win.shape[1], xr.shape[0]
    rows, feats = xr.shape[1:]
    quarter = xq.shape[3]
    half = rows // 2
    width = feats * n_tp
    units = len(PIECES)
    core = lax.rem(s, 2)
    flip = 1 - 2 * core
    left = s < n_sp // 2
    side = jnp.where(left, 1, -1)
    own_half = jnp.where(left, 0, 1)
    plane = lax.div(s, 2)
    planes = n_sp // 2
    is_end = jnp.logical_or(plane == 0, plane == planes - 1)
    is_mid = jnp.logical_not(is_end)
    partner = s + flip
    near = jnp.where(is_mid, s - 2 * side, s + 2 * side)
    opp = jnp.where(is_mid, s + 2 * side, s + 4 * side)
    far = jnp.where(is_mid, s + 4 * side, s + 6 * side)
    tx = t + 1 - 2 * lax.rem(t, 2)
    ty = t + 2 - 4 * lax.div(t, 2)
    td = n_tp - 1 - t

    small = (
        pltpu.make_async_copy(gain_hbm, gain, sem_small.at[0]),
        pltpu.make_async_copy(taps_hbm, taps, sem_small.at[1]),
    )
    for copy in small:
        copy.start()
    barrier = pltpu.get_barrier_semaphore()

    def greet(sp, tp):
        pl.semaphore_signal(barrier, inc=1, device_id=(sp, tp), device_id_type=MESH)

    greet(partner, t)
    greet(s, tx)
    greet(s, ty)
    greet(near, t)
    greet(near + flip, t)

    @pl.when(is_mid)
    def _():
        greet(opp, t)
        greet(opp + flip, t)
    pl.semaphore_wait(barrier, jnp.where(is_mid, 7, 5))
    for copy in small:
        copy.wait()

    projections = (w_outer, w_inner, w_value)

    def own_w(u):
        layer, m = u // 4, u % 4
        return projections[m].at[layer] if m < 3 else w_back.at[layer]

    def held_w(u, source):
        layer, m = u // 4, u % 4
        return win.at[3 * layer + m, source] if m < 3 else wback.at[layer, source]

    def remote(a, b, ssem, rsem, sp, tp):
        return pltpu.make_async_remote_copy(
            src_ref=a, dst_ref=b, send_sem=ssem, recv_sem=rsem, device_id=(sp, tp), device_id_type=MESH
        )

    def piece(ref, u, k):
        size = ref.shape[0] // PIECES[u]
        return ref.at[pl.ds(k * size, size)]

    OWN, NEAR, OPP, FAR = 0, 1, 2, 3
    source_of = (s, near, opp, far)

    def w_copy(u, k, role, kind, to_role, target):
        to = piece(held_w(u, source_of[role]), u, k)
        a = piece(own_w(u), u, k) if role == OWN else to
        return remote(a, to, w_send.at[kind], w_recv.at[first_chunk(u) + k, to_role - 1], target, t)

    def to_partner(u, k, role):
        to = piece(held_w(u, source_of[role]), u, k)
        a = piece(own_w(u), u, k) if role == OWN else to
        return remote(a, to, w_send.at[role], p_recv.at[group_of(u, role)], partner, t)

    def pieces_of(u):
        return range(PIECES[u])

    def arrived(u, k, role):
        to = piece(held_w(u, source_of[role]), u, k)
        remote(to, to, w_send.at[0], w_recv.at[first_chunk(u) + k, role - 1], partner, t).wait_recv()

    def send_opp(u):
        for k in pieces_of(u):
            w_copy(u, k, OWN, 4, OPP, opp).start()

    def send_near(u):
        for k in pieces_of(u):
            w_copy(u, k, OWN, 5, NEAR, near).start()

    def send_partner(u):
        for k in pieces_of(u):
            to_partner(u, k, OWN).start()

    def relay_near(u, ks=None):
        for k in ks or pieces_of(u):
            arrived(u, k, NEAR)

            if u >= 3:
                @pl.when(is_mid)
                def _():
                    w_copy(u, k, NEAR, 6, FAR, opp).start()
            to_partner(u, k, NEAR).start()

    def relay_across(u, role, ks=None):
        for k in ks or pieces_of(u):
            arrived(u, k, role)

            @pl.when(is_mid)
            def _():
                w_copy(u, k, role, 5 + role, role, near).start()
            to_partner(u, k, role).start()

    def relay_opp(u, ks=None):
        relay_across(u, OPP, ks)

    def relay_far(u, ks=None):
        relay_across(u, FAR, ks)

    counts = {INNER: 2, VALUE: 2, OUTER: 2, BACK: 4, GROUP: 9, GROUP + 1: 1, GROUP + 2: 1, GROUP + 3: 1, 7: 3, GROUP + 4: 1}

    def group_of(u, role):
        if u <= BACK:
            return u
        if u == 7:
            return GROUP + 4 if role == FAR else 7
        return GROUP + 1 + SECOND.index(u) if role == FAR else GROUP

    def settle(group):
        count = counts[group]
        ref = win.at[pl.ds(0, 3), pl.ds(0, 3)] if count == 9 else win.at[0, pl.ds(0, count)]
        remote(ref, ref, w_send.at[0], p_recv.at[group], partner, t).wait_recv()

    def sent(kind, count):
        ref = win.at[0, pl.ds(0, count)]
        remote(ref, ref, w_send.at[kind], p_recv.at[0], partner, t).wait_send()

    def local_w(u):
        return pltpu.make_async_copy(own_w(u), held_w(u, s), sem_local)

    def local_w_wait(count):
        ref = win.at[0, pl.ds(0, count)]
        pltpu.make_async_copy(ref, ref, sem_local).wait()

    def tok_cols(j):
        return tok.at[:, pl.ds(pl.multiple_of(j * feats, feats), feats)]

    def tok_local(j):
        return pltpu.make_async_copy(tok_cols(j), xr.at[j], sem_tok)

    def tok_local_wait():
        pltpu.make_async_copy(xr, xr, sem_tok).wait()

    def tok_quarter(of_half):
        start = of_half * (width // 2) + t * quarter
        return tok.at[:, pl.ds(pl.multiple_of(start, quarter), quarter)]

    def end_tok():
        return remote(tok_quarter(own_half), xq.at[0, t], t_send.at[0], t_recv.at[0], near, t)

    def mid_tok():
        return remote(tok_quarter(1 - own_half), xq.at[2, t], t_send.at[0], t_recv.at[2], opp, t)

    def to_stage(h):
        span = pl.ds(h * half, half)
        a = tok_quarter(1 - own_half).at[span]
        return remote(a, stage.at[span], t_send.at[1], t_recv.at[3 + h], near, t)

    def from_stage(h):
        span = pl.ds(h * half, half)
        return remote(stage.at[span], xq.at[1, t, span], t_send.at[1], t_recv.at[1], opp, t)

    def tok_arrived(i):
        remote(stage, stage, t_send.at[0], t_recv.at[i], partner, t).wait_recv()

    def part_sum(m, b):
        return remote(cbuf.at[m, b], cin.at[m, b], c_send.at[m], c_recv.at[m], opp, t)

    def part_sums(m):
        return remote(cbuf.at[m], cin.at[m], c_send.at[m], c_recv.at[m], opp, t)

    def squares_copy():
        return remote(ss.at[1], ss.at[0], s_send, s_recv, near, t)

    def end_part(h):
        return remote(
            gat_end.at[pl.ds(h * half, half)], gat.at[0, t, pl.ds(h * half, half)],
            e_send.at[h], e_recv.at[h], near, t,
        )

    class Gather:
        def __init__(self, g, buf):
            self.g, self.buf = g, buf

        def part(self, block, h, k, target):
            size = self.buf.shape[1] // 2
            ref = self.buf.at[block, pl.ds(h * size, size)]
            slot = (0, 1, 2, 2, 3, 3)[k]
            return remote(ref, ref, g_send.at[self.g], g_recv.at[self.g, slot], s, target)

        def whole(self, blocks, slot):
            ref = self.buf.at[pl.ds(0, blocks)]
            return remote(ref, ref, g_send.at[self.g], g_recv.at[self.g, slot], s, tx)

        def start(self, h):
            if h == 0:
                self.part(t, 0, 0, tx).start()
                self.part(t, 0, 3, ty).start()
            else:
                self.part(t, 1, 1, ty).start()
                self.part(t, 1, 2, tx).start()

        def start_all(self):
            self.part(t, 0, 0, tx).start()
            self.part(t, 1, 1, ty).start()
            self.part(t, 1, 2, tx).start()
            self.part(t, 0, 3, ty).start()

        def forward(self, h):
            if h == 0:
                self.part(tx, 0, 0, tx).wait_recv()
                self.part(tx, 0, 4, ty).start()
            else:
                self.part(ty, 1, 1, ty).wait_recv()
                self.part(ty, 1, 5, tx).start()

        def beside(self):
            self.whole(1, 2).wait_recv()

        def across(self):
            self.whole(1, 3).wait_recv()

        def drain(self):
            self.whole(3, 0).wait_send()

    gather_tok = (Gather(0, xq.at[0]), Gather(4, xq.at[1]), Gather(5, xq.at[2]))
    gather_gat = (Gather(1, gat.at[0]), Gather(3, gat.at[1]))
    gather_x = Gather(2, x1)

    def row_tiles(body):
        step = 64

        def tile(r, carry):
            body(pl.ds(pl.multiple_of(r * step, step), step))
            return carry

        lax.fori_loop(0, rows // step, tile, 0)

    def lane_sums(x):
        sq = x * x
        part = sq[:, :128]
        for q in range(1, x.shape[1] // 128):
            part = part + sq[:, 128 * q : 128 * (q + 1)]
        return part

    def squares(b):
        ss[b] = jnp.zeros(ss.shape[1:], f32)

        def one(j, carry):
            def body(span):
                ss[b, span, :] += lane_sums(xr[j, span, :].astype(f32))
            row_tiles(body)
            return carry

        lax.fori_loop(0, n_tp, one, 0)

    def scale(j):
        def body(span):
            x = x1[j, span, :].astype(f32)
            ss[0, span, :] += lane_sums(x)
            cols = pl.ds(pl.multiple_of(j * feats, feats), feats)
            scl[j, span, :] = (x * gain[1:2, cols]).astype(bf16)
        row_tiles(body)

    def scale_part(load, block, j):
        at = pl.multiple_of(j * quarter, quarter)
        cols = pl.ds(pl.multiple_of(own_half * (width // 2) + at, quarter), quarter)

        def body(span):
            sclh[block, span, pl.ds(at, quarter)] = (load(span).astype(f32) * gain[0:1, cols]).astype(bf16)
        row_tiles(body)

    def scale_sent(i, j):
        scale_part(lambda span: xq[i, j, span, :], (0, 2, 3)[i], j)

    def half_dot(m, block):
        depth = win.shape[2]
        sources = pl.ds(own_half * (n_sp // 2), n_sp // 2)
        w = win[m, sources].reshape(n_sp // 2 * depth, win.shape[3])
        return jnp.dot(sclh[block], w, preferred_element_type=f32)

    def send_part_sum(m, b):
        cbuf[m, b] = half_dot(m, 2 + b).astype(bf16)
        part_sum(m, b).start()

    def add_part_sums(m):
        part_sums(m).wait_recv()
        for b in range(2):
            acc[m, b] += cin[m, b].astype(f32)

    def project(m, sources, first):
        depth = win.shape[2]
        total = None
        for role in sources:
            z = lax.div(source_of[role], 2)
            w = win[3 + m, pl.ds(2 * z, 2)].reshape(2 * depth, win.shape[3])
            dot = jnp.dot(scl[z], w, preferred_element_type=f32)
            total = dot if total is None else total + dot
        if first:
            acc[m, 0] = total
        else:
            acc[m, 0] += total

    def inv_of(b):
        return lax.rsqrt(jnp.sum(ss[b], axis=-1, keepdims=True) / width + eps)

    def mix(b, slot):
        inv = inv_of(b)
        inner = (acc[INNER, b] * inv).astype(bf16)
        value = (acc[VALUE, b] * inv).astype(bf16)
        mixed[slot] = (inner.astype(f32) * value.astype(f32)).astype(bf16)

    def convolve(layer, b, slot):
        now = mixed[slot].astype(f32)
        tail = halo[slot].astype(f32)
        row = lax.broadcasted_iota(jnp.int32, now.shape, 0)
        one = jnp.where(row == 0, tail[15:16], pltpu.roll(now, 1, 0))
        two = pltpu.roll(now, 2, 0)
        two = jnp.where(row == 0, tail[14:15], jnp.where(row == 1, tail[15:16], two))
        acc[VALUE, b] = taps[0, layer : layer + 1] * two + taps[1, layer : layer + 1] * one + taps[2, layer : layer + 1] * now

    def gate(b):
        outer = (acc[OUTER, b] * inv_of(b)).astype(bf16).astype(f32)
        return (outer * acc[VALUE, b]).astype(bf16)

    def tail_copy(slot, to_slot, h, target):
        return remote(
            mixed.at[slot, pl.ds(rows - 16, 16)], halo.at[to_slot], h_send.at[slot], h_recv.at[h], target, t
        )

    def back_dot(layer, sources, cols):
        total = None
        for role in sources:
            z = lax.div(source_of[role], 2)
            w = wback[layer, pl.ds(2 * z, 2), :, cols].reshape(2 * wback.shape[2], cols.size)
            dot = jnp.dot(gat[layer, z], w, preferred_element_type=f32)
            total = dot if total is None else total + dot
        return total

    def by_columns(body):
        step = 256
        for c in range(feats // step):
            body(pl.ds(c * step, step))

    @pl.when(is_mid)
    def _():
        mid_tok().start()
        for u in FIRST + SHARED:
            send_partner(u)
        for u in SHARED:
            send_near(u)
        for j in range(n_tp):
            tok_local(j).start()
        for u in FIRST + SHARED:
            local_w(u).start()
        tok_local_wait()
        squares(1)

        def scale_own(j, carry):
            piece_of = own_half * (n_tp // 2) + lax.div(j, 2)
            cols = pl.ds(pl.multiple_of(lax.rem(j, 2) * quarter, quarter), quarter)
            scale_part(lambda span: xr[piece_of, span, cols], 1, j)
            return carry

        lax.fori_loop(0, n_tp, scale_own, 0)
        local_w_wait(units)
        own_end, far_end, far_mid = gather_tok
        for h in range(2):
            to_stage(h).wait_recv()
            from_stage(h).start()
        send_opp(BACK)
        send_opp(SECOND[0])
        tok_arrived(2)
        far_mid.start_all()
        scale_sent(2, t)
        far_mid.forward(0)
        far_mid.forward(1)
        tok_arrived(1)
        far_end.start_all()
        far_mid.beside()
        scale_sent(2, tx)
        scale_sent(2, ty)
        far_mid.across()
        scale_sent(2, td)
        relay_near(INNER)
        scale_sent(1, t)
        relay_opp(BACK)

        settle(INNER)
        send_part_sum(INNER, 1)
        far_end.forward(0)
        far_end.forward(1)
        tok_arrived(0)
        own_end.start_all()
        scale_sent(0, t)
        far_end.beside()
        scale_sent(1, tx)
        scale_sent(1, ty)
        relay_near(VALUE)
        relay_opp(SECOND[0])
        settle(VALUE)
        send_part_sum(VALUE, 1)
        far_end.across()
        scale_sent(1, td)
        send_part_sum(INNER, 0)
        send_part_sum(VALUE, 0)
        own_end.forward(0)
        own_end.forward(1)
        relay_near(OUTER)
        settle(OUTER)
        send_part_sum(OUTER, 1)
        send_part_sum(OUTER, 0)
        own_end.beside()
        scale_sent(0, tx)
        scale_sent(0, ty)
        own_end.across()
        scale_sent(0, td)
        for m in FIRST:
            for b in range(2):
                acc[m, b] = half_dot(m, b)
        add_part_sums(INNER)
        add_part_sums(VALUE)
        squares_copy().wait_recv()
        for b in range(2):
            mix(b, b)

        @pl.when(core == 0)
        def _():
            for b in range(2):
                tail_copy(b, b, b, partner).start()

        @pl.when(jnp.logical_and(core == 1, left))
        def _():
            tail_copy(1, 1, 1, s + 1).start()
            tail_copy(0, 1, 1, partner).start()

        @pl.when(jnp.logical_and(core == 1, jnp.logical_not(left)))
        def _():
            tail_copy(1, 0, 0, partner).start()
        relay_near(BACK)
        send_opp(SECOND[1])
        send_opp(SECOND[2])
        add_part_sums(OUTER)
        for b in range(2):
            if b == 0:
                start_of_all = s == 2

                @pl.when(start_of_all)
                def _():
                    halo[0] = jnp.zeros(halo.shape[1:], bf16)

                @pl.when(jnp.logical_not(start_of_all))
                def _():
                    tail_copy(0, 0, 0, partner).wait_recv()
            else:
                tail_copy(1, 1, 1, partner).wait_recv()
            convolve(0, b, b)
            if b == 0:
                gat_end[...] = gate(0)
                for h in range(2):
                    end_part(h).start()
        gat[0, t] = gate(1)
        gather_gat[0].start_all()
        relay_far(BACK, (0,))
        gather_gat[0].forward(0)
        gather_gat[0].forward(1)
        relay_near(SECOND[0])
        relay_far(BACK, (1,))

    @pl.when(is_end)
    def _():
        for h in range(2):
            to_stage(h).start()
        end_tok().start()
        for u in FIRST + (BACK,):
            send_near(u)
        for j in range(n_tp):
            tok_local(j).start()
        for u in SHARED:
            send_partner(u)
        for u in SHARED:
            local_w(u).start()
        tok_local_wait()
        squares(1)
        squares_copy().start()
        for u in SECOND:
            send_near(u)
        local_w_wait(units - 3)
        for u in SHARED:
            relay_near(u)
        relay_opp(BACK)
        relay_opp(SECOND[0])
        for h in range(2):
            end_part(h).wait_recv()
            gather_gat[0].start(h)
        gather_gat[0].forward(0)
        relay_far(BACK, (0,))
        gather_gat[0].forward(1)
        relay_far(BACK, (1,))

    gather_gat[0].beside()
    gather_gat[0].across()
    settle(BACK)

    @pl.when(is_mid)
    def _():
        relay_opp(SECOND[1], (0,))

    def finish_first(cols):
        total = xr[t, :, cols].astype(f32) + back_dot(0, (OWN, NEAR, OPP, FAR), cols)
        x1[t, :, cols] = total.astype(bf16)

    by_columns(finish_first)
    gather_x.start_all()

    @pl.when(is_end)
    def _():
        relay_opp(SECOND[1], (0,))
    relay_opp(SECOND[1], (1,))

    @pl.when(is_mid)
    def _():
        relay_near(SECOND[1])
    ss[0] = jnp.zeros(ss.shape[1:], f32)
    scale(t)
    relay_opp(SECOND[2])

    @pl.when(is_mid)
    def _():
        relay_near(SECOND[2])
    gather_x.forward(0)
    gather_x.forward(1)
    relay_far(SECOND[0])
    gather_x.beside()
    scale(tx)
    scale(ty)
    relay_far(SECOND[1])
    gather_x.across()
    scale(td)
    settle(GROUP)
    def early_far(k):
        @pl.when(is_mid)
        def _():
            relay_far(SECOND[2], (k,))

    early_far(0)
    settle(GROUP + 1)
    project(INNER, (OWN, NEAR, OPP, FAR), True)
    early_far(1)
    project(VALUE, (OWN, NEAR, OPP), True)
    settle(GROUP + 2)
    project(VALUE, (FAR,), False)
    early_far(2)
    mix(0, 2)

    @pl.when(s < n_sp - 1)
    def _():
        tail_copy(2, 2, 2, s + 1).start()
    last = SECOND[3]

    @pl.when(is_mid)
    def _():
        send_opp(last)
        relay_near(last)
    project(OUTER, (OWN, NEAR, OPP), True)

    @pl.when(is_end)
    def _():
        relay_far(SECOND[2], (0, 1, 2))
    relay_far(SECOND[2], (3,))

    @pl.when(is_mid)
    def _():
        relay_opp(last)

    @pl.when(s == 0)
    def _():
        halo[2] = jnp.zeros(halo.shape[1:], bf16)

    @pl.when(s > 0)
    def _():
        tail_copy(2, 2, 2, partner).wait_recv()
    convolve(1, 0, 2)
    settle(GROUP + 3)
    project(OUTER, (FAR,), False)
    gat[1, t] = gate(0)
    gather_gat[1].start_all()

    @pl.when(is_end)
    def _():
        relay_opp(last, (0, 1))

    @pl.when(is_mid)
    def _():
        relay_far(last, (0, 1))
    gather_gat[1].forward(0)
    gather_gat[1].forward(1)

    @pl.when(is_end)
    def _():
        relay_opp(last, (2, 3))

    @pl.when(is_mid)
    def _():
        relay_far(last, (2, 3))
    gather_gat[1].beside()
    gather_gat[1].across()
    settle(last)

    def start_last(cols):
        bacc[:, cols] = x1[t, :, cols].astype(f32) + back_dot(1, (OWN, NEAR, OPP), cols)

    by_columns(start_last)

    @pl.when(is_end)
    def _():
        relay_far(last)
    settle(GROUP + 4)

    def finish_last(cols):
        out[:, cols] = (bacc[:, cols] + back_dot(1, (FAR,), cols)).astype(bf16)

    by_columns(finish_last)

    some = units - 3

    @pl.when(is_mid)
    def _():
        for kind in (0, 1):
            sent(kind, units)
        for kind in (2, 3, 4, 5, 6, 7, 8):
            sent(kind, some)
        for g in gather_tok:
            g.drain()
        for i in range(2):
            remote(stage, stage, t_send.at[i], t_recv.at[0], partner, t).wait_send()
        for m in range(3):
            part_sums(m).wait_send()
        for h in range(2):
            end_part(h).wait_send()

        @pl.when(core == 0)
        def _():
            for b in range(2):
                tail_copy(b, b, b, partner).wait_send()

        @pl.when(jnp.logical_and(core == 1, left))
        def _():
            tail_copy(0, 1, 1, partner).wait_send()
            tail_copy(1, 1, 1, s + 1).wait_send()

        @pl.when(jnp.logical_and(core == 1, jnp.logical_not(left)))
        def _():
            tail_copy(1, 0, 0, partner).wait_send()

    @pl.when(is_end)
    def _():
        for kind in (0, 1, 2, 3):
            sent(kind, some)
        sent(5, units)
        for i in range(2):
            remote(stage, stage, t_send.at[i], t_recv.at[0], partner, t).wait_send()
        squares_copy().wait_send()
    gather_gat[0].drain()
    gather_x.drain()
    gather_gat[1].drain()

    @pl.when(s < n_sp - 1)
    def _():
        tail_copy(2, 2, 2, partner).wait_send()


def fused(tokens, norm_gain, w_outer, w_inner, w_value, w_back, taps):
    n_sp, n_tp = lax.axis_size("sp"), lax.axis_size("tp")
    rows, width = tokens.shape
    layers, depth, chans = w_outer.shape
    back_rows, feats = w_back.shape[1:]
    if 4 * layers != len(PIECES):
        return per_device(tokens, norm_gain, w_outer, w_inner, w_value, w_back, taps)
    chunks = sum(PIECES)
    dma = pltpu.SemaphoreType.DMA
    hbm, vmem = pl.BlockSpec(memory_space=pl.ANY), pl.BlockSpec(memory_space=pltpu.VMEM)
    held = [
        pltpu.with_memory_space_constraint(a, pltpu.HBM)
        for a in (tokens, norm_gain, w_outer, w_inner, w_value, w_back, taps.transpose(1, 0, 2))
    ]
    return pl.pallas_call(
        mixer_kernel,
        out_shape=jax.ShapeDtypeStruct((rows, feats), bf16),
        in_specs=[hbm] * 7,
        out_specs=vmem,
        scratch_shapes=[
            pltpu.VMEM((layers, width), f32),
            pltpu.VMEM(taps.shape[1:2] + taps.shape[:1] + taps.shape[2:], f32),
            pltpu.VMEM((n_tp, rows, feats), bf16),
            pltpu.VMEM((3, n_tp, rows, width // 2 // n_tp), bf16),
            pltpu.VMEM((rows, width // 2 // n_tp), bf16),
            pltpu.VMEM((n_tp, rows, feats), bf16),
            pltpu.VMEM((n_tp, rows, feats), bf16),
            pltpu.VMEM((4, rows, width // 2), bf16),
            pltpu.VMEM((3, 2, rows, chans), bf16),
            pltpu.VMEM((3, 2, rows, chans), bf16),
            pltpu.VMEM((3 * layers, n_sp, depth, chans), bf16),
            pltpu.VMEM((layers, n_sp, back_rows, feats), bf16),
            pltpu.VMEM((3, 2, rows, chans), f32),
            pltpu.VMEM((rows, feats), f32),
            pltpu.VMEM((2, rows, 128), f32),
            pltpu.VMEM((layers, n_tp, rows, chans), bf16),
            pltpu.VMEM((rows, chans), bf16),
            pltpu.VMEM((3, rows, chans), bf16),
            pltpu.VMEM((3, 16, chans), bf16),
            dma((2,)),
            dma,
            dma,
            dma((2,)),
            dma((5,)),
            dma((3,)),
            dma((3,)),
            dma,
            dma,
            dma((KINDS,)),
            dma((chunks, 3)),
            dma((GROUP + 5,)),
            dma((6,)),
            dma((6, 4)),
            dma((3,)),
            dma((3,)),
            dma((2,)),
            dma((2,)),
        ],
        compiler_params=pltpu.CompilerParams(
            collective_id=0, has_side_effects=True, vmem_limit_bytes=48 * 1024 * 1024
        ),
        name="mixer",
    )(*held)


def solution(mesh):
    in_specs = (
        P("sp", None),
        P(),
        P(None, "sp", "tp"),
        P(None, "sp", "tp"),
        P(None, "sp", "tp"),
        P(None, "sp", "tp"),
        P(None, None, "tp"),
    )
    out_specs = P("sp", "tp")
    body = fused if (mesh.shape["sp"], mesh.shape["tp"]) == (8, 4) else per_device
    return jax.shard_map(
        body, mesh=mesh, in_specs=in_specs, out_specs=out_specs, check_vma=False
    )
```

```python
import functools

import jax
import jax.numpy as jnp
from jax import lax
from jax.experimental import pallas as pl
from jax.experimental.pallas import tpu as pltpu
from jax.sharding import PartitionSpec as P

MESH = pl.DeviceIdType.MESH
f32 = jnp.float32
bf16 = jnp.bfloat16

eps = 1e-06

OUTER, INNER, VALUE, BACK = 0, 1, 2, 3
FIRST = (INNER, VALUE, OUTER)
SECOND = tuple(4 + m for m in FIRST + (BACK,))
SHARED = (BACK,) + SECOND
PIECES = (1, 1, 1, 2, 4, 2, 2, 4)
GROUP = 8


def shifted(block, axis, distance):
    devices = range(lax.axis_size(axis))
    route = [(i - distance, i) for i in devices if i - distance in devices]
    return lax.ppermute(block, axis, route)


def per_device(tokens, norm_gain, w_outer, w_inner, w_value, w_back, taps):
    layers = w_outer.shape[0]
    count = tokens.shape[0]
    feats = w_back.shape[2]
    own = lax.axis_index("tp")
    held = (
        lax.all_gather(w_outer, "sp", axis=1, tiled=True),
        lax.all_gather(w_inner, "sp", axis=1, tiled=True),
        lax.all_gather(w_value, "sp", axis=1, tiled=True),
        lax.all_gather(w_back, "sp", axis=1, tiled=True),
    )
    current = tokens
    resid = lax.dynamic_slice_in_dim(tokens, own * feats, feats, 1)
    for layer in range(layers):
        if layer > 0:
            current = lax.all_gather(resid, "tp", axis=1, tiled=True)
        xf = current.astype(jnp.float32)
        normed = (
            xf * lax.rsqrt(jnp.mean(xf * xf, axis=-1, keepdims=True) + eps) * norm_gain[layer]
        ).astype(jnp.bfloat16)
        outer = jnp.dot(normed, held[0][layer], preferred_element_type=jnp.float32)
        inner = jnp.dot(normed, held[1][layer], preferred_element_type=jnp.float32)
        value = jnp.dot(normed, held[2][layer], preferred_element_type=jnp.float32)
        outer = outer.astype(jnp.bfloat16)
        inner = inner.astype(jnp.bfloat16)
        value = value.astype(jnp.bfloat16)
        mixed = (inner.astype(jnp.float32) * value.astype(jnp.float32)).astype(jnp.bfloat16)
        before = shifted(mixed[count - 2 :], "sp", 1)
        padded = jnp.concatenate([before, mixed], axis=0).astype(jnp.float32)
        conv = (
            taps[layer, 0] * padded[:count]
            + taps[layer, 1] * padded[1 : count + 1]
            + taps[layer, 2] * padded[2:]
        )
        gated = (outer.astype(jnp.float32) * conv).astype(jnp.bfloat16)
        whole = lax.all_gather(gated, "tp", axis=1, tiled=True)
        proj = jnp.dot(whole, held[3][layer], preferred_element_type=jnp.float32)
        resid = (resid.astype(jnp.float32) + proj).astype(jnp.bfloat16)
    return resid


def chunk(u, k, role):
    if u < BACK:
        return u
    return 3 + 3 * (sum(PIECES[BACK:u]) + k) + role - 1


def mixer_kernel(
    tok, gain_hbm, w_outer, w_inner, w_value, w_back, taps_hbm, out,
    gain, taps, xr, xq, stage, x1, scl, sclh, cbuf, cin, win, wback, acc, bacc, ss, gat, gat_end, mixed, halo,
    sem_small, sem_local, sem_tok, t_send, t_recv, c_send, c_recv, s_send, s_recv, w_send, w_recv, p_recv,
    g_send, g_recv, h_send, h_recv, e_send, e_recv,
):
    s, t = lax.axis_index("sp"), lax.axis_index("tp")
    n_sp, n_tp = win.shape[1], xr.shape[0]
    rows, feats = xr.shape[1:]
    quarter = xq.shape[3]
    half = rows // 2
    width = feats * n_tp
    units = len(PIECES)
    core = lax.rem(s, 2)
    flip = 1 - 2 * core
    left = s < n_sp // 2
    side = jnp.where(left, 1, -1)
    own_half = jnp.where(left, 0, 1)
    plane = lax.div(s, 2)
    planes = n_sp // 2
    is_end = jnp.logical_or(plane == 0, plane == planes - 1)
    is_mid = jnp.logical_not(is_end)
    partner = s + flip
    near = jnp.where(is_mid, s - 2 * side, s + 2 * side)
    opp = jnp.where(is_mid, s + 2 * side, s + 4 * side)
    far = jnp.where(is_mid, s + 4 * side, s + 6 * side)
    tx = t + 1 - 2 * lax.rem(t, 2)
    ty = t + 2 - 4 * lax.div(t, 2)
    td = n_tp - 1 - t

    small = (
        pltpu.make_async_copy(gain_hbm, gain, sem_small.at[0]),
        pltpu.make_async_copy(taps_hbm, taps, sem_small.at[1]),
    )
    for copy in small:
        copy.start()
    barrier = pltpu.get_barrier_semaphore()

    def greet(sp, tp):
        pl.semaphore_signal(barrier, inc=1, device_id=(sp, tp), device_id_type=MESH)

    greet(partner, t)
    greet(s, tx)
    greet(s, ty)
    greet(near, t)
    greet(near + flip, t)

    @pl.when(is_mid)
    def _():
        greet(opp, t)
        greet(opp + flip, t)
    pl.semaphore_wait(barrier, jnp.where(is_mid, 7, 5))
    for copy in small:
        copy.wait()

    projections = (w_outer, w_inner, w_value)

    def own_w(u):
        layer, m = u // 4, u % 4
        return projections[m].at[layer] if m < 3 else w_back.at[layer]

    def held_w(u, source):
        layer, m = u // 4, u % 4
        return win.at[3 * layer + m, source] if m < 3 else wback.at[layer, source]

    def remote(a, b, ssem, rsem, sp, tp):
        return pltpu.make_async_remote_copy(
            src_ref=a, dst_ref=b, send_sem=ssem, recv_sem=rsem, device_id=(sp, tp), device_id_type=MESH
        )

    def piece(ref, u, k):
        size = ref.shape[0] // PIECES[u]
        return ref.at[pl.ds(k * size, size)]

    OWN, NEAR, OPP, FAR = 0, 1, 2, 3
    source_of = (s, near, opp, far)

    def w_copy(u, k, role, kind, to_role, target):
        to = piece(held_w(u, source_of[role]), u, k)
        a = piece(own_w(u), u, k) if role == OWN else to
        return remote(a, to, w_send.at[min(kind // 2, 1)], w_recv.at[chunk(u, k, to_role)], target, t)

    def to_partner(u, k, role):
        to = piece(held_w(u, source_of[role]), u, k)
        a = piece(own_w(u), u, k) if role == OWN else to
        return remote(a, to, w_send.at[role // 2], p_recv.at[group_of(u, role)], partner, t)

    def pieces_of(u):
        return range(PIECES[u])

    def arrived(u, k, role):
        to = piece(held_w(u, source_of[role]), u, k)
        remote(to, to, w_send.at[0], w_recv.at[chunk(u, k, role)], partner, t).wait_recv()

    def send_opp(u, ks=None):
        for k in ks or pieces_of(u):
            w_copy(u, k, OWN, 4, OPP, opp).start()

    def send_near(u):
        for k in pieces_of(u):
            w_copy(u, k, OWN, 5, NEAR, near).start()

    def send_partner(u):
        for k in pieces_of(u):
            to_partner(u, k, OWN).start()

    def relay_near(u, ks=None):
        for k in ks or pieces_of(u):
            arrived(u, k, NEAR)

            if u >= 3:
                @pl.when(is_mid)
                def _():
                    w_copy(u, k, NEAR, 6, FAR, opp).start()
            to_partner(u, k, NEAR).start()

    def relay_across(u, role, ks=None):
        for k in ks or pieces_of(u):
            arrived(u, k, role)

            @pl.when(is_mid)
            def _():
                w_copy(u, k, role, 5 + role, role, near).start()
            to_partner(u, k, role).start()

    def relay_opp(u, ks=None):
        relay_across(u, OPP, ks)

    def relay_far(u, ks=None):
        relay_across(u, FAR, ks)

    counts = {INNER: 2, VALUE: 2, OUTER: 2, BACK: 4, GROUP: 9, GROUP + 1: 1, GROUP + 2: 1, GROUP + 3: 1, 7: 3, GROUP + 4: 1}

    def group_of(u, role):
        if u <= BACK:
            return u
        if u == 7:
            return GROUP + 4 if role == FAR else 7
        return GROUP + 1 + SECOND.index(u) if role == FAR else GROUP

    def settle(group):
        count = counts[group]
        ref = win.at[pl.ds(0, 3), pl.ds(0, 3)] if count == 9 else win.at[0, pl.ds(0, count)]
        remote(ref, ref, w_send.at[0], p_recv.at[group], partner, t).wait_recv()

    def sent(slot, planes_of, count):
        ref = win.at[pl.ds(0, planes_of), pl.ds(0, count)]
        remote(ref, ref, w_send.at[slot], p_recv.at[0], partner, t).wait_send()

    def local_w(u):
        return pltpu.make_async_copy(own_w(u), held_w(u, s), sem_local)

    def local_w_wait(count):
        ref = win.at[0, pl.ds(0, count)]
        pltpu.make_async_copy(ref, ref, sem_local).wait()

    def tok_cols(j):
        return tok.at[:, pl.ds(pl.multiple_of(j * feats, feats), feats)]

    def tok_local(j):
        return pltpu.make_async_copy(tok_cols(j), xr.at[j], sem_tok)

    def tok_local_wait():
        pltpu.make_async_copy(xr, xr, sem_tok).wait()

    def tok_quarter(of_half):
        start = of_half * (width // 2) + t * quarter
        return tok.at[:, pl.ds(pl.multiple_of(start, quarter), quarter)]

    def end_tok():
        return remote(tok_quarter(own_half), xq.at[0, t], t_send.at[0], t_recv.at[0], near, t)

    def mid_tok():
        return remote(tok_quarter(1 - own_half), xq.at[2, t], t_send.at[0], t_recv.at[2], opp, t)

    def to_stage(h):
        span = pl.ds(h * half, half)
        a = tok_quarter(1 - own_half).at[span]
        return remote(a, stage.at[span], t_send.at[1], t_recv.at[3 + h], near, t)

    def from_stage(h):
        span = pl.ds(h * half, half)
        return remote(stage.at[span], xq.at[1, t, span], t_send.at[1], t_recv.at[1], opp, t)

    def tok_arrived(i):
        remote(stage, stage, t_send.at[0], t_recv.at[i], partner, t).wait_recv()

    def part_sum(m, b):
        return remote(cbuf.at[m, b], cin.at[m, b], c_send, c_recv.at[m], opp, t)

    def part_sums(m):
        return remote(cbuf.at[m], cin.at[m], c_send, c_recv.at[m], opp, t)

    def squares_copy():
        return remote(ss.at[1], ss.at[0], s_send, s_recv, near, t)

    def end_part(h):
        return remote(
            gat_end.at[pl.ds(h * half, half)], gat.at[0, t, pl.ds(h * half, half)],
            e_send, e_recv.at[h], near, t,
        )

    class Gather:
        def __init__(self, g, buf, joint=False):
            self.g, self.buf, self.joint = g, buf, joint

        def part(self, block, h, k, target):
            size = self.buf.shape[1] // 2
            ref = self.buf.at[block, pl.ds(h * size, size)]
            slot = (0, 1, 2, 2, 2, 2)[k] if self.joint else (0, 1, 2, 2, 3, 3)[k]
            return remote(ref, ref, g_send.at[self.g], g_recv.at[self.g, slot], s, target)

        def whole(self, blocks, slot):
            ref = self.buf.at[pl.ds(0, blocks)]
            return remote(ref, ref, g_send.at[self.g], g_recv.at[self.g, slot], s, tx)

        def start(self, h):
            if h == 0:
                self.part(t, 0, 0, tx).start()
                self.part(t, 0, 3, ty).start()
            else:
                self.part(t, 1, 1, ty).start()
                self.part(t, 1, 2, tx).start()

        def start_all(self):
            self.part(t, 0, 0, tx).start()
            self.part(t, 1, 1, ty).start()
            self.part(t, 1, 2, tx).start()
            self.part(t, 0, 3, ty).start()

        def forward(self, h):
            if h == 0:
                self.part(tx, 0, 0, tx).wait_recv()
                self.part(tx, 0, 4, ty).start()
            else:
                self.part(ty, 1, 1, ty).wait_recv()
                self.part(ty, 1, 5, tx).start()

        def beside(self):
            self.whole(1, 2).wait_recv()

        def across(self):
            self.whole(1, 3).wait_recv()

        def rest(self):
            self.whole(2, 2).wait_recv()

        def drain(self):
            self.whole(3, 0).wait_send()

    gather_tok = (Gather(0, xq.at[0]), Gather(4, xq.at[1]), Gather(5, xq.at[2]))
    gather_gat = (Gather(1, gat.at[0], True), Gather(3, gat.at[1], True))
    gather_x = Gather(2, x1)

    def row_tiles(body):
        step = 64

        def tile(r, carry):
            body(pl.ds(pl.multiple_of(r * step, step), step))
            return carry

        lax.fori_loop(0, rows // step, tile, 0)

    def lane_sums(x):
        sq = x * x
        part = sq[:, :128]
        for q in range(1, x.shape[1] // 128):
            part = part + sq[:, 128 * q : 128 * (q + 1)]
        return part

    def squares(b):
        ss[b] = jnp.zeros(ss.shape[1:], f32)

        def one(j, carry):
            def body(span):
                ss[b, span, :] += lane_sums(xr[j, span, :].astype(f32))
            row_tiles(body)
            return carry

        lax.fori_loop(0, n_tp, one, 0)

    def scale(j):
        def body(span):
            x = x1[j, span, :].astype(f32)
            ss[0, span, :] += lane_sums(x)
            cols = pl.ds(pl.multiple_of(j * feats, feats), feats)
            scl[j, span, :] = (x * gain[1:2, cols]).astype(bf16)
        row_tiles(body)

    def scale_part(load, block, j):
        at = pl.multiple_of(j * quarter, quarter)
        cols = pl.ds(pl.multiple_of(own_half * (width // 2) + at, quarter), quarter)

        def body(span):
            sclh[block, span, pl.ds(at, quarter)] = (load(span).astype(f32) * gain[0:1, cols]).astype(bf16)
        row_tiles(body)

    def scale_sent(i, j):
        scale_part(lambda span: xq[i, j, span, :], (0, 2, 3)[i], j)

    def half_dot(m, block):
        depth = win.shape[2]
        sources = pl.ds(own_half * (n_sp // 2), n_sp // 2)
        w = win[m, sources].reshape(n_sp // 2 * depth, win.shape[3])
        return jnp.dot(sclh[block], w, preferred_element_type=f32)

    def send_part_sum(m, b):
        cbuf[m, b] = half_dot(m, 2 + b).astype(bf16)
        part_sum(m, b).start()

    def add_part_sums(m):
        part_sums(m).wait_recv()
        for b in range(2):
            acc[m, b] += cin[m, b].astype(f32)

    def project(m, sources, first):
        depth = win.shape[2]
        total = None
        for role in sources:
            z = lax.div(source_of[role], 2)
            w = win[3 + m, pl.ds(2 * z, 2)].reshape(2 * depth, win.shape[3])
            dot = jnp.dot(scl[z], w, preferred_element_type=f32)
            total = dot if total is None else total + dot
        if first:
            acc[m, 0] = total
        else:
            acc[m, 0] += total

    def inv_of(b):
        return lax.rsqrt(jnp.sum(ss[b], axis=-1, keepdims=True) / width + eps)

    def mix(b, slot):
        inv = inv_of(b)
        inner = (acc[INNER, b] * inv).astype(bf16)
        value = (acc[VALUE, b] * inv).astype(bf16)
        mixed[slot] = (inner.astype(f32) * value.astype(f32)).astype(bf16)

    def convolve(layer, b, slot):
        now = mixed[slot].astype(f32)
        tail = halo[slot].astype(f32)
        row = lax.broadcasted_iota(jnp.int32, now.shape, 0)
        one = jnp.where(row == 0, tail[15:16], pltpu.roll(now, 1, 0))
        two = pltpu.roll(now, 2, 0)
        two = jnp.where(row == 0, tail[14:15], jnp.where(row == 1, tail[15:16], two))
        acc[VALUE, b] = taps[0, layer : layer + 1] * two + taps[1, layer : layer + 1] * one + taps[2, layer : layer + 1] * now

    def gate(b):
        outer = (acc[OUTER, b] * inv_of(b)).astype(bf16).astype(f32)
        return (outer * acc[VALUE, b]).astype(bf16)

    def tail_copy(slot, to_slot, h, target):
        return remote(
            mixed.at[slot, pl.ds(rows - 16, 16)], halo.at[to_slot], h_send.at[slot], h_recv.at[h], target, t
        )

    def back_dot(layer, sources, cols):
        total = None
        for role in sources:
            z = lax.div(source_of[role], 2)
            w = wback[layer, pl.ds(2 * z, 2), :, cols].reshape(2 * wback.shape[2], cols.size)
            dot = jnp.dot(gat[layer, z], w, preferred_element_type=f32)
            total = dot if total is None else total + dot
        return total

    def by_columns(body):
        step = 256
        for c in range(feats // step):
            body(pl.ds(c * step, step))

    @pl.when(is_mid)
    def _():
        mid_tok().start()
        for u in FIRST + SHARED:
            send_partner(u)
        for u in SHARED:
            send_near(u)
        for j in range(n_tp):
            tok_local(j).start()
        for u in FIRST + SHARED:
            local_w(u).start()
        tok_local_wait()
        squares(1)

        def scale_own(j, carry):
            piece_of = own_half * (n_tp // 2) + lax.div(j, 2)
            cols = pl.ds(pl.multiple_of(lax.rem(j, 2) * quarter, quarter), quarter)
            scale_part(lambda span: xr[piece_of, span, cols], 1, j)
            return carry

        lax.fori_loop(0, n_tp, scale_own, 0)
        local_w_wait(units)
        own_end, far_end, far_mid = gather_tok
        for h in range(2):
            to_stage(h).wait_recv()
            from_stage(h).start()
        send_opp(BACK)
        send_opp(SECOND[0])
        tok_arrived(2)
        far_mid.start_all()
        scale_sent(2, t)
        far_mid.forward(0)
        far_mid.forward(1)
        tok_arrived(1)
        far_end.start_all()
        far_mid.beside()
        scale_sent(2, tx)
        scale_sent(2, ty)
        far_mid.across()
        scale_sent(2, td)
        relay_near(INNER)
        settle(INNER)
        send_part_sum(INNER, 1)
        far_end.forward(0)
        far_end.forward(1)
        relay_near(VALUE)
        settle(VALUE)
        send_part_sum(VALUE, 1)
        relay_opp(BACK)
        scale_sent(1, t)
        far_end.beside()
        scale_sent(1, tx)
        scale_sent(1, ty)
        relay_opp(SECOND[0])
        tok_arrived(0)
        own_end.start_all()
        scale_sent(0, t)
        far_end.across()
        scale_sent(1, td)
        send_part_sum(INNER, 0)
        send_part_sum(VALUE, 0)
        relay_near(OUTER)
        settle(OUTER)
        own_end.forward(0)
        own_end.forward(1)
        send_part_sum(OUTER, 0)
        send_part_sum(OUTER, 1)
        own_end.beside()
        scale_sent(0, tx)
        scale_sent(0, ty)
        own_end.across()
        scale_sent(0, td)
        for m in FIRST:
            for b in range(2):
                acc[m, b] = half_dot(m, b)
        add_part_sums(INNER)
        add_part_sums(VALUE)
        squares_copy().wait_recv()
        for b in range(2):
            mix(b, b)

        @pl.when(core == 0)
        def _():
            for b in range(2):
                tail_copy(b, b, b, partner).start()

        @pl.when(jnp.logical_and(core == 1, left))
        def _():
            tail_copy(1, 1, 1, s + 1).start()
            tail_copy(0, 1, 1, partner).start()

        @pl.when(jnp.logical_and(core == 1, jnp.logical_not(left)))
        def _():
            tail_copy(1, 0, 0, partner).start()
        relay_near(BACK)
        send_opp(SECOND[1])
        send_opp(SECOND[2])
        @pl.when(s == 2)
        def _():
            halo[0] = jnp.zeros(halo.shape[1:], bf16)

        @pl.when(s != 2)
        def _():
            tail_copy(0, 0, 0, partner).wait_recv()
        convolve(0, 0, 0)
        add_part_sums(OUTER)
        gat_end[...] = gate(0)
        for h in range(2):
            end_part(h).start()
        tail_copy(1, 1, 1, partner).wait_recv()
        convolve(0, 1, 1)
        gat[0, t] = gate(1)
        gather_gat[0].start_all()
        relay_far(BACK, (0,))
        gather_gat[0].forward(0)
        gather_gat[0].forward(1)
        relay_near(SECOND[0])
        relay_far(BACK, (1,))

    @pl.when(is_end)
    def _():
        for h in range(2):
            to_stage(h).start()
        send_near(INNER)
        send_near(VALUE)
        end_tok().start()
        send_near(OUTER)
        for j in range(n_tp):
            tok_local(j).start()
        for u in SHARED:
            send_partner(u)
        for u in SHARED:
            local_w(u).start()
        tok_local_wait()
        squares(1)
        squares_copy().start()
        for u in SHARED:
            send_near(u)
        local_w_wait(units - 3)
        for u in SHARED:
            relay_near(u)
        relay_opp(BACK)
        relay_opp(SECOND[0])
        for h in range(2):
            end_part(h).wait_recv()
            gather_gat[0].start(h)
        gather_gat[0].forward(0)
        relay_far(BACK, (0,))
        gather_gat[0].forward(1)
        relay_far(BACK, (1,))

    gather_gat[0].rest()
    settle(BACK)

    @pl.when(is_mid)
    def _():
        relay_opp(SECOND[1], (0,))

    def finish_first(cols):
        total = xr[t, :, cols].astype(f32) + back_dot(0, (OWN, NEAR, OPP, FAR), cols)
        x1[t, :, cols] = total.astype(bf16)

    by_columns(finish_first)
    gather_x.start_all()

    @pl.when(is_end)
    def _():
        relay_opp(SECOND[1], (0,))
    relay_opp(SECOND[1], (1,))

    @pl.when(is_mid)
    def _():
        relay_near(SECOND[1])
    ss[0] = jnp.zeros(ss.shape[1:], f32)
    scale(t)
    relay_opp(SECOND[2])

    @pl.when(is_mid)
    def _():
        relay_near(SECOND[2])
    gather_x.forward(0)
    gather_x.forward(1)
    relay_far(SECOND[0])
    gather_x.beside()
    scale(tx)
    scale(ty)
    relay_far(SECOND[1])
    gather_x.across()
    scale(td)
    settle(GROUP)
    def early_far(k):
        @pl.when(is_mid)
        def _():
            relay_far(SECOND[2], (k,))

    last = SECOND[3]

    @pl.when(is_mid)
    def _():
        send_opp(last, (0, 1))
    early_far(0)
    settle(GROUP + 1)
    project(INNER, (OWN, NEAR, OPP, FAR), True)
    early_far(1)
    project(VALUE, (OWN, NEAR, OPP), True)
    settle(GROUP + 2)
    project(VALUE, (FAR,), False)
    early_far(2)
    mix(0, 2)

    @pl.when(s < n_sp - 1)
    def _():
        tail_copy(2, 2, 2, s + 1).start()

    @pl.when(is_mid)
    def _():
        send_opp(last, (2, 3))
        relay_near(last)
    project(OUTER, (OWN, NEAR, OPP), True)

    @pl.when(is_end)
    def _():
        relay_far(SECOND[2], (0, 1, 2))
    relay_far(SECOND[2], (3,))

    @pl.when(is_mid)
    def _():
        relay_opp(last)

    @pl.when(s == 0)
    def _():
        halo[2] = jnp.zeros(halo.shape[1:], bf16)

    @pl.when(s > 0)
    def _():
        tail_copy(2, 2, 2, partner).wait_recv()
    convolve(1, 0, 2)
    settle(GROUP + 3)
    project(OUTER, (FAR,), False)
    gat[1, t] = gate(0)
    gather_gat[1].start_all()

    @pl.when(is_end)
    def _():
        relay_opp(last, (0, 1))

    @pl.when(is_mid)
    def _():
        relay_far(last, (0, 1))
    gather_gat[1].forward(0)
    gather_gat[1].forward(1)

    @pl.when(is_end)
    def _():
        relay_opp(last, (2, 3))

    @pl.when(is_mid)
    def _():
        relay_far(last, (2, 3))
    gather_gat[1].rest()
    settle(last)

    def start_last(cols):
        bacc[:, cols] = x1[t, :, cols].astype(f32) + back_dot(1, (OWN, NEAR, OPP), cols)

    by_columns(start_last)

    @pl.when(is_end)
    def _():
        relay_far(last)
    settle(GROUP + 4)

    def finish_last(cols):
        out[:, cols] = (bacc[:, cols] + back_dot(1, (FAR,), cols)).astype(bf16)

    by_columns(finish_last)

    some = units - 3

    @pl.when(is_mid)
    def _():
        sent(0, 2, units)
        sent(1, some, 7)
        for g in gather_tok:
            g.drain()
        for i in range(2):
            remote(stage, stage, t_send.at[i], t_recv.at[0], partner, t).wait_send()
        remote(cbuf, cin, c_send, c_recv.at[0], partner, t).wait_send()
        remote(gat_end, gat_end, e_send, e_recv.at[0], partner, t).wait_send()

        @pl.when(core == 0)
        def _():
            for b in range(2):
                tail_copy(b, b, b, partner).wait_send()

        @pl.when(jnp.logical_and(core == 1, left))
        def _():
            tail_copy(0, 1, 1, partner).wait_send()
            tail_copy(1, 1, 1, s + 1).wait_send()

        @pl.when(jnp.logical_and(core == 1, jnp.logical_not(left)))
        def _():
            tail_copy(1, 0, 0, partner).wait_send()

    @pl.when(is_end)
    def _():
        sent(0, 2, some)
        sent(1, 3, 6)
        for i in range(2):
            remote(stage, stage, t_send.at[i], t_recv.at[0], partner, t).wait_send()
        squares_copy().wait_send()
    gather_gat[0].drain()
    gather_x.drain()
    gather_gat[1].drain()

    @pl.when(s < n_sp - 1)
    def _():
        tail_copy(2, 2, 2, partner).wait_send()


def fused(tokens, norm_gain, w_outer, w_inner, w_value, w_back, taps):
    n_sp, n_tp = lax.axis_size("sp"), lax.axis_size("tp")
    rows, width = tokens.shape
    layers, depth, chans = w_outer.shape
    back_rows, feats = w_back.shape[1:]
    if 4 * layers != len(PIECES):
        return per_device(tokens, norm_gain, w_outer, w_inner, w_value, w_back, taps)
    chunks = 3 + 3 * sum(PIECES[BACK:])
    dma = pltpu.SemaphoreType.DMA
    hbm, vmem = pl.BlockSpec(memory_space=pl.ANY), pl.BlockSpec(memory_space=pltpu.VMEM)
    held = [
        pltpu.with_memory_space_constraint(a, pltpu.HBM)
        for a in (tokens, norm_gain, w_outer, w_inner, w_value, w_back, taps.transpose(1, 0, 2))
    ]
    return pl.pallas_call(
        mixer_kernel,
        out_shape=jax.ShapeDtypeStruct((rows, feats), bf16),
        in_specs=[hbm] * 7,
        out_specs=vmem,
        scratch_shapes=[
            pltpu.VMEM((layers, width), f32),
            pltpu.VMEM(taps.shape[1:2] + taps.shape[:1] + taps.shape[2:], f32),
            pltpu.VMEM((n_tp, rows, feats), bf16),
            pltpu.VMEM((3, n_tp, rows, width // 2 // n_tp), bf16),
            pltpu.VMEM((rows, width // 2 // n_tp), bf16),
            pltpu.VMEM((n_tp, rows, feats), bf16),
            pltpu.VMEM((n_tp, rows, feats), bf16),
            pltpu.VMEM((4, rows, width // 2), bf16),
            pltpu.VMEM((3, 2, rows, chans), bf16),
            pltpu.VMEM((3, 2, rows, chans), bf16),
            pltpu.VMEM((3 * layers, n_sp, depth, chans), bf16),
            pltpu.VMEM((layers, n_sp, back_rows, feats), bf16),
            pltpu.VMEM((3, 2, rows, chans), f32),
            pltpu.VMEM((rows, feats), f32),
            pltpu.VMEM((2, rows, 128), f32),
            pltpu.VMEM((layers, n_tp, rows, chans), bf16),
            pltpu.VMEM((rows, chans), bf16),
            pltpu.VMEM((3, rows, chans), bf16),
            pltpu.VMEM((3, 16, chans), bf16),
            dma((2,)),
            dma,
            dma,
            dma((2,)),
            dma((5,)),
            dma,
            dma((3,)),
            dma,
            dma,
            dma((2,)),
            dma((chunks,)),
            dma((GROUP + 5,)),
            dma((6,)),
            dma((6, 4)),
            dma((3,)),
            dma((3,)),
            dma,
            dma((2,)),
        ],
        compiler_params=pltpu.CompilerParams(
            collective_id=0, has_side_effects=True, vmem_limit_bytes=48 * 1024 * 1024
        ),
        name="mixer",
    )(*held)


def solution(mesh):
    in_specs = (
        P("sp", None),
        P(),
        P(None, "sp", "tp"),
        P(None, "sp", "tp"),
        P(None, "sp", "tp"),
        P(None, "sp", "tp"),
        P(None, None, "tp"),
    )
    out_specs = P("sp", "tp")
    body = fused if (mesh.shape["sp"], mesh.shape["tp"]) == (8, 4) else per_device
    return jax.shard_map(
        body, mesh=mesh, in_specs=in_specs, out_specs=out_specs, check_vma=False
    )
```

```python
import functools

import jax
import jax.numpy as jnp
from jax import lax
from jax.experimental import pallas as pl
from jax.experimental.pallas import tpu as pltpu
from jax.sharding import PartitionSpec as P

MESH = pl.DeviceIdType.MESH
f32 = jnp.float32
bf16 = jnp.bfloat16

eps = 1e-06

OUTER, INNER, VALUE, BACK = 0, 1, 2, 3
FIRST = (INNER, VALUE, OUTER)
SECOND = tuple(4 + m for m in FIRST + (BACK,))
SHARED = (BACK,) + SECOND
PIECES = (1, 1, 1, 2, 4, 2, 2, 4)
GROUP = 8


def shifted(block, axis, distance):
    devices = range(lax.axis_size(axis))
    route = [(i - distance, i) for i in devices if i - distance in devices]
    return lax.ppermute(block, axis, route)


def per_device(tokens, norm_gain, w_outer, w_inner, w_value, w_back, taps):
    layers = w_outer.shape[0]
    count = tokens.shape[0]
    feats = w_back.shape[2]
    own = lax.axis_index("tp")
    held = (
        lax.all_gather(w_outer, "sp", axis=1, tiled=True),
        lax.all_gather(w_inner, "sp", axis=1, tiled=True),
        lax.all_gather(w_value, "sp", axis=1, tiled=True),
        lax.all_gather(w_back, "sp", axis=1, tiled=True),
    )
    current = tokens
    resid = lax.dynamic_slice_in_dim(tokens, own * feats, feats, 1)
    for layer in range(layers):
        if layer > 0:
            current = lax.all_gather(resid, "tp", axis=1, tiled=True)
        xf = current.astype(jnp.float32)
        normed = (
            xf * lax.rsqrt(jnp.mean(xf * xf, axis=-1, keepdims=True) + eps) * norm_gain[layer]
        ).astype(jnp.bfloat16)
        outer = jnp.dot(normed, held[0][layer], preferred_element_type=jnp.float32)
        inner = jnp.dot(normed, held[1][layer], preferred_element_type=jnp.float32)
        value = jnp.dot(normed, held[2][layer], preferred_element_type=jnp.float32)
        outer = outer.astype(jnp.bfloat16)
        inner = inner.astype(jnp.bfloat16)
        value = value.astype(jnp.bfloat16)
        mixed = (inner.astype(jnp.float32) * value.astype(jnp.float32)).astype(jnp.bfloat16)
        before = shifted(mixed[count - 2 :], "sp", 1)
        padded = jnp.concatenate([before, mixed], axis=0).astype(jnp.float32)
        conv = (
            taps[layer, 0] * padded[:count]
            + taps[layer, 1] * padded[1 : count + 1]
            + taps[layer, 2] * padded[2:]
        )
        gated = (outer.astype(jnp.float32) * conv).astype(jnp.bfloat16)
        whole = lax.all_gather(gated, "tp", axis=1, tiled=True)
        proj = jnp.dot(whole, held[3][layer], preferred_element_type=jnp.float32)
        resid = (resid.astype(jnp.float32) + proj).astype(jnp.bfloat16)
    return resid


def chunk(u, k, role):
    if u < BACK:
        return u
    return 3 + 3 * (sum(PIECES[BACK:u]) + k) + role - 1


def mixer_kernel(
    tok, gain_hbm, w_outer, w_inner, w_value, w_back, taps_hbm, out,
    gain, taps, xr, xq, stage, x1, scl, sclh, cbuf, cin, win, wback, acc, bacc, ss, gat, gat_end, mixed, halo,
    sem_small, sem_local, sem_tok, t_send, t_recv, c_send, c_recv, s_send, s_recv, w_send, w_recv, p_recv,
    g_send, g_recv, h_send, h_recv, e_send, e_recv,
):
    s, t = lax.axis_index("sp"), lax.axis_index("tp")
    n_sp, n_tp = win.shape[1], xr.shape[0]
    rows, feats = xr.shape[1:]
    quarter = xq.shape[3]
    half = rows // 2
    width = feats * n_tp
    units = len(PIECES)
    core = lax.rem(s, 2)
    flip = 1 - 2 * core
    left = s < n_sp // 2
    side = jnp.where(left, 1, -1)
    own_half = jnp.where(left, 0, 1)
    plane = lax.div(s, 2)
    planes = n_sp // 2
    is_end = jnp.logical_or(plane == 0, plane == planes - 1)
    is_mid = jnp.logical_not(is_end)
    partner = s + flip
    near = jnp.where(is_mid, s - 2 * side, s + 2 * side)
    opp = jnp.where(is_mid, s + 2 * side, s + 4 * side)
    far = jnp.where(is_mid, s + 4 * side, s + 6 * side)
    tx = t + 1 - 2 * lax.rem(t, 2)
    ty = t + 2 - 4 * lax.div(t, 2)
    td = n_tp - 1 - t

    small = (
        pltpu.make_async_copy(gain_hbm, gain, sem_small.at[0]),
        pltpu.make_async_copy(taps_hbm, taps, sem_small.at[1]),
    )

    ahead = (1 - own_half) * (n_tp // 2) + lax.div(t, 2)
    ahead_cols = pl.ds(pl.multiple_of(lax.rem(t, 2) * quarter, quarter), quarter)

    def tok_local(i):
        j = lax.rem(ahead + i, n_tp)
        cols = pl.ds(pl.multiple_of(j * feats, feats), feats)
        return pltpu.make_async_copy(tok.at[:, cols], xr.at[j], sem_tok.at[min(i, 1)])

    def tok_local_wait(slot, count):
        ref = xr.at[pl.ds(0, count)]
        pltpu.make_async_copy(ref, ref, sem_tok.at[slot]).wait()

    for i in range(n_tp):
        tok_local(i).start()
    for copy in small:
        copy.start()
    barrier = pltpu.get_barrier_semaphore()

    def greet(sp, tp):
        pl.semaphore_signal(barrier, inc=1, device_id=(sp, tp), device_id_type=MESH)

    greet(partner, t)
    greet(s, tx)
    greet(s, ty)
    greet(near, t)
    greet(near + flip, t)

    @pl.when(is_mid)
    def _():
        greet(opp, t)
        greet(opp + flip, t)
    pl.semaphore_wait(barrier, jnp.where(is_mid, 7, 5))
    for copy in small:
        copy.wait()

    projections = (w_outer, w_inner, w_value)

    def own_w(u):
        layer, m = u // 4, u % 4
        return projections[m].at[layer] if m < 3 else w_back.at[layer]

    def held_w(u, source):
        layer, m = u // 4, u % 4
        return win.at[3 * layer + m, source] if m < 3 else wback.at[layer, source]

    def remote(a, b, ssem, rsem, sp, tp):
        return pltpu.make_async_remote_copy(
            src_ref=a, dst_ref=b, send_sem=ssem, recv_sem=rsem, device_id=(sp, tp), device_id_type=MESH
        )

    def piece(ref, u, k):
        size = ref.shape[0] // PIECES[u]
        return ref.at[pl.ds(k * size, size)]

    OWN, NEAR, OPP, FAR = 0, 1, 2, 3
    source_of = (s, near, opp, far)

    def w_copy(u, k, role, kind, to_role, target):
        to = piece(held_w(u, source_of[role]), u, k)
        a = piece(own_w(u), u, k) if role == OWN else to
        return remote(a, to, w_send.at[min(kind // 2, 1)], w_recv.at[chunk(u, k, to_role)], target, t)

    def to_partner(u, k, role):
        to = piece(held_w(u, source_of[role]), u, k)
        a = piece(own_w(u), u, k) if role == OWN else to
        return remote(a, to, w_send.at[role // 2], p_recv.at[group_of(u, role)], partner, t)

    def pieces_of(u):
        return range(PIECES[u])

    def arrived(u, k, role):
        to = piece(held_w(u, source_of[role]), u, k)
        remote(to, to, w_send.at[0], w_recv.at[chunk(u, k, role)], partner, t).wait_recv()

    def send_opp(u, ks=None):
        for k in ks or pieces_of(u):
            w_copy(u, k, OWN, 4, OPP, opp).start()

    def send_near(u):
        for k in pieces_of(u):
            w_copy(u, k, OWN, 5, NEAR, near).start()

    def send_partner(u):
        for k in pieces_of(u):
            to_partner(u, k, OWN).start()

    def relay_near(u, ks=None):
        for k in ks or pieces_of(u):
            arrived(u, k, NEAR)

            if u >= 3:
                @pl.when(is_mid)
                def _():
                    w_copy(u, k, NEAR, 6, FAR, opp).start()
            to_partner(u, k, NEAR).start()

    def relay_across(u, role, ks=None):
        for k in ks or pieces_of(u):
            arrived(u, k, role)

            @pl.when(is_mid)
            def _():
                w_copy(u, k, role, 5 + role, role, near).start()
            to_partner(u, k, role).start()

    def relay_opp(u, ks=None):
        relay_across(u, OPP, ks)

    def relay_far(u, ks=None):
        relay_across(u, FAR, ks)

    counts = {INNER: 2, VALUE: 2, OUTER: 2, BACK: 4, GROUP: 9, GROUP + 1: 1, GROUP + 2: 1, GROUP + 3: 1, 7: 3, GROUP + 4: 1}

    def group_of(u, role):
        if u <= BACK:
            return u
        if u == 7:
            return GROUP + 4 if role == FAR else 7
        return GROUP + 1 + SECOND.index(u) if role == FAR else GROUP

    def settle(group):
        count = counts[group]
        ref = win.at[pl.ds(0, 3), pl.ds(0, 3)] if count == 9 else win.at[0, pl.ds(0, count)]
        remote(ref, ref, w_send.at[0], p_recv.at[group], partner, t).wait_recv()

    def sent(slot, planes_of, count):
        ref = win.at[pl.ds(0, planes_of), pl.ds(0, count)]
        remote(ref, ref, w_send.at[slot], p_recv.at[0], partner, t).wait_send()

    def local_w(u):
        return pltpu.make_async_copy(own_w(u), held_w(u, s), sem_local)

    def local_w_wait(count):
        ref = win.at[0, pl.ds(0, count)]
        pltpu.make_async_copy(ref, ref, sem_local).wait()

    def tok_quarter(of_half):
        start = of_half * (width // 2) + t * quarter
        return tok.at[:, pl.ds(pl.multiple_of(start, quarter), quarter)]

    def end_tok():
        return remote(tok_quarter(own_half), xq.at[0, t], t_send.at[0], t_recv.at[0], near, t)

    def mid_tok():
        return remote(xr.at[ahead, :, ahead_cols], xq.at[2, t], t_send.at[0], t_recv.at[2], opp, t)

    def to_stage(h):
        span = pl.ds(h * half, half)
        a = xr.at[ahead, span, ahead_cols]
        return remote(a, stage.at[span], t_send.at[1], t_recv.at[3 + h], near, t)

    def from_stage(h):
        span = pl.ds(h * half, half)
        return remote(stage.at[span], xq.at[1, t, span], t_send.at[1], t_recv.at[1], opp, t)

    def tok_arrived(i):
        remote(stage, stage, t_send.at[0], t_recv.at[i], partner, t).wait_recv()

    def part_sum(m, b):
        return remote(cbuf.at[m, b], cin.at[m, b], c_send, c_recv.at[m], opp, t)

    def part_sums(m):
        return remote(cbuf.at[m], cin.at[m], c_send, c_recv.at[m], opp, t)

    def squares_copy():
        return remote(ss.at[1], ss.at[0], s_send, s_recv, near, t)

    def end_part(h):
        return remote(
            gat_end.at[pl.ds(h * half, half)], gat.at[0, t, pl.ds(h * half, half)],
            e_send, e_recv.at[h], near, t,
        )

    class Gather:
        def __init__(self, g, buf, joint=False):
            self.g, self.buf, self.joint = g, buf, joint

        def part(self, block, h, k, target):
            size = self.buf.shape[1] // 2
            ref = self.buf.at[block, pl.ds(h * size, size)]
            slot = (0, 1, 2, 2, 2, 2)[k] if self.joint else (0, 1, 2, 2, 3, 3)[k]
            return remote(ref, ref, g_send.at[self.g], g_recv.at[self.g, slot], s, target)

        def whole(self, blocks, slot):
            ref = self.buf.at[pl.ds(0, blocks)]
            return remote(ref, ref, g_send.at[self.g], g_recv.at[self.g, slot], s, tx)

        def start(self, h):
            if h == 0:
                self.part(t, 0, 0, tx).start()
                self.part(t, 0, 3, ty).start()
            else:
                self.part(t, 1, 1, ty).start()
                self.part(t, 1, 2, tx).start()

        def start_all(self):
            self.part(t, 0, 0, tx).start()
            self.part(t, 1, 1, ty).start()
            self.part(t, 1, 2, tx).start()
            self.part(t, 0, 3, ty).start()

        def forward(self, h):
            if h == 0:
                self.part(tx, 0, 0, tx).wait_recv()
                self.part(tx, 0, 4, ty).start()
            else:
                self.part(ty, 1, 1, ty).wait_recv()
                self.part(ty, 1, 5, tx).start()

        def beside(self):
            self.whole(1, 2).wait_recv()

        def across(self):
            self.whole(1, 3).wait_recv()

        def rest(self):
            self.whole(2, 2).wait_recv()

        def drain(self):
            self.whole(3, 0).wait_send()

    gather_tok = (Gather(0, xq.at[0]), Gather(4, xq.at[1]), Gather(5, xq.at[2]))
    gather_gat = (Gather(1, gat.at[0], True), Gather(3, gat.at[1], True))
    gather_x = Gather(2, x1)

    def row_tiles(body):
        step = 64

        def tile(r, carry):
            body(pl.ds(pl.multiple_of(r * step, step), step))
            return carry

        lax.fori_loop(0, rows // step, tile, 0)

    def lane_sums(x):
        sq = x * x
        part = sq[:, :128]
        for q in range(1, x.shape[1] // 128):
            part = part + sq[:, 128 * q : 128 * (q + 1)]
        return part

    def squares(b):
        ss[b] = jnp.zeros(ss.shape[1:], f32)

        def one(j, carry):
            def body(span):
                ss[b, span, :] += lane_sums(xr[j, span, :].astype(f32))
            row_tiles(body)
            return carry

        lax.fori_loop(0, n_tp, one, 0)

    def scale(j):
        def body(span):
            x = x1[j, span, :].astype(f32)
            ss[0, span, :] += lane_sums(x)
            cols = pl.ds(pl.multiple_of(j * feats, feats), feats)
            scl[j, span, :] = (x * gain[1:2, cols]).astype(bf16)
        row_tiles(body)

    def scale_part(load, block, j):
        at = pl.multiple_of(j * quarter, quarter)
        cols = pl.ds(pl.multiple_of(own_half * (width // 2) + at, quarter), quarter)

        def body(span):
            sclh[block, span, pl.ds(at, quarter)] = (load(span).astype(f32) * gain[0:1, cols]).astype(bf16)
        row_tiles(body)

    def scale_sent(i, j):
        scale_part(lambda span: xq[i, j, span, :], (0, 2, 3)[i], j)

    def half_dot(m, block):
        depth = win.shape[2]
        sources = pl.ds(own_half * (n_sp // 2), n_sp // 2)
        w = win[m, sources].reshape(n_sp // 2 * depth, win.shape[3])
        return jnp.dot(sclh[block], w, preferred_element_type=f32)

    def send_part_sum(m, b):
        cbuf[m, b] = half_dot(m, 2 + b).astype(bf16)
        part_sum(m, b).start()

    def add_part_sums(m):
        part_sums(m).wait_recv()
        for b in range(2):
            acc[m, b] += cin[m, b].astype(f32)

    def project(m, sources, first):
        depth = win.shape[2]
        total = None
        for role in sources:
            z = lax.div(source_of[role], 2)
            w = win[3 + m, pl.ds(2 * z, 2)].reshape(2 * depth, win.shape[3])
            dot = jnp.dot(scl[z], w, preferred_element_type=f32)
            total = dot if total is None else total + dot
        if first:
            acc[m, 0] = total
        else:
            acc[m, 0] += total

    def inv_of(b):
        return lax.rsqrt(jnp.sum(ss[b], axis=-1, keepdims=True) / width + eps)

    def mix(b, slot):
        inv = inv_of(b)
        inner = (acc[INNER, b] * inv).astype(bf16)
        value = (acc[VALUE, b] * inv).astype(bf16)
        mixed[slot] = (inner.astype(f32) * value.astype(f32)).astype(bf16)

    def convolve(layer, b, slot):
        now = mixed[slot].astype(f32)
        tail = halo[slot].astype(f32)
        row = lax.broadcasted_iota(jnp.int32, now.shape, 0)
        one = jnp.where(row == 0, tail[15:16], pltpu.roll(now, 1, 0))
        two = pltpu.roll(now, 2, 0)
        two = jnp.where(row == 0, tail[14:15], jnp.where(row == 1, tail[15:16], two))
        acc[VALUE, b] = taps[0, layer : layer + 1] * two + taps[1, layer : layer + 1] * one + taps[2, layer : layer + 1] * now

    def gate(b):
        outer = (acc[OUTER, b] * inv_of(b)).astype(bf16).astype(f32)
        return (outer * acc[VALUE, b]).astype(bf16)

    def tail_copy(slot, to_slot, h, target):
        return remote(
            mixed.at[slot, pl.ds(rows - 16, 16)], halo.at[to_slot], h_send.at[slot], h_recv.at[h], target, t
        )

    def back_dot(layer, sources, cols):
        total = None
        for role in sources:
            z = lax.div(source_of[role], 2)
            w = wback[layer, pl.ds(2 * z, 2), :, cols].reshape(2 * wback.shape[2], cols.size)
            dot = jnp.dot(gat[layer, z], w, preferred_element_type=f32)
            total = dot if total is None else total + dot
        return total

    def by_columns(body):
        step = 256
        for c in range(feats // step):
            body(pl.ds(c * step, step))

    @pl.when(is_mid)
    def _():
        tok_local_wait(0, 1)
        mid_tok().start()
        for u in FIRST + SHARED:
            send_partner(u)
        for u in SHARED:
            send_near(u)
        for u in FIRST + SHARED:
            local_w(u).start()
        tok_local_wait(1, n_tp - 1)
        squares(1)

        def scale_own(j, carry):
            piece_of = own_half * (n_tp // 2) + lax.div(j, 2)
            cols = pl.ds(pl.multiple_of(lax.rem(j, 2) * quarter, quarter), quarter)
            scale_part(lambda span: xr[piece_of, span, cols], 1, j)
            return carry

        lax.fori_loop(0, n_tp, scale_own, 0)
        local_w_wait(units)
        own_end, far_end, far_mid = gather_tok
        for h in range(2):
            to_stage(h).wait_recv()
            from_stage(h).start()
        send_opp(BACK)
        send_opp(SECOND[0])
        tok_arrived(2)
        far_mid.start_all()
        scale_sent(2, t)
        far_mid.forward(0)
        far_mid.forward(1)
        tok_arrived(1)
        far_end.start_all()
        far_mid.beside()
        scale_sent(2, tx)
        scale_sent(2, ty)
        far_mid.across()
        scale_sent(2, td)
        relay_near(INNER)
        settle(INNER)
        send_part_sum(INNER, 1)
        far_end.forward(0)
        far_end.forward(1)
        relay_near(VALUE)
        settle(VALUE)
        send_part_sum(VALUE, 1)
        relay_opp(BACK)
        scale_sent(1, t)
        far_end.beside()
        scale_sent(1, tx)
        scale_sent(1, ty)
        relay_opp(SECOND[0])
        tok_arrived(0)
        own_end.start_all()
        scale_sent(0, t)
        far_end.across()
        scale_sent(1, td)
        send_part_sum(INNER, 0)
        send_part_sum(VALUE, 0)
        relay_near(OUTER)
        settle(OUTER)
        own_end.forward(0)
        own_end.forward(1)
        send_part_sum(OUTER, 0)
        send_part_sum(OUTER, 1)
        own_end.beside()
        scale_sent(0, tx)
        scale_sent(0, ty)
        own_end.across()
        scale_sent(0, td)
        for m in FIRST:
            for b in range(2):
                acc[m, b] = half_dot(m, b)
        add_part_sums(INNER)
        add_part_sums(VALUE)
        squares_copy().wait_recv()
        for b in range(2):
            mix(b, b)

        @pl.when(core == 0)
        def _():
            for b in range(2):
                tail_copy(b, b, b, partner).start()

        @pl.when(jnp.logical_and(core == 1, left))
        def _():
            tail_copy(1, 1, 1, s + 1).start()
            tail_copy(0, 1, 1, partner).start()

        @pl.when(jnp.logical_and(core == 1, jnp.logical_not(left)))
        def _():
            tail_copy(1, 0, 0, partner).start()
        relay_near(BACK)
        send_opp(SECOND[1])
        send_opp(SECOND[2])
        @pl.when(s == 2)
        def _():
            halo[0] = jnp.zeros(halo.shape[1:], bf16)

        @pl.when(s != 2)
        def _():
            tail_copy(0, 0, 0, partner).wait_recv()
        convolve(0, 0, 0)
        add_part_sums(OUTER)
        gat_end[...] = gate(0)
        for h in range(2):
            end_part(h).start()
        tail_copy(1, 1, 1, partner).wait_recv()
        convolve(0, 1, 1)
        gat[0, t] = gate(1)
        gather_gat[0].start_all()
        relay_far(BACK, (0,))
        gather_gat[0].forward(0)
        gather_gat[0].forward(1)
        relay_near(SECOND[0])
        relay_far(BACK, (1,))

    @pl.when(is_end)
    def _():
        tok_local_wait(0, 1)
        for h in range(2):
            to_stage(h).start()
        send_near(INNER)
        send_near(VALUE)
        end_tok().start()
        send_near(OUTER)
        for u in SHARED:
            send_partner(u)
        for u in SHARED:
            local_w(u).start()
        tok_local_wait(1, n_tp - 1)
        squares(1)
        squares_copy().start()
        for u in SHARED:
            send_near(u)
        local_w_wait(units - 3)
        for u in SHARED:
            relay_near(u)
        relay_opp(BACK)
        relay_opp(SECOND[0])
        for h in range(2):
            end_part(h).wait_recv()
            gather_gat[0].start(h)
        gather_gat[0].forward(0)
        relay_far(BACK, (0,))
        gather_gat[0].forward(1)
        relay_far(BACK, (1,))

    gather_gat[0].rest()
    settle(BACK)

    @pl.when(is_mid)
    def _():
        relay_opp(SECOND[1], (0,))

    def finish_first(cols):
        total = xr[t, :, cols].astype(f32) + back_dot(0, (OWN, NEAR, OPP, FAR), cols)
        x1[t, :, cols] = total.astype(bf16)

    by_columns(finish_first)
    gather_x.start_all()

    @pl.when(is_end)
    def _():
        relay_opp(SECOND[1], (0,))
    relay_opp(SECOND[1], (1,))

    @pl.when(is_mid)
    def _():
        relay_near(SECOND[1])
    ss[0] = jnp.zeros(ss.shape[1:], f32)
    scale(t)
    relay_opp(SECOND[2])

    @pl.when(is_mid)
    def _():
        relay_near(SECOND[2])
    gather_x.forward(0)
    gather_x.forward(1)
    relay_far(SECOND[0])
    gather_x.beside()
    scale(tx)
    scale(ty)
    relay_far(SECOND[1])
    gather_x.across()
    scale(td)
    settle(GROUP)
    def early_far(k):
        @pl.when(is_mid)
        def _():
            relay_far(SECOND[2], (k,))

    last = SECOND[3]

    @pl.when(is_mid)
    def _():
        send_opp(last, (0, 1))
    early_far(0)
    settle(GROUP + 1)
    project(INNER, (OWN, NEAR, OPP, FAR), True)
    early_far(1)
    project(VALUE, (OWN, NEAR, OPP), True)
    settle(GROUP + 2)
    project(VALUE, (FAR,), False)
    early_far(2)
    mix(0, 2)

    @pl.when(s < n_sp - 1)
    def _():
        tail_copy(2, 2, 2, s + 1).start()

    @pl.when(is_mid)
    def _():
        send_opp(last, (2, 3))
        relay_near(last)
    project(OUTER, (OWN, NEAR, OPP), True)

    @pl.when(is_end)
    def _():
        relay_far(SECOND[2], (0, 1, 2))
    relay_far(SECOND[2], (3,))

    @pl.when(is_mid)
    def _():
        relay_opp(last)

    @pl.when(s == 0)
    def _():
        halo[2] = jnp.zeros(halo.shape[1:], bf16)

    @pl.when(s > 0)
    def _():
        tail_copy(2, 2, 2, partner).wait_recv()
    convolve(1, 0, 2)
    settle(GROUP + 3)
    project(OUTER, (FAR,), False)
    gat[1, t] = gate(0)
    gather_gat[1].start_all()

    @pl.when(is_end)
    def _():
        relay_opp(last, (0, 1))

    @pl.when(is_mid)
    def _():
        relay_far(last, (0, 1))
    gather_gat[1].forward(0)
    gather_gat[1].forward(1)

    @pl.when(is_end)
    def _():
        relay_opp(last, (2, 3))
        relay_far(last, (0, 1))

    @pl.when(is_mid)
    def _():
        relay_far(last, (2, 3))
    gather_gat[1].rest()
    settle(last)

    def start_last(cols):
        bacc[:, cols] = x1[t, :, cols].astype(f32) + back_dot(1, (OWN, NEAR, OPP), cols)

    by_columns(start_last)

    @pl.when(is_end)
    def _():
        relay_far(last, (2, 3))
    settle(GROUP + 4)

    def finish_last(cols):
        out[:, cols] = (bacc[:, cols] + back_dot(1, (FAR,), cols)).astype(bf16)

    by_columns(finish_last)

    some = units - 3

    @pl.when(is_mid)
    def _():
        sent(0, 2, units)
        sent(1, some, 7)
        for g in gather_tok:
            g.drain()
        for i in range(2):
            remote(stage, stage, t_send.at[i], t_recv.at[0], partner, t).wait_send()
        remote(cbuf, cin, c_send, c_recv.at[0], partner, t).wait_send()
        remote(gat_end, gat_end, e_send, e_recv.at[0], partner, t).wait_send()

        @pl.when(core == 0)
        def _():
            for b in range(2):
                tail_copy(b, b, b, partner).wait_send()

        @pl.when(jnp.logical_and(core == 1, left))
        def _():
            tail_copy(0, 1, 1, partner).wait_send()
            tail_copy(1, 1, 1, s + 1).wait_send()

        @pl.when(jnp.logical_and(core == 1, jnp.logical_not(left)))
        def _():
            tail_copy(1, 0, 0, partner).wait_send()

    @pl.when(is_end)
    def _():
        sent(0, 2, some)
        sent(1, 3, 6)
        for i in range(2):
            remote(stage, stage, t_send.at[i], t_recv.at[0], partner, t).wait_send()
        squares_copy().wait_send()
    gather_gat[0].drain()
    gather_x.drain()
    gather_gat[1].drain()

    @pl.when(s < n_sp - 1)
    def _():
        tail_copy(2, 2, 2, partner).wait_send()


def fused(tokens, norm_gain, w_outer, w_inner, w_value, w_back, taps):
    n_sp, n_tp = lax.axis_size("sp"), lax.axis_size("tp")
    rows, width = tokens.shape
    layers, depth, chans = w_outer.shape
    back_rows, feats = w_back.shape[1:]
    if 4 * layers != len(PIECES):
        return per_device(tokens, norm_gain, w_outer, w_inner, w_value, w_back, taps)
    chunks = 3 + 3 * sum(PIECES[BACK:])
    dma = pltpu.SemaphoreType.DMA
    hbm, vmem = pl.BlockSpec(memory_space=pl.ANY), pl.BlockSpec(memory_space=pltpu.VMEM)
    held = [
        pltpu.with_memory_space_constraint(a, pltpu.HBM)
        for a in (tokens, norm_gain, w_outer, w_inner, w_value, w_back, taps.transpose(1, 0, 2))
    ]
    return pl.pallas_call(
        mixer_kernel,
        out_shape=jax.ShapeDtypeStruct((rows, feats), bf16),
        in_specs=[hbm] * 7,
        out_specs=vmem,
        scratch_shapes=[
            pltpu.VMEM((layers, width), f32),
            pltpu.VMEM(taps.shape[1:2] + taps.shape[:1] + taps.shape[2:], f32),
            pltpu.VMEM((n_tp, rows, feats), bf16),
            pltpu.VMEM((3, n_tp, rows, width // 2 // n_tp), bf16),
            pltpu.VMEM((rows, width // 2 // n_tp), bf16),
            pltpu.VMEM((n_tp, rows, feats), bf16),
            pltpu.VMEM((n_tp, rows, feats), bf16),
            pltpu.VMEM((4, rows, width // 2), bf16),
            pltpu.VMEM((3, 2, rows, chans), bf16),
            pltpu.VMEM((3, 2, rows, chans), bf16),
            pltpu.VMEM((3 * layers, n_sp, depth, chans), bf16),
            pltpu.VMEM((layers, n_sp, back_rows, feats), bf16),
            pltpu.VMEM((3, 2, rows, chans), f32),
            pltpu.VMEM((rows, feats), f32),
            pltpu.VMEM((2, rows, 128), f32),
            pltpu.VMEM((layers, n_tp, rows, chans), bf16),
            pltpu.VMEM((rows, chans), bf16),
            pltpu.VMEM((3, rows, chans), bf16),
            pltpu.VMEM((3, 16, chans), bf16),
            dma((2,)),
            dma,
            dma((2,)),
            dma((2,)),
            dma((5,)),
            dma,
            dma((3,)),
            dma,
            dma,
            dma((2,)),
            dma((chunks,)),
            dma((GROUP + 5,)),
            dma((6,)),
            dma((6, 4)),
            dma((3,)),
            dma((3,)),
            dma,
            dma((2,)),
        ],
        compiler_params=pltpu.CompilerParams(
            collective_id=0, has_side_effects=True, vmem_limit_bytes=48 * 1024 * 1024
        ),
        name="mixer",
    )(*held)


def solution(mesh):
    in_specs = (
        P("sp", None),
        P(),
        P(None, "sp", "tp"),
        P(None, "sp", "tp"),
        P(None, "sp", "tp"),
        P(None, "sp", "tp"),
        P(None, None, "tp"),
    )
    out_specs = P("sp", "tp")
    body = fused if (mesh.shape["sp"], mesh.shape["tp"]) == (8, 4) else per_device
    return jax.shard_map(
        body, mesh=mesh, in_specs=in_specs, out_specs=out_specs, check_vma=False
    )
```

```python
import functools

import jax
import jax.numpy as jnp
from jax import lax
from jax.experimental import pallas as pl
from jax.experimental.pallas import tpu as pltpu
from jax.sharding import PartitionSpec as P

MESH = pl.DeviceIdType.MESH
f32 = jnp.float32
bf16 = jnp.bfloat16

eps = 1e-06

OUTER, INNER, VALUE, BACK = 0, 1, 2, 3
FIRST = (INNER, VALUE, OUTER)
SECOND = tuple(4 + m for m in FIRST + (BACK,))
SHARED = (BACK,) + SECOND
PIECES = (1, 1, 1, 2, 4, 2, 2, 4)
GROUP = 8


def shifted(block, axis, distance):
    devices = range(lax.axis_size(axis))
    route = [(i - distance, i) for i in devices if i - distance in devices]
    return lax.ppermute(block, axis, route)


def per_device(tokens, norm_gain, w_outer, w_inner, w_value, w_back, taps):
    layers = w_outer.shape[0]
    count = tokens.shape[0]
    feats = w_back.shape[2]
    own = lax.axis_index("tp")
    held = (
        lax.all_gather(w_outer, "sp", axis=1, tiled=True),
        lax.all_gather(w_inner, "sp", axis=1, tiled=True),
        lax.all_gather(w_value, "sp", axis=1, tiled=True),
        lax.all_gather(w_back, "sp", axis=1, tiled=True),
    )
    current = tokens
    resid = lax.dynamic_slice_in_dim(tokens, own * feats, feats, 1)
    for layer in range(layers):
        if layer > 0:
            current = lax.all_gather(resid, "tp", axis=1, tiled=True)
        xf = current.astype(jnp.float32)
        normed = (
            xf * lax.rsqrt(jnp.mean(xf * xf, axis=-1, keepdims=True) + eps) * norm_gain[layer]
        ).astype(jnp.bfloat16)
        outer = jnp.dot(normed, held[0][layer], preferred_element_type=jnp.float32)
        inner = jnp.dot(normed, held[1][layer], preferred_element_type=jnp.float32)
        value = jnp.dot(normed, held[2][layer], preferred_element_type=jnp.float32)
        outer = outer.astype(jnp.bfloat16)
        inner = inner.astype(jnp.bfloat16)
        value = value.astype(jnp.bfloat16)
        mixed = (inner.astype(jnp.float32) * value.astype(jnp.float32)).astype(jnp.bfloat16)
        before = shifted(mixed[count - 2 :], "sp", 1)
        padded = jnp.concatenate([before, mixed], axis=0).astype(jnp.float32)
        conv = (
            taps[layer, 0] * padded[:count]
            + taps[layer, 1] * padded[1 : count + 1]
            + taps[layer, 2] * padded[2:]
        )
        gated = (outer.astype(jnp.float32) * conv).astype(jnp.bfloat16)
        whole = lax.all_gather(gated, "tp", axis=1, tiled=True)
        proj = jnp.dot(whole, held[3][layer], preferred_element_type=jnp.float32)
        resid = (resid.astype(jnp.float32) + proj).astype(jnp.bfloat16)
    return resid


def chunk(u, k, role):
    if u < BACK:
        return u
    return 3 + 3 * (sum(PIECES[BACK:u]) + k) + role - 1


def mixer_kernel(
    tok, gain_hbm, w_outer, w_inner, w_value, w_back, taps_hbm, out,
    gain, taps, xr, xq, stage, x1, scl, sclh, cbuf, cin, win, wback, acc, bacc, ss, gat, gat_end, mixed, halo,
    sem_small, sem_local, sem_tok, t_send, t_recv, c_send, c_recv, s_send, s_recv, w_send, w_recv, p_recv,
    g_send, g_recv, h_send, h_recv, e_send, e_recv,
):
    s, t = lax.axis_index("sp"), lax.axis_index("tp")
    n_sp, n_tp = win.shape[1], xr.shape[0]
    rows, feats = xr.shape[1:]
    quarter = xq.shape[3]
    half = rows // 2
    width = feats * n_tp
    units = len(PIECES)
    core = lax.rem(s, 2)
    flip = 1 - 2 * core
    left = s < n_sp // 2
    side = jnp.where(left, 1, -1)
    own_half = jnp.where(left, 0, 1)
    plane = lax.div(s, 2)
    planes = n_sp // 2
    is_end = jnp.logical_or(plane == 0, plane == planes - 1)
    is_mid = jnp.logical_not(is_end)
    partner = s + flip
    near = jnp.where(is_mid, s - 2 * side, s + 2 * side)
    opp = jnp.where(is_mid, s + 2 * side, s + 4 * side)
    far = jnp.where(is_mid, s + 4 * side, s + 6 * side)
    tx = t + 1 - 2 * lax.rem(t, 2)
    ty = t + 2 - 4 * lax.div(t, 2)
    td = n_tp - 1 - t

    small = (
        pltpu.make_async_copy(gain_hbm, gain, sem_small.at[0]),
        pltpu.make_async_copy(taps_hbm, taps, sem_small.at[1]),
    )

    ahead = (1 - own_half) * (n_tp // 2) + lax.div(t, 2)
    ahead_cols = pl.ds(pl.multiple_of(lax.rem(t, 2) * quarter, quarter), quarter)

    def tok_local(i):
        j = lax.rem(ahead + i, n_tp)
        cols = pl.ds(pl.multiple_of(j * feats, feats), feats)
        return pltpu.make_async_copy(tok.at[:, cols], xr.at[j], sem_tok.at[min(i, 1)])

    def tok_local_wait(slot, count):
        ref = xr.at[pl.ds(0, count)]
        pltpu.make_async_copy(ref, ref, sem_tok.at[slot]).wait()

    for i in range(n_tp):
        tok_local(i).start()
    for copy in small:
        copy.start()
    barrier = pltpu.get_barrier_semaphore()

    def greet(sp, tp):
        pl.semaphore_signal(barrier, inc=1, device_id=(sp, tp), device_id_type=MESH)

    greet(partner, t)
    greet(s, tx)
    greet(s, ty)
    greet(near, t)
    greet(near + flip, t)

    @pl.when(is_mid)
    def _():
        greet(opp, t)
        greet(opp + flip, t)
    pl.semaphore_wait(barrier, jnp.where(is_mid, 7, 5))
    for copy in small:
        copy.wait()

    projections = (w_outer, w_inner, w_value)

    def own_w(u):
        layer, m = u // 4, u % 4
        return projections[m].at[layer] if m < 3 else w_back.at[layer]

    def held_w(u, source):
        layer, m = u // 4, u % 4
        return win.at[3 * layer + m, source] if m < 3 else wback.at[layer, source]

    def remote(a, b, ssem, rsem, sp, tp):
        return pltpu.make_async_remote_copy(
            src_ref=a, dst_ref=b, send_sem=ssem, recv_sem=rsem, device_id=(sp, tp), device_id_type=MESH
        )

    def piece(ref, u, k):
        if u == 7:
            size = ref.shape[1] // PIECES[u]
            return ref.at[:, pl.ds(k * size, size)]
        size = ref.shape[0] // PIECES[u]
        return ref.at[pl.ds(k * size, size)]

    OWN, NEAR, OPP, FAR = 0, 1, 2, 3
    source_of = (s, near, opp, far)

    def w_copy(u, k, role, kind, to_role, target):
        to = piece(held_w(u, source_of[role]), u, k)
        a = piece(own_w(u), u, k) if role == OWN else to
        return remote(a, to, w_send.at[min(kind // 2, 1)], w_recv.at[chunk(u, k, to_role)], target, t)

    def to_partner(u, k, role):
        to = piece(held_w(u, source_of[role]), u, k)
        a = piece(own_w(u), u, k) if role == OWN else to
        return remote(a, to, w_send.at[role // 2], p_recv.at[group_of(u, role, k)], partner, t)

    def pieces_of(u):
        return range(PIECES[u])

    def arrived(u, k, role):
        to = piece(held_w(u, source_of[role]), u, k)
        remote(to, to, w_send.at[0], w_recv.at[chunk(u, k, role)], partner, t).wait_recv()

    def send_opp(u, ks=None):
        for k in ks or pieces_of(u):
            w_copy(u, k, OWN, 4, OPP, opp).start()

    def send_near(u):
        for k in pieces_of(u):
            w_copy(u, k, OWN, 5, NEAR, near).start()

    def send_partner(u):
        for k in pieces_of(u):
            to_partner(u, k, OWN).start()

    def relay_near(u, ks=None):
        for k in ks or pieces_of(u):
            arrived(u, k, NEAR)

            if u >= 3:
                @pl.when(is_mid)
                def _():
                    w_copy(u, k, NEAR, 6, FAR, opp).start()
            to_partner(u, k, NEAR).start()

    def relay_across(u, role, ks=None):
        for k in ks or pieces_of(u):
            arrived(u, k, role)

            @pl.when(is_mid)
            def _():
                w_copy(u, k, role, 5 + role, role, near).start()
            to_partner(u, k, role).start()

    def relay_opp(u, ks=None):
        relay_across(u, OPP, ks)

    def relay_far(u, ks=None):
        relay_across(u, FAR, ks)

    counts = {INNER: 2, VALUE: 2, OUTER: 2, BACK: 4, GROUP: 9, GROUP + 1: 1, GROUP + 2: 1, GROUP + 3: 1, 7: 3}

    def group_of(u, role, k):
        if u <= BACK:
            return u
        if u == 7:
            return GROUP + 4 + k if role == FAR else 7
        return GROUP + 1 + SECOND.index(u) if role == FAR else GROUP

    def settle(group):
        count = counts[group]
        ref = win.at[pl.ds(0, 3), pl.ds(0, 3)] if count == 9 else win.at[0, pl.ds(0, count)]
        remote(ref, ref, w_send.at[0], p_recv.at[group], partner, t).wait_recv()

    def settle_last(k):
        to = piece(held_w(7, far + flip), 7, k)
        remote(to, to, w_send.at[0], p_recv.at[GROUP + 4 + k], partner, t).wait_recv()

    def sent(slot, planes_of, count):
        ref = win.at[pl.ds(0, planes_of), pl.ds(0, count)]
        remote(ref, ref, w_send.at[slot], p_recv.at[0], partner, t).wait_send()

    def local_w(u):
        return pltpu.make_async_copy(own_w(u), held_w(u, s), sem_local)

    def local_w_wait(count):
        ref = win.at[0, pl.ds(0, count)]
        pltpu.make_async_copy(ref, ref, sem_local).wait()

    def tok_quarter(of_half):
        start = of_half * (width // 2) + t * quarter
        return tok.at[:, pl.ds(pl.multiple_of(start, quarter), quarter)]

    def end_tok():
        return remote(tok_quarter(own_half), xq.at[0, t], t_send.at[0], t_recv.at[0], near, t)

    def mid_tok():
        return remote(xr.at[ahead, :, ahead_cols], xq.at[2, t], t_send.at[0], t_recv.at[2], opp, t)

    def to_stage(h):
        span = pl.ds(h * half, half)
        a = xr.at[ahead, span, ahead_cols]
        return remote(a, stage.at[span], t_send.at[1], t_recv.at[3 + h], near, t)

    def from_stage(h):
        span = pl.ds(h * half, half)
        return remote(stage.at[span], xq.at[1, t, span], t_send.at[1], t_recv.at[1], opp, t)

    def tok_arrived(i):
        remote(stage, stage, t_send.at[0], t_recv.at[i], partner, t).wait_recv()

    def part_sum(m, b):
        return remote(cbuf.at[m, b], cin.at[m, b], c_send, c_recv.at[m], opp, t)

    def part_sums(m):
        return remote(cbuf.at[m], cin.at[m], c_send, c_recv.at[m], opp, t)

    def squares_copy():
        return remote(ss.at[1], ss.at[0], s_send, s_recv, near, t)

    def end_part(h):
        return remote(
            gat_end.at[pl.ds(h * half, half)], gat.at[0, t, pl.ds(h * half, half)],
            e_send, e_recv.at[h], near, t,
        )

    class Gather:
        def __init__(self, g, buf, joint=False):
            self.g, self.buf, self.joint = g, buf, joint

        def part(self, block, h, k, target):
            size = self.buf.shape[1] // 2
            ref = self.buf.at[block, pl.ds(h * size, size)]
            slot = (0, 1, 2, 2, 2, 2)[k] if self.joint else (0, 1, 2, 2, 3, 3)[k]
            return remote(ref, ref, g_send.at[self.g], g_recv.at[self.g, slot], s, target)

        def whole(self, blocks, slot):
            ref = self.buf.at[pl.ds(0, blocks)]
            return remote(ref, ref, g_send.at[self.g], g_recv.at[self.g, slot], s, tx)

        def start(self, h):
            if h == 0:
                self.part(t, 0, 0, tx).start()
                self.part(t, 0, 3, ty).start()
            else:
                self.part(t, 1, 1, ty).start()
                self.part(t, 1, 2, tx).start()

        def start_all(self):
            self.part(t, 0, 0, tx).start()
            self.part(t, 1, 1, ty).start()
            self.part(t, 1, 2, tx).start()
            self.part(t, 0, 3, ty).start()

        def forward(self, h):
            if h == 0:
                self.part(tx, 0, 0, tx).wait_recv()
                self.part(tx, 0, 4, ty).start()
            else:
                self.part(ty, 1, 1, ty).wait_recv()
                self.part(ty, 1, 5, tx).start()

        def beside(self):
            self.whole(1, 2).wait_recv()

        def across(self):
            self.whole(1, 3).wait_recv()

        def rest(self):
            self.whole(2, 2).wait_recv()

        def drain(self):
            self.whole(3, 0).wait_send()

    gather_tok = (Gather(0, xq.at[0]), Gather(4, xq.at[1]), Gather(5, xq.at[2]))
    gather_gat = (Gather(1, gat.at[0], True), Gather(3, gat.at[1], True))
    gather_x = Gather(2, x1)

    def row_tiles(body):
        step = 64

        def tile(r, carry):
            body(pl.ds(pl.multiple_of(r * step, step), step))
            return carry

        lax.fori_loop(0, rows // step, tile, 0)

    def lane_sums(x):
        sq = x * x
        part = sq[:, :128]
        for q in range(1, x.shape[1] // 128):
            part = part + sq[:, 128 * q : 128 * (q + 1)]
        return part

    def squares(b):
        ss[b] = jnp.zeros(ss.shape[1:], f32)

        def one(j, carry):
            def body(span):
                ss[b, span, :] += lane_sums(xr[j, span, :].astype(f32))
            row_tiles(body)
            return carry

        lax.fori_loop(0, n_tp, one, 0)

    def scale(j):
        def body(span):
            x = x1[j, span, :].astype(f32)
            ss[0, span, :] += lane_sums(x)
            cols = pl.ds(pl.multiple_of(j * feats, feats), feats)
            scl[j, span, :] = (x * gain[1:2, cols]).astype(bf16)
        row_tiles(body)

    def scale_part(load, block, j):
        at = pl.multiple_of(j * quarter, quarter)
        cols = pl.ds(pl.multiple_of(own_half * (width // 2) + at, quarter), quarter)

        def body(span):
            sclh[block, span, pl.ds(at, quarter)] = (load(span).astype(f32) * gain[0:1, cols]).astype(bf16)
        row_tiles(body)

    def scale_sent(i, j):
        scale_part(lambda span: xq[i, j, span, :], (0, 2, 3)[i], j)

    def half_dot(m, block):
        depth = win.shape[2]
        sources = pl.ds(own_half * (n_sp // 2), n_sp // 2)
        w = win[m, sources].reshape(n_sp // 2 * depth, win.shape[3])
        return jnp.dot(sclh[block], w, preferred_element_type=f32)

    def send_part_sum(m, b):
        cbuf[m, b] = half_dot(m, 2 + b).astype(bf16)
        part_sum(m, b).start()

    def add_part_sums(m):
        part_sums(m).wait_recv()
        for b in range(2):
            acc[m, b] += cin[m, b].astype(f32)

    def project(m, sources, first):
        depth = win.shape[2]
        total = None
        for role in sources:
            z = lax.div(source_of[role], 2)
            w = win[3 + m, pl.ds(2 * z, 2)].reshape(2 * depth, win.shape[3])
            dot = jnp.dot(scl[z], w, preferred_element_type=f32)
            total = dot if total is None else total + dot
        if first:
            acc[m, 0] = total
        else:
            acc[m, 0] += total

    def inv_of(b):
        return lax.rsqrt(jnp.sum(ss[b], axis=-1, keepdims=True) / width + eps)

    def mix(b, slot):
        inv = inv_of(b)
        inner = (acc[INNER, b] * inv).astype(bf16)
        value = (acc[VALUE, b] * inv).astype(bf16)
        mixed[slot] = (inner.astype(f32) * value.astype(f32)).astype(bf16)

    def convolve(layer, b, slot):
        now = mixed[slot].astype(f32)
        tail = halo[slot].astype(f32)
        row = lax.broadcasted_iota(jnp.int32, now.shape, 0)
        one = jnp.where(row == 0, tail[15:16], pltpu.roll(now, 1, 0))
        two = pltpu.roll(now, 2, 0)
        two = jnp.where(row == 0, tail[14:15], jnp.where(row == 1, tail[15:16], two))
        acc[VALUE, b] = taps[0, layer : layer + 1] * two + taps[1, layer : layer + 1] * one + taps[2, layer : layer + 1] * now

    def gate(b):
        outer = (acc[OUTER, b] * inv_of(b)).astype(bf16).astype(f32)
        return (outer * acc[VALUE, b]).astype(bf16)

    def tail_copy(slot, to_slot, h, target):
        return remote(
            mixed.at[slot, pl.ds(rows - 16, 16)], halo.at[to_slot], h_send.at[slot], h_recv.at[h], target, t
        )

    def back_dot(layer, sources, cols):
        total = None
        for role in sources:
            z = lax.div(source_of[role], 2)
            w = wback[layer, pl.ds(2 * z, 2), :, cols].reshape(2 * wback.shape[2], cols.size)
            dot = jnp.dot(gat[layer, z], w, preferred_element_type=f32)
            total = dot if total is None else total + dot
        return total

    def by_columns(body):
        step = 256
        for c in range(feats // step):
            body(pl.ds(c * step, step))

    @pl.when(is_mid)
    def _():
        tok_local_wait(0, 1)
        mid_tok().start()
        for u in FIRST + SHARED:
            send_partner(u)
        for u in SHARED:
            send_near(u)
        for u in FIRST + SHARED:
            local_w(u).start()
        tok_local_wait(1, n_tp - 1)
        squares(1)

        def scale_own(j, carry):
            piece_of = own_half * (n_tp // 2) + lax.div(j, 2)
            cols = pl.ds(pl.multiple_of(lax.rem(j, 2) * quarter, quarter), quarter)
            scale_part(lambda span: xr[piece_of, span, cols], 1, j)
            return carry

        lax.fori_loop(0, n_tp, scale_own, 0)
        local_w_wait(units)
        own_end, far_end, far_mid = gather_tok
        for h in range(2):
            to_stage(h).wait_recv()
            from_stage(h).start()
        send_opp(BACK)
        send_opp(SECOND[0])
        tok_arrived(2)
        far_mid.start_all()
        scale_sent(2, t)
        far_mid.forward(0)
        far_mid.forward(1)
        tok_arrived(1)
        far_end.start_all()
        far_mid.beside()
        scale_sent(2, tx)
        scale_sent(2, ty)
        far_mid.across()
        scale_sent(2, td)
        relay_near(INNER)
        settle(INNER)
        send_part_sum(INNER, 1)
        far_end.forward(0)
        far_end.forward(1)
        relay_near(VALUE)
        settle(VALUE)
        send_part_sum(VALUE, 1)
        relay_opp(BACK)
        scale_sent(1, t)
        far_end.beside()
        scale_sent(1, tx)
        scale_sent(1, ty)
        relay_opp(SECOND[0])
        tok_arrived(0)
        own_end.start_all()
        scale_sent(0, t)
        far_end.across()
        scale_sent(1, td)
        send_part_sum(INNER, 0)
        send_part_sum(VALUE, 0)
        relay_near(OUTER)
        settle(OUTER)
        own_end.forward(0)
        own_end.forward(1)
        send_part_sum(OUTER, 0)
        send_part_sum(OUTER, 1)
        own_end.beside()
        scale_sent(0, tx)
        scale_sent(0, ty)
        own_end.across()
        scale_sent(0, td)
        for m in FIRST:
            for b in range(2):
                acc[m, b] = half_dot(m, b)
        add_part_sums(INNER)
        add_part_sums(VALUE)
        squares_copy().wait_recv()
        for b in range(2):
            mix(b, b)

        @pl.when(core == 0)
        def _():
            for b in range(2):
                tail_copy(b, b, b, partner).start()

        @pl.when(jnp.logical_and(core == 1, left))
        def _():
            tail_copy(1, 1, 1, s + 1).start()
            tail_copy(0, 1, 1, partner).start()

        @pl.when(jnp.logical_and(core == 1, jnp.logical_not(left)))
        def _():
            tail_copy(1, 0, 0, partner).start()
        relay_near(BACK)
        send_opp(SECOND[1])
        send_opp(SECOND[2])
        @pl.when(s == 2)
        def _():
            halo[0] = jnp.zeros(halo.shape[1:], bf16)

        @pl.when(s != 2)
        def _():
            tail_copy(0, 0, 0, partner).wait_recv()
        convolve(0, 0, 0)
        add_part_sums(OUTER)
        gat_end[...] = gate(0)
        for h in range(2):
            end_part(h).start()
        tail_copy(1, 1, 1, partner).wait_recv()
        convolve(0, 1, 1)
        gat[0, t] = gate(1)
        gather_gat[0].start_all()
        relay_far(BACK, (0,))
        gather_gat[0].forward(0)
        gather_gat[0].forward(1)
        relay_near(SECOND[0])
        relay_far(BACK, (1,))

    @pl.when(is_end)
    def _():
        tok_local_wait(0, 1)
        for h in range(2):
            to_stage(h).start()
        send_near(INNER)
        send_near(VALUE)
        end_tok().start()
        send_near(OUTER)
        for u in SHARED:
            send_partner(u)
        for u in SHARED:
            local_w(u).start()
        tok_local_wait(1, n_tp - 1)
        squares(1)
        squares_copy().start()
        for u in SHARED:
            send_near(u)
        local_w_wait(units - 3)
        for u in SHARED:
            relay_near(u)
        relay_opp(BACK)
        relay_opp(SECOND[0])
        for h in range(2):
            end_part(h).wait_recv()
            gather_gat[0].start(h)
        gather_gat[0].forward(0)
        relay_far(BACK, (0,))
        gather_gat[0].forward(1)
        relay_far(BACK, (1,))

    gather_gat[0].rest()
    settle(BACK)

    @pl.when(is_mid)
    def _():
        relay_opp(SECOND[1], (0,))

    def finish_first(cols):
        total = xr[t, :, cols].astype(f32) + back_dot(0, (OWN, NEAR, OPP, FAR), cols)
        x1[t, :, cols] = total.astype(bf16)

    by_columns(finish_first)
    gather_x.start_all()

    @pl.when(is_end)
    def _():
        relay_opp(SECOND[1], (0,))
    relay_opp(SECOND[1], (1,))

    @pl.when(is_mid)
    def _():
        relay_near(SECOND[1])
    ss[0] = jnp.zeros(ss.shape[1:], f32)
    scale(t)
    relay_opp(SECOND[2])

    @pl.when(is_mid)
    def _():
        relay_near(SECOND[2])
    gather_x.forward(0)
    gather_x.forward(1)
    relay_far(SECOND[0])
    gather_x.beside()
    scale(tx)
    scale(ty)
    relay_far(SECOND[1])
    gather_x.across()
    scale(td)
    settle(GROUP)
    def early_far(k):
        @pl.when(is_mid)
        def _():
            relay_far(SECOND[2], (k,))

    last = SECOND[3]

    @pl.when(is_mid)
    def _():
        send_opp(last, (0, 1))
    early_far(0)
    settle(GROUP + 1)
    project(INNER, (OWN, NEAR, OPP, FAR), True)
    early_far(1)
    project(VALUE, (OWN, NEAR, OPP), True)
    settle(GROUP + 2)
    project(VALUE, (FAR,), False)
    early_far(2)
    mix(0, 2)

    @pl.when(s < n_sp - 1)
    def _():
        tail_copy(2, 2, 2, s + 1).start()

    @pl.when(is_mid)
    def _():
        send_opp(last, (2, 3))
        relay_near(last)
    project(OUTER, (OWN, NEAR, OPP), True)

    @pl.when(is_end)
    def _():
        relay_far(SECOND[2], (0, 1, 2))
    relay_far(SECOND[2], (3,))

    @pl.when(is_mid)
    def _():
        relay_opp(last)

    @pl.when(s == 0)
    def _():
        halo[2] = jnp.zeros(halo.shape[1:], bf16)

    @pl.when(s > 0)
    def _():
        tail_copy(2, 2, 2, partner).wait_recv()
    convolve(1, 0, 2)
    settle(GROUP + 3)
    project(OUTER, (FAR,), False)
    gat[1, t] = gate(0)
    gather_gat[1].start_all()

    @pl.when(is_end)
    def _():
        relay_opp(last, (0, 1))

    @pl.when(is_mid)
    def _():
        relay_far(last, (0, 1))
    gather_gat[1].forward(0)
    gather_gat[1].forward(1)

    @pl.when(is_end)
    def _():
        relay_opp(last, (2, 3))
        relay_far(last, (0, 1))

    @pl.when(is_mid)
    def _():
        relay_far(last, (2, 3))
    gather_gat[1].rest()
    settle(last)

    def start_last(cols):
        bacc[:, cols] = x1[t, :, cols].astype(f32) + back_dot(1, (OWN, NEAR, OPP), cols)

    by_columns(start_last)

    @pl.when(is_end)
    def _():
        relay_far(last, (2, 3))

    def finish_last(cols):
        out[:, cols] = (bacc[:, cols] + back_dot(1, (FAR,), cols)).astype(bf16)

    size = feats // PIECES[last]
    for k in pieces_of(last):
        settle_last(k)
        finish_last(pl.ds(k * size, size))

    some = units - 3

    @pl.when(is_mid)
    def _():
        sent(0, 2, units)
        sent(1, some, 7)
        for g in gather_tok:
            g.drain()
        for i in range(2):
            remote(stage, stage, t_send.at[i], t_recv.at[0], partner, t).wait_send()
        remote(cbuf, cin, c_send, c_recv.at[0], partner, t).wait_send()
        remote(gat_end, gat_end, e_send, e_recv.at[0], partner, t).wait_send()

        @pl.when(core == 0)
        def _():
            for b in range(2):
                tail_copy(b, b, b, partner).wait_send()

        @pl.when(jnp.logical_and(core == 1, left))
        def _():
            tail_copy(0, 1, 1, partner).wait_send()
            tail_copy(1, 1, 1, s + 1).wait_send()

        @pl.when(jnp.logical_and(core == 1, jnp.logical_not(left)))
        def _():
            tail_copy(1, 0, 0, partner).wait_send()

    @pl.when(is_end)
    def _():
        sent(0, 2, some)
        sent(1, 3, 6)
        for i in range(2):
            remote(stage, stage, t_send.at[i], t_recv.at[0], partner, t).wait_send()
        squares_copy().wait_send()
    gather_gat[0].drain()
    gather_x.drain()
    gather_gat[1].drain()

    @pl.when(s < n_sp - 1)
    def _():
        tail_copy(2, 2, 2, partner).wait_send()


def fused(tokens, norm_gain, w_outer, w_inner, w_value, w_back, taps):
    n_sp, n_tp = lax.axis_size("sp"), lax.axis_size("tp")
    rows, width = tokens.shape
    layers, depth, chans = w_outer.shape
    back_rows, feats = w_back.shape[1:]
    if 4 * layers != len(PIECES):
        return per_device(tokens, norm_gain, w_outer, w_inner, w_value, w_back, taps)
    chunks = 3 + 3 * sum(PIECES[BACK:])
    dma = pltpu.SemaphoreType.DMA
    hbm, vmem = pl.BlockSpec(memory_space=pl.ANY), pl.BlockSpec(memory_space=pltpu.VMEM)
    held = [
        pltpu.with_memory_space_constraint(a, pltpu.HBM)
        for a in (tokens, norm_gain, w_outer, w_inner, w_value, w_back, taps.transpose(1, 0, 2))
    ]
    return pl.pallas_call(
        mixer_kernel,
        out_shape=jax.ShapeDtypeStruct((rows, feats), bf16),
        in_specs=[hbm] * 7,
        out_specs=vmem,
        scratch_shapes=[
            pltpu.VMEM((layers, width), f32),
            pltpu.VMEM(taps.shape[1:2] + taps.shape[:1] + taps.shape[2:], f32),
            pltpu.VMEM((n_tp, rows, feats), bf16),
            pltpu.VMEM((3, n_tp, rows, width // 2 // n_tp), bf16),
            pltpu.VMEM((rows, width // 2 // n_tp), bf16),
            pltpu.VMEM((n_tp, rows, feats), bf16),
            pltpu.VMEM((n_tp, rows, feats), bf16),
            pltpu.VMEM((4, rows, width // 2), bf16),
            pltpu.VMEM((3, 2, rows, chans), bf16),
            pltpu.VMEM((3, 2, rows, chans), bf16),
            pltpu.VMEM((3 * layers, n_sp, depth, chans), bf16),
            pltpu.VMEM((layers, n_sp, back_rows, feats), bf16),
            pltpu.VMEM((3, 2, rows, chans), f32),
            pltpu.VMEM((rows, feats), f32),
            pltpu.VMEM((2, rows, 128), f32),
            pltpu.VMEM((layers, n_tp, rows, chans), bf16),
            pltpu.VMEM((rows, chans), bf16),
            pltpu.VMEM((3, rows, chans), bf16),
            pltpu.VMEM((3, 16, chans), bf16),
            dma((2,)),
            dma,
            dma((2,)),
            dma((2,)),
            dma((5,)),
            dma,
            dma((3,)),
            dma,
            dma,
            dma((2,)),
            dma((chunks,)),
            dma((GROUP + 4 + PIECES[-1],)),
            dma((6,)),
            dma((6, 4)),
            dma((3,)),
            dma((3,)),
            dma,
            dma((2,)),
        ],
        compiler_params=pltpu.CompilerParams(
            collective_id=0, has_side_effects=True, vmem_limit_bytes=48 * 1024 * 1024
        ),
        name="mixer",
    )(*held)


def solution(mesh):
    in_specs = (
        P("sp", None),
        P(),
        P(None, "sp", "tp"),
        P(None, "sp", "tp"),
        P(None, "sp", "tp"),
        P(None, "sp", "tp"),
        P(None, None, "tp"),
    )
    out_specs = P("sp", "tp")
    body = fused if (mesh.shape["sp"], mesh.shape["tp"]) == (8, 4) else per_device
    return jax.shard_map(
        body, mesh=mesh, in_specs=in_specs, out_specs=out_specs, check_vma=False
    )
```
